32 devices in a mesh: sp: 8 (over z, y), tp: 4 (over x, core).
Axes of the slice: x: 2, y: 2, z: 4, core: 2. Of those that a mesh axis runs over, the one named last changes fastest.
Arguments:
- queries: bfloat16 [4096, 512], P('sp', 'tp'), may hold values from -6 to 6
- key_matrix: bfloat16 [4096, 512], P('sp', 'tp'), may hold values from -6 to 6
- value_matrix: bfloat16 [4096, 1024], P('sp', 'tp'), may hold values from -6 to 6
- channel_decay_input: bfloat16 [4096, 512], P('sp', 'tp')
- head_decay_offset: float32 [4096, 8], P('sp', 'tp'), may hold values from -1 to 0
- output_gate_input: bfloat16 [4096, 1024], P('sp', 'tp'), may hold values from -6 to 6
- head_norm_gain: float32 [128], replicated, may hold values from 0.1 to 1.9
- residual: bfloat16 [4096, 2048], P(('sp', 'tp')), may hold values from -6 to 6
- mixer_output_weight: bfloat16 [1024, 2048], replicated, may hold values from -0.1875 to 0.1875
- expert_norm_gain: float32 [2048], replicated, may hold values from 0.1 to 1.9
- routes: int32 [4096, 4], P(('sp', 'tp')), may hold values from 0 to 63, all different within a row; in each aligned block of 128 rows (0 to 127, 128 to 255, ...) at most 16 rows name the same one
- chosen_router_scores: float32 [4096, 4], P(('sp', 'tp')), may hold values from 0.1 to 1
- routed_gate_weight: bfloat16 [64, 2048, 512], P(('sp', 'tp')), may hold values from -0.125 to 0.125
- routed_up_weight: bfloat16 [64, 2048, 512], P(('sp', 'tp')), may hold values from -0.125 to 0.125
- routed_down_weight: bfloat16 [64, 512, 2048], P(('sp', 'tp')), may hold values from -0.25 to 0.25
- common_gate_weight: bfloat16 [2048, 512], replicated, may hold values from -0.125 to 0.125
- common_up_weight: bfloat16 [2048, 512], replicated, may hold values from -0.125 to 0.125
- common_down_weight: bfloat16 [512, 2048], replicated, may hold values from -0.25 to 0.25
Outputs:
- layer_out: bfloat16 [4096, 2048], P(('sp', 'tp'))
The draws below stay inside these ranges and needn't reach their ends.
Inputs may be any that keep to these rules, and one draw needn't show every extreme that they name: `routes`: each row names 4 different experts. In each aligned block of 128 rows (the rows of one device) no expert is named by more than 16 rows, a bound that some block reaches.
All inputs are finite; a program needn't handle non-finite values.
Results may differ from the reference program's by a relative error of at most 0.017.
Values may be sent and summed in bfloat16 or wider, within the bound.
A program may use at most 128 MiB of HBM per device.

```python
import math
import jax
import jax.numpy as jnp
import numpy as np
from jax import lax

D = 2048
HEADS = 8
KEY_CHANNELS = 64
VDIM = 128
BLOCK = 64
FFE = 512
SFF = 512
TOP_K = 4
TOK_DEV = 128
KW = 512
VW = 1024
TOK_SP = 512
TOKENS = 4096
EXPERTS = 64
CAP = 16


def draw_channel_decay_input(key, part):
    head_key = jax.random.fold_in(key, 11)
    channel_key = jax.random.fold_in(key, 12)
    shift_key = jax.random.fold_in(key, 13)
    jitter_key = jax.random.fold_in(key, 14)
    slow_heads = jax.random.bernoulli(head_key, 0.5, (HEADS,))
    jitter = jnp.clip(0.5 * jax.random.normal(jitter_key, (TOKENS, HEADS * KEY_CHANNELS), jnp.float32), -1.5, 1.5)
    head_base = jnp.where(slow_heads, math.log(TOKENS) - 1.5, 0.5).astype(jnp.float32)
    channel = jax.random.uniform(channel_key, (HEADS, KEY_CHANNELS), jnp.float32, -0.5, 0.5)
    column = (head_base[:, None] + channel).reshape(HEADS * KEY_CHANNELS)
    shifts = jax.random.uniform(shift_key, (TOKENS // TOK_SP,), jnp.float32, 0.0, math.log(4.0))
    rows_shift = jnp.repeat(shifts, TOK_SP)
    return (column[None, :] + jitter - rows_shift[:, None]).astype(jnp.bfloat16)


def draw_head_decay_offset(key, part):
    place_key = jax.random.fold_in(key, 21)
    size_key = jax.random.fold_in(key, 22)
    places = jax.random.randint(place_key, (3, HEADS), 0, TOKENS)
    drops = jax.random.uniform(size_key, (3, HEADS), jnp.float32, math.log(0.5), math.log(0.8))
    positions = jnp.arange(TOKENS, dtype=jnp.int32)
    landed = positions[:, None, None] == places[None, :, :]
    return jnp.sum(jnp.where(landed, drops[None, :, :], 0.0), axis=1).astype(jnp.float32)


def level_of(own_key, shape, shards, low, high):
    def one(position, blocks):
        heights = jax.random.uniform(jax.random.fold_in(jax.random.fold_in(own_key, 6), position), (blocks,), jnp.float32, low / len(shards), high / len(shards))
        return jnp.repeat(jnp.exp(heights), shape[position] // blocks).reshape((-1,) + (1,) * (len(shape) - position - 1))

    loudness = one(*shards[0])
    for cut in shards[1:]:
        loudness = loudness * one(*cut)
    return loudness


def routed_block(stream_key, own, number, rows, number_of, top, reach, skew):
    order = jax.random.permutation(stream_key, number_of)
    heavy_load, ordinary = portions_of(number_of, rows * top, reach, skew, True), portions_of(number_of, rows * top, reach, skew, False)
    places = jnp.arange(number_of)

    def named(sizes, offset_by):
        used = int((sizes > 0).sum())
        fixed = max(1, used // 4)
        passed = fixed + (places - fixed + offset_by * (used - fixed)) % max(1, number_of - fixed)
        return jnp.zeros((number_of,), jnp.int32).at[order[jnp.where(places < fixed, places, passed)]].set(jnp.asarray(sizes, jnp.int32))

    sizes = jnp.where(number % 4 == 0, named(heavy_load, number // 4), named(ordinary, number - number // 4 - 1))
    mixed = jax.random.permutation(jax.random.fold_in(own, 3), number_of)
    giver, taker = mixed[0:number_of // 2 * 2:2], mixed[1:number_of // 2 * 2:2]
    margin = jnp.minimum(sizes[giver] - 1, reach - sizes[taker]) // 2
    margin = jnp.where((giver == order[0]) | (taker == order[0]) | (sizes[taker] == 0), 0, jnp.maximum(margin, 0))
    passed = jax.random.randint(jax.random.fold_in(own, 4), (number_of // 2,), 0, 1 << 20) % (margin + 1)
    sizes = sizes.at[giver].add(-passed).at[taker].add(passed)
    items = jnp.searchsorted(jnp.cumsum(sizes), jnp.arange(rows * top), side="right").astype(jnp.int32)
    listing = items.reshape(top, rows).T
    listing = listing[jax.random.permutation(jax.random.fold_in(own, 1), rows)]
    offset_by = jax.random.randint(jax.random.fold_in(own, 2), (rows, 1), 0, top)
    return jnp.take_along_axis(listing, (jnp.arange(top)[None, :] + offset_by) % top, axis=1)


def portions_of(amount, total, reach, skew, full):
    portions = [(1 << 20) // math.isqrt(grade ** skew) + 1 for grade in range(1, amount + 1)]
    largest = reach if full else min(reach, max(-(-total // amount), total * portions[0] // sum(portions)))
    least = 1 if total - largest >= amount - 1 else 0
    given, surplus = [largest] + [least] * (amount - 1), total - largest - least * (amount - 1)
    while surplus > 0:
        movable = [i for i in range(1, amount) if given[i] < largest] or [i for i in range(1, amount) if given[i] < reach]
        mass, budget = sum([portions[i] for i in movable]), surplus
        for i in movable:
            extra = min(reach - given[i], max(1, budget * portions[i] // mass), surplus)
            given[i] = given[i] + extra
            surplus = surplus - extra
    return np.array(given)


def scatter_about(own_key, shape, deviation, reach, cuts=(), held_as=jnp.bfloat16):
    values = jax.random.normal(own_key, shape, jnp.float32) * deviation
    if len(cuts) > 0:
        values = level_of(own_key, shape, cuts, -0.22, 0.18) * values
    return jnp.clip(values, min=-reach, max=reach).astype(held_as)


def setup_inputs(seed: int = 0) -> dict:
    arg_keys = jax.random.split(jax.random.key(seed), 19)
    queries = scatter_about(arg_keys[0], (TOKENS, KW), 1.0, 6.0, ((0, 8), (1, 4)))
    key_matrix = scatter_about(arg_keys[1], (TOKENS, KW), 1.0, 6.0, ((0, 8), (1, 4)))
    value_matrix = scatter_about(arg_keys[2], (TOKENS, VW), 1.0, 6.0, ((0, 8), (1, 4)))
    channel_decay_input = draw_channel_decay_input(jax.random.fold_in(arg_keys[18], 71), 0)
    head_decay_offset = draw_head_decay_offset(jax.random.fold_in(arg_keys[18], 71), 0)
    output_gate_input = scatter_about(arg_keys[5], (TOKENS, VW), 1.0, 6.0, ((0, 8), (1, 4)))
    head_norm_gain = jnp.clip(1.0 + 0.18 * jax.random.normal(arg_keys[6], (VDIM,), jnp.float32), 0.1, 1.9)
    residual = scatter_about(arg_keys[7], (TOKENS, D), 1.0, 6.0, ((0, 32),))
    mixer_output_weight = scatter_about(arg_keys[8], (VW, D), VW ** -0.5, 0.1875)
    expert_norm_gain = jnp.clip(1.0 + 0.18 * jax.random.normal(arg_keys[9], (D,), jnp.float32), 0.1, 1.9)
    routes_keys = jax.random.split(jax.random.fold_in(arg_keys[10], 1), TOKENS // TOK_DEV)
    routes_turns = jax.random.permutation(jax.random.fold_in(arg_keys[10], 3), TOKENS // TOK_DEV)
    routes = jax.vmap(lambda own, number: routed_block(jax.random.fold_in(arg_keys[10], 2), own, number, TOK_DEV, EXPERTS, TOP_K, CAP, 2))(routes_keys, routes_turns).reshape((TOKENS, TOP_K))
    chosen_router_scores = jnp.clip(jnp.exp(math.log(1.0) - 2.3025851 * jax.random.uniform(arg_keys[11], (TOKENS, TOP_K), jnp.float32) ** level_of(arg_keys[11], (TOKENS, TOP_K), ((0, 32),), -0.2, 0.2)), 0.1, 1.0)
    routed_gate_weight = scatter_about(arg_keys[12], (EXPERTS, D, FFE), D ** -0.5, 0.125, ((0, 32),))
    routed_up_weight = scatter_about(arg_keys[13], (EXPERTS, D, FFE), D ** -0.5, 0.125, ((0, 32),))
    routed_down_weight = scatter_about(arg_keys[14], (EXPERTS, FFE, D), FFE ** -0.5, 0.25, ((0, 32),))
    common_gate_weight = scatter_about(arg_keys[15], (D, SFF), D ** -0.5, 0.125)
    common_up_weight = scatter_about(arg_keys[16], (D, SFF), D ** -0.5, 0.125)
    common_down_weight = scatter_about(arg_keys[17], (SFF, D), SFF ** -0.5, 0.25)
    return dict(queries=queries, key_matrix=key_matrix, value_matrix=value_matrix, channel_decay_input=channel_decay_input, head_decay_offset=head_decay_offset, output_gate_input=output_gate_input, head_norm_gain=head_norm_gain, residual=residual, mixer_output_weight=mixer_output_weight, expert_norm_gain=expert_norm_gain, routes=routes, chosen_router_scores=chosen_router_scores, routed_gate_weight=routed_gate_weight, routed_up_weight=routed_up_weight, routed_down_weight=routed_down_weight, common_gate_weight=common_gate_weight, common_up_weight=common_up_weight, common_down_weight=common_down_weight)


eps_norm = 1e-06
decay_running = 16.0
routed_scale = 2.5

def split_heads(values, columns):
    blocks = values.shape[0] // BLOCK
    return values.astype(jnp.float32).reshape(blocks, BLOCK, HEADS, columns).transpose(2, 0, 1, 3)

def recurrent_mixer(queries, key_matrix, value_matrix, channel_decay_input, head_decay_offset, output_gate_input, head_norm_gain):
    decay_spike_columns = jnp.repeat(head_decay_offset, KEY_CHANNELS, axis=1)
    decay_logarithm = jax.nn.log_sigmoid(channel_decay_input.astype(jnp.float32)) / decay_running + decay_spike_columns
    within = jnp.cumsum(split_heads(decay_logarithm, KEY_CHANNELS), axis=2)
    block_end = within[:, :, -1:, :]
    q_heads = split_heads(queries, KEY_CHANNELS) * KEY_CHANNELS ** (-0.5)
    k_heads = split_heads(key_matrix, KEY_CHANNELS)
    v_heads = split_heads(value_matrix, VDIM)
    q_decay = q_heads * jnp.exp(within)
    k_grow = k_heads * jnp.exp(-within)
    k_tail = k_heads * jnp.exp(block_end - within)
    causal = jnp.tril(jnp.ones((BLOCK, BLOCK), dtype=bool))
    scores = jnp.where(causal, jnp.einsum('hnid,hnjd->hnij', q_decay, k_grow), 0.0)
    output = jnp.einsum('hnij,hnje->hnie', scores, v_heads)
    block_state = jnp.einsum('hncd,hnce->nhde', k_tail, v_heads)
    block_decay = jnp.moveaxis(jnp.exp(block_end[:, :, 0, :]), 1, 0)

    def advance(carried, block_inputs):
        added_state, factor = block_inputs
        return (factor[..., None] * carried + added_state, carried)
    start_state = jnp.zeros((HEADS, KEY_CHANNELS, VDIM), jnp.float32)
    _, entering = lax.scan(advance, start_state, (block_state, block_decay))
    output = output + jnp.einsum('hncd,nhde->hnce', q_decay, entering)
    output = output.transpose(1, 2, 0, 3).reshape(-1, HEADS, VDIM)
    inv_rms = lax.rsqrt(lax.optimization_barrier(jnp.mean(output * output, axis=-1, keepdims=True)) + eps_norm)
    normed = (output * inv_rms * head_norm_gain).reshape(-1, HEADS * VDIM)
    return (normed * jax.nn.silu(output_gate_input.astype(jnp.float32))).astype(jnp.bfloat16)

def expert_block(picked_rows, gate_weight, up_weight, down_weight):
    gate_pre = jnp.dot(picked_rows, gate_weight, preferred_element_type=jnp.float32)
    up_pre = jnp.dot(picked_rows, up_weight, preferred_element_type=jnp.float32)
    hidden = (jax.nn.silu(gate_pre) * up_pre).astype(jnp.bfloat16)
    return jnp.dot(hidden, down_weight, preferred_element_type=jnp.float32)

def reference(queries, key_matrix, value_matrix, channel_decay_input, head_decay_offset, output_gate_input, head_norm_gain, residual, mixer_output_weight, expert_norm_gain, routes, chosen_router_scores, routed_gate_weight, routed_up_weight, routed_down_weight, common_gate_weight, common_up_weight, common_down_weight):
    gated_output = recurrent_mixer(queries, key_matrix, value_matrix, channel_decay_input, head_decay_offset, output_gate_input, head_norm_gain)
    middle = (residual.astype(jnp.float32) + jnp.dot(gated_output, mixer_output_weight, preferred_element_type=jnp.float32)).astype(jnp.bfloat16)
    middle_wide = middle.astype(jnp.float32)
    inv_rms = lax.rsqrt(lax.optimization_barrier(jnp.mean(middle_wide * middle_wide, axis=-1, keepdims=True)) + eps_norm)
    normed = (middle_wide * inv_rms * expert_norm_gain).astype(jnp.bfloat16)
    weights = routed_scale * chosen_router_scores / lax.optimization_barrier(jnp.sum(chosen_router_scores, axis=-1, keepdims=True))
    flat_expert = routes.reshape(-1).astype(jnp.int32)
    assigned = TOKENS * TOP_K
    flat_token = (jnp.arange(assigned, dtype=jnp.int32) // TOP_K).astype(jnp.int32)
    flat_weight = weights.reshape(-1)
    sorted_ids = jnp.argsort(flat_expert, stable=True).astype(jnp.int32)
    counts = jnp.bincount(flat_expert, length=EXPERTS).astype(jnp.int32)
    starts = (jnp.cumsum(counts) - counts).astype(jnp.int32)
    slot_room = TOKENS // TOK_DEV * CAP
    order_pad = jnp.concatenate([sorted_ids, jnp.full((slot_room,), assigned, jnp.int32)])
    token_pad = jnp.concatenate([flat_token, jnp.full((1,), TOKENS, jnp.int32)])
    weight_pad = jnp.concatenate([flat_weight, jnp.zeros((1,), jnp.float32)])
    normed_pad = jnp.concatenate([normed, jnp.zeros((1, D), jnp.bfloat16)], axis=0)

    def one_expert(summed, expert_id):
        picked = lax.dynamic_slice_in_dim(order_pad, starts[expert_id], slot_room)
        live_slot = jnp.arange(slot_room, dtype=jnp.int32) < counts[expert_id]
        picked = jnp.where(live_slot, picked, assigned).astype(jnp.int32)
        tokens = token_pad[picked]
        picked_rows = normed_pad[tokens]
        result = expert_block(picked_rows, routed_gate_weight[expert_id], routed_up_weight[expert_id], routed_down_weight[expert_id]).astype(jnp.bfloat16)
        return (summed.at[tokens].add(weight_pad[picked][:, None] * result.astype(jnp.float32)), None)
    routed, _ = lax.scan(one_expert, jnp.zeros((TOKENS + 1, D), jnp.float32), jnp.arange(EXPERTS, dtype=jnp.int32))
    shared = expert_block(normed, common_gate_weight, common_up_weight, common_down_weight)
    return (middle_wide + routed[:TOKENS] + shared).astype(jnp.bfloat16)
```

```python
import functools
import math

import jax
import jax.numpy as jnp
from jax import lax
from jax.experimental import pallas as pl
from jax.experimental.pallas import tpu as pltpu
from jax.sharding import PartitionSpec as P

D = 2048
KEY_CHANNELS = 64
VDIM = 128
BLOCK = 64
TOP_K = 4


eps_norm = 1e-06
decay_running = 16.0
routed_scale = 2.5


def peer(sp, tp):
    return {"sp": sp, "tp": tp}


def greet(targets):
    barrier = pltpu.get_barrier_semaphore()
    for target in targets:
        pl.semaphore_signal(
            barrier, inc=1, device_id=target, device_id_type=pl.DeviceIdType.MESH
        )
    pl.semaphore_wait(barrier, len(targets))


def remote(src, dst, send, recv, target):
    return pltpu.make_async_remote_copy(
        src_ref=src,
        dst_ref=dst,
        send_sem=send,
        recv_sem=recv,
        device_id=target,
        device_id_type=pl.DeviceIdType.MESH,
    )


def remote_call(kernel, out_shape, operands, scratch, number, flops=1_000_000):
    multi = isinstance(out_shape, (tuple, list))
    vmem = pl.BlockSpec(memory_space=pltpu.VMEM)
    return pl.pallas_call(
        kernel,
        out_shape=out_shape,
        in_specs=[vmem] * len(operands),
        out_specs=[vmem] * len(out_shape) if multi else vmem,
        scratch_shapes=scratch,
        compiler_params=pltpu.CompilerParams(
            collective_id=number, has_side_effects=True, vmem_limit_bytes=56 * 1024 * 1024
        ),
    )(*operands)


def gather_sp_kernel(count, x_ref, y_ref, xs_ref, ys_ref, send, recv):
    me, tp = lax.axis_index("sp"), lax.axis_index("tp")
    targets = [peer(lax.rem(me + d, count), tp) for d in range(1, count)]
    greet(targets)
    copies = []
    for d in range(1, count):
        for i, (src, dst) in enumerate(((x_ref, xs_ref), (y_ref, ys_ref))):
            copies.append(
                remote(src, dst.at[me], send.at[i, d], recv.at[i, d], targets[d - 1])
            )
            copies[-1].start()
    xs_ref[me] = x_ref[...]
    ys_ref[me] = y_ref[...]
    for copy in copies:
        copy.wait()


def gather_sp(state, packet):
    count = lax.axis_size("sp")
    return remote_call(
        functools.partial(gather_sp_kernel, count),
        [
            jax.ShapeDtypeStruct((count,) + state.shape, state.dtype),
            jax.ShapeDtypeStruct((count,) + packet.shape, packet.dtype),
        ],
        [state, packet],
        [pltpu.SemaphoreType.DMA((2, count)), pltpu.SemaphoreType.DMA((2, count))],
        0,
    )


def swap_tp_kernel(count, x_ref, out_ref, send, recv):
    sp, me = lax.axis_index("sp"), lax.axis_index("tp")
    width = x_ref.shape[2]
    targets = [peer(sp, lax.rem(me + d, count)) for d in range(1, count)]
    greet(targets)
    columns = pl.ds(pl.multiple_of(me * width, width), width)
    copies = []
    for d in range(1, count):
        copies.append(
            remote(
                x_ref.at[lax.rem(me + d, count)],
                out_ref.at[:, columns],
                send.at[d],
                recv.at[d],
                targets[d - 1],
            )
        )
        copies[-1].start()
    out_ref[:, columns] = x_ref[me]
    for copy in copies:
        copy.wait()


def swap_tp(stacked):
    count = lax.axis_size("tp")
    return remote_call(
        functools.partial(swap_tp_kernel, count),
        jax.ShapeDtypeStruct((stacked.shape[1], count * stacked.shape[2]), stacked.dtype),
        [stacked],
        [pltpu.SemaphoreType.DMA((count,)), pltpu.SemaphoreType.DMA((count,))],
        1,
    )


class Place:
    def __init__(self, sp_size, tp_size):
        self.deep = math.gcd(sp_size, 4)
        self.rows = sp_size // self.deep
        self.tp_size = tp_size
        self.flat = self.rows * tp_size

    def here(self):
        sp, tp = lax.axis_index("sp"), lax.axis_index("tp")
        self.sp, self.tp = sp, tp
        self.a = sp // self.rows
        self.b = lax.rem(sp, self.rows)
        self.p = self.b * self.tp_size + tp
        return self

    def column(self, a):
        return peer(a * self.rows + self.b, self.tp)

    def plane(self, p):
        return peer(self.a * self.rows + p // self.tp_size, lax.rem(p, self.tp_size))

    def across(self, q):
        return lax.rem(self.p + q, self.flat)

    def nearest(self, i):
        last = self.deep - 1
        span = jnp.minimum(self.a, last - self.a)
        zigzag = self.a + ((i + 1) // 2 if i % 2 else -(i // 2))
        return jnp.where(i <= 2 * span, zigzag, jnp.where(self.a < last - self.a, i, last - i))


def tiles_of(width, most=512):
    step = math.gcd(width, most)
    return [slice(i, i + step) for i in range(0, width, step)]


def flatten_rows(block):
    groups, rows, width = block.shape
    if rows % 16 == 0:
        return block.reshape(groups * rows, width)
    return block.astype(jnp.float32).reshape(groups * rows, width).astype(jnp.bfloat16)


def experts_kernel(
    sizes, x_ref, middle_ref, select_ref, mix_ref, gate_ref, up_ref, down_ref,
    wide_gate, wide_up, wide_down, out_ref,
    column_ref, stage_ref, arrived_ref, made_ref, back_ref, sent_ref, came_ref, base_ref,
    hidden_ref, shared_ref, own_gate, own_up, own_down,
    weight_sem, zs, zr, ps, pr, bs, br, ss, sr,
):
    at = Place(*sizes).here()
    last = at.deep - 1
    flat, rows = stage_ref.shape[1], stage_ref.shape[2]
    width = x_ref.shape[1]
    experts = own_gate.shape[0]
    cap = rows // experts
    cuts = tiles_of(width)
    loads = [
        pltpu.make_async_copy(wide_gate, own_gate, weight_sem.at[0]),
        pltpu.make_async_copy(wide_up, own_up, weight_sem.at[1]),
        pltpu.make_async_copy(wide_down, own_down, weight_sem.at[2]),
    ]
    for load in loads:
        load.start()
    has_right, has_left = at.a < last, at.a > 0
    greet(
        [at.column(lax.rem(at.a + d, at.deep)) for d in range(1, at.deep)]
        + [at.plane(at.across(q)) for q in range(1, flat)]
    )

    def relay(source, owner, side):
        return remote(
            source,
            column_ref.at[owner],
            zs.at[side, owner],
            zr.at[owner],
            at.column(at.a + (1 if side == 0 else -1)),
        )

    def sends(owner):
        right = has_right & (owner <= at.a)
        left = has_left & (owner >= at.a)
        return right, left

    def forward(source, owner):
        right, left = sends(owner)
        pl.when(right)(lambda: relay(source, owner, 0).start())
        pl.when(left)(lambda: relay(source, owner, 1).start())

    def out_copy(owner, q):
        target = at.across(q)
        return remote(
            stage_ref.at[owner, target],
            arrived_ref.at[owner, at.p],
            ps.at[owner, q],
            pr.at[owner, q],
            at.plane(target),
        )

    def back_copy(owner, q, i):
        target = at.across(q)
        return remote(
            made_ref.at[owner, target, :, cuts[i]],
            back_ref.at[owner, at.p, :, cuts[i]],
            bs.at[owner, q, i],
            br.at[owner, q, i],
            at.plane(target),
        )

    def pass_on(owner, source):
        for cut in cuts:
            picked = jnp.dot(
                select_ref[owner], source[:, cut], preferred_element_type=jnp.float32
            )
            stage_ref[owner, :, :, cut] = picked.reshape(flat, rows, -1).astype(jnp.bfloat16)
        for q in range(1, flat):
            out_copy(owner, q).start()
        arrived_ref[owner, at.p] = stage_ref[owner, at.p]

    def send_back(owner, i):
        for q in range(1, flat):
            back_copy(owner, q, i).start()

    def run_experts(owner, hold=False):
        for q in range(1, flat):
            out_copy(owner, q).wait_recv()
        for e in range(experts):
            mine = slice(e * cap, (e + 1) * cap)
            block = flatten_rows(arrived_ref[owner, :, mine, :])
            for cut in tiles_of(own_gate.shape[2], 256):
                gate = jnp.dot(block, own_gate[e, :, cut], preferred_element_type=jnp.float32)
                up = jnp.dot(block, own_up[e, :, cut], preferred_element_type=jnp.float32)
                hidden_ref[e, :, cut] = (jax.nn.silu(gate) * up).astype(jnp.bfloat16)
        for i, cut in enumerate(cuts):
            for e in range(experts):
                mine = slice(e * cap, (e + 1) * cap)
                down = jnp.dot(
                    hidden_ref[e], own_down[e, :, cut], preferred_element_type=jnp.float32
                )
                made_ref[owner, :, mine, cut] = down.reshape(flat, cap, -1).astype(jnp.bfloat16)
            if not hold:
                send_back(owner, i)
        back_ref[owner, at.p] = made_ref[owner, at.p]

    def mixed(owner, i):
        for q in range(1, flat):
            back_copy(owner, q, i).wait_recv()
        block = flatten_rows(back_ref[owner, :, :, cuts[i]])
        return jnp.dot(mix_ref[owner], block, preferred_element_type=jnp.float32)

    def toward(owner, side, i):
        return remote(
            sent_ref.at[owner, :, cuts[i]],
            came_ref.at[side, owner, :, cuts[i]],
            ss.at[owner, i],
            sr.at[side, owner, i],
            at.column(at.a + (-1 if side == 0 else 1)),
        )

    def step(owner, side, more):
        for i, cut in enumerate(cuts):
            part = mixed(owner, i)
            if more:
                toward(owner, side, i).wait_recv()
                part = part + came_ref[side, owner, :, cut].astype(jnp.float32)
            sent_ref[owner, :, cut] = part.astype(jnp.bfloat16)
            toward(owner, side, i).start()

    def homeward(turn):
        for owner, side, far in ((last - turn, 0, has_right), (turn, 1, has_left)):
            goes = (owner < at.a) if side == 0 else (owner > at.a)
            pl.when(goes & far)(lambda owner=owner, side=side: step(owner, side, True))
            pl.when(goes & jnp.logical_not(far))(
                lambda owner=owner, side=side: step(owner, side, False)
            )

    def take(i):
        relay(x_ref, order[i], 0).wait_recv()
        forward(column_ref.at[order[i]], order[i])
        pass_on(order[i], column_ref.at[order[i]])

    order = [at.nearest(i) for i in range(at.deep)]
    forward(x_ref, at.a)
    pass_on(at.a, x_ref)
    for cut in tiles_of(gate_ref.shape[1], 256):
        gate = jnp.dot(x_ref[...], gate_ref[:, cut], preferred_element_type=jnp.float32)
        up = jnp.dot(x_ref[...], up_ref[:, cut], preferred_element_type=jnp.float32)
        shared_ref[:, cut] = (jax.nn.silu(gate) * up).astype(jnp.bfloat16)
    for cut in cuts:
        base_ref[:, cut] = middle_ref[:, cut].astype(jnp.float32) + jnp.dot(
            shared_ref[...], down_ref[:, cut], preferred_element_type=jnp.float32
        )
    for i in range(1, at.deep + 1):
        if i < at.deep:
            take(i)
        if i == 1:
            for load in loads:
                load.wait()
        if i == at.deep:
            for turn in range(1, at.deep - 2):
                homeward(turn)
        run_experts(order[i - 1], hold=i == 1)
    for i in range(len(cuts)):
        send_back(at.a, i)
    for turn in range(max(1, at.deep - 2), at.deep):
        homeward(turn)

    for side, far in ((0, has_right), (1, has_left)):

        @pl.when(far)
        def _(side=side):
            for i, cut in enumerate(cuts):
                toward(at.a, side, i).wait_recv()
                base_ref[:, cut] += came_ref[side, at.a, :, cut].astype(jnp.float32)

    for i, cut in enumerate(cuts):
        out_ref[:, cut] = (base_ref[:, cut] + mixed(at.a, i)).astype(out_ref.dtype)
    for i in range(at.deep):
        owner = order[i]
        right, left = sends(owner)
        pl.when(right)(lambda owner=owner: relay(x_ref, owner, 0).wait_send())
        pl.when(left)(lambda owner=owner: relay(x_ref, owner, 1).wait_send())
        for q in range(1, flat):
            out_copy(owner, q).wait_send()
            for j in range(len(cuts)):
                back_copy(owner, q, j).wait_send()
        if i > 0:
            for j in range(len(cuts)):
                toward(owner, 0, j).wait_send()


def experts_layer(normed, middle, select, mix, common, routed):
    sizes = (lax.axis_size("sp"), lax.axis_size("tp"))
    at = Place(*sizes)
    tokens, width = normed.shape
    slots = select.shape[1]
    box = (at.deep, at.flat, slots // at.flat, width)
    chunk = (at.deep, tokens, width)
    dma = pltpu.SemaphoreType.DMA
    half = jnp.bfloat16
    vmem = pl.BlockSpec(memory_space=pltpu.VMEM)
    far = pl.BlockSpec(memory_space=pl.ANY)
    experts = routed[0].shape[0]
    parts = len(tiles_of(width))
    return pl.pallas_call(
        functools.partial(experts_kernel, sizes),
        out_shape=jax.ShapeDtypeStruct((tokens, width), half),
        in_specs=[vmem] * 7 + [far] * 3,
        out_specs=vmem,
        scratch_shapes=[
            pltpu.VMEM(chunk, half),
            pltpu.VMEM(box, half),
            pltpu.VMEM(box, half),
            pltpu.VMEM(box, half),
            pltpu.VMEM(box, half),
            pltpu.VMEM(chunk, half),
            pltpu.VMEM((2,) + chunk, half),
            pltpu.VMEM((tokens, width), jnp.float32),
            pltpu.VMEM((experts, slots // experts, routed[0].shape[2]), half),
            pltpu.VMEM((tokens, common[0].shape[1]), half),
            pltpu.VMEM(routed[0].shape, half),
            pltpu.VMEM(routed[1].shape, half),
            pltpu.VMEM(routed[2].shape, half),
            dma((3,)),
            dma((2, at.deep)),
            dma((at.deep,)),
            dma((at.deep, at.flat)),
            dma((at.deep, at.flat)),
            dma((at.deep, at.flat, parts)),
            dma((at.deep, at.flat, parts)),
            dma((at.deep, parts)),
            dma((2, at.deep, parts)),
        ],
        compiler_params=pltpu.CompilerParams(
            collective_id=2, has_side_effects=True, vmem_limit_bytes=60 * 1024 * 1024
        ),
    )(normed, middle, select, mix, *common, *routed)


def on_device(
    queries,
    key_matrix,
    value_matrix,
    channel_decay_input,
    head_decay_offset,
    output_gate_input,
    head_norm_gain,
    residual,
    mixer_output_weight,
    expert_norm_gain,
    routes,
    chosen_router_scores,
    routed_gate_weight,
    routed_up_weight,
    routed_down_weight,
    common_gate_weight,
    common_up_weight,
    common_down_weight,
):
    device_heads = head_decay_offset.shape[1]
    seq_rows = queries.shape[0]
    blocks = seq_rows // BLOCK

    def split_local(values, columns):
        return (
            values.astype(jnp.float32)
            .reshape(blocks, BLOCK, device_heads, columns)
            .transpose(2, 0, 1, 3)
        )

    decay_spike_columns = jnp.repeat(head_decay_offset, KEY_CHANNELS, axis=1)
    decay_logarithm = (
        jax.nn.log_sigmoid(channel_decay_input.astype(jnp.float32)) / decay_running
        + decay_spike_columns
    )
    within = jnp.einsum(
        "ij,hnjd->hnid",
        jnp.tril(jnp.ones((BLOCK, BLOCK), jnp.float32)),
        split_local(decay_logarithm, KEY_CHANNELS),
        precision=lax.Precision.HIGHEST,
    )
    block_end = within[:, :, -1, :]
    q_heads = split_local(queries, KEY_CHANNELS) * KEY_CHANNELS ** (-0.5)
    k_heads = split_local(key_matrix, KEY_CHANNELS)
    v_heads = split_local(value_matrix, VDIM)
    q_decay = q_heads * jnp.exp(within)
    k_grow = k_heads * jnp.exp(-within)
    k_tail = k_heads * jnp.exp(block_end[:, :, None, :] - within)
    causal = jnp.tril(jnp.ones((BLOCK, BLOCK), dtype=bool))
    scores = jnp.where(causal, jnp.einsum("hnid,hnjd->hnij", q_decay, k_grow), 0.0)
    inside = jnp.einsum("hnij,hnje->hnie", scores, v_heads)
    block_state = jnp.einsum("hncd,hnce->hnde", k_tail, v_heads)
    inclusive = jnp.cumsum(block_end, axis=1)
    exclusive = inclusive - block_end
    before = jnp.arange(blocks)[:, None] > jnp.arange(blocks)[None, :]
    spread = jnp.exp(
        jnp.where(
            before[None, :, :, None], exclusive[:, :, None, :] - inclusive[:, None, :, :], -jnp.inf
        )
    )
    local_start = jnp.einsum("hnmd,hmde->hnde", spread, block_state)
    total_log = inclusive[:, -1, :]
    tail_weight = jnp.exp(total_log[:, None, :] - inclusive)
    device_state = jnp.einsum("hnd,hnde->hde", tail_weight, block_state)
    lanes = VDIM
    tok_count = residual.shape[0]
    sp_index = lax.axis_index("sp")
    sp_size = lax.axis_size("sp")
    state_rows = device_heads * KEY_CHANNELS
    parts = [
        total_log.reshape(-1, lanes),
        routes.T.astype(jnp.float32).reshape(-1, lanes),
        chosen_router_scores.T.reshape(-1, lanes),
    ]
    stops = [sum(part.shape[0] for part in parts[: i + 1]) for i in range(len(parts))]
    spare = -stops[-1] % 8
    packet = jnp.concatenate(parts + [jnp.zeros((spare, lanes), jnp.float32)], axis=0)
    state = device_state.reshape(state_rows, lanes).astype(jnp.bfloat16)
    states, gathered = gather_sp(state, packet)
    states = states.reshape(sp_size, device_heads, KEY_CHANNELS, VDIM).astype(jnp.float32)
    logs = gathered[:, : stops[0]].reshape(sp_size, device_heads, KEY_CHANNELS)
    ahead = (jnp.arange(sp_size) < sp_index)[:, None, None]
    logs = jnp.where(ahead, logs, 0.0)
    later = (jnp.arange(sp_size)[:, None] < jnp.arange(sp_size)[None, :])[:, :, None, None]
    after = jnp.sum(jnp.where(later, logs[None], 0.0), axis=1)
    reach = jnp.where(ahead, jnp.exp(after), 0.0)
    carried = jnp.sum(reach[..., None] * states, axis=0)
    entering = local_start + jnp.exp(exclusive)[..., None] * carried[:, None, :, :]
    output = inside + jnp.einsum("hncd,hnde->hnce", q_decay, entering)
    output = output.transpose(1, 2, 0, 3).reshape(seq_rows, device_heads, VDIM)
    inv_rms = lax.rsqrt(jnp.mean(output * output, axis=-1, keepdims=True) + eps_norm)
    normed_heads = (output * inv_rms * head_norm_gain).reshape(seq_rows, device_heads * VDIM)
    gated_output = (normed_heads * jax.nn.silu(output_gate_input.astype(jnp.float32))).astype(
        jnp.bfloat16
    )
    stacked = gated_output.reshape(lax.axis_size("tp"), tok_count, gated_output.shape[1])
    projected = jnp.dot(
        swap_tp(stacked), mixer_output_weight, preferred_element_type=jnp.float32
    )
    middle = (residual.astype(jnp.float32) + projected).astype(jnp.bfloat16)
    middle_wide = middle.astype(jnp.float32)
    norm_scale = lax.rsqrt(jnp.mean(middle_wide * middle_wide, axis=-1, keepdims=True) + eps_norm)
    normed = (middle_wide * norm_scale * expert_norm_gain).astype(jnp.bfloat16)
    devices = sp_size * lax.axis_size("tp")
    exp_dev = routed_gate_weight.shape[0]
    cap_slots = 2 * TOP_K * tok_count // (exp_dev * devices)
    at = Place(sp_size, lax.axis_size("tp")).here()
    column = lax.dynamic_index_in_dim(
        gathered.reshape(at.deep, at.rows, -1, lanes), at.b, 1, False
    )
    names = column[:, stops[0] : stops[1]].reshape(at.deep, TOP_K, 1, tok_count)
    scores_all = column[:, stops[1] : stops[2]].reshape(at.deep, TOP_K, 1, tok_count)
    weights = routed_scale * scores_all / jnp.sum(scores_all, axis=1, keepdims=True)
    plane_experts = at.flat * exp_dev
    expert = (at.a * plane_experts + jnp.arange(plane_experts)).astype(jnp.float32)
    hit = (names == expert[None, None, :, None]).astype(jnp.float32)
    chosen = jnp.sum(hit, axis=1)
    weight_of = jnp.sum(hit * weights, axis=1)
    sooner = jnp.triu(jnp.ones((tok_count, tok_count), jnp.bfloat16), 1)
    rank = jnp.einsum(
        "aeu,ut->aet",
        chosen.astype(jnp.bfloat16),
        sooner,
        preferred_element_type=jnp.float32,
    )
    slot = jnp.arange(cap_slots, dtype=jnp.float32)[None, None, :, None]
    taken = (rank[:, :, None, :] == slot) & (chosen[:, :, None, :] > 0.0)
    slots = plane_experts * cap_slots
    select = taken.astype(jnp.bfloat16).reshape(at.deep, slots, tok_count)
    mix = jnp.where(taken, weight_of[:, :, None, :], 0.0).astype(jnp.bfloat16)
    mix = mix.reshape(at.deep, slots, tok_count).transpose(0, 2, 1)
    return experts_layer(
        normed,
        middle,
        select,
        mix,
        (common_gate_weight, common_up_weight, common_down_weight),
        (routed_gate_weight, routed_up_weight, routed_down_weight),
    )


def solution(mesh):
    placed = (
        P("sp", "tp"),
        P("sp", "tp"),
        P("sp", "tp"),
        P("sp", "tp"),
        P("sp", "tp"),
        P("sp", "tp"),
        P(),
        P(("sp", "tp"), None),
        P(),
        P(),
        P(("sp", "tp"), None),
        P(("sp", "tp"), None),
        P(("sp", "tp"), None, None),
        P(("sp", "tp"), None, None),
        P(("sp", "tp"), None, None),
        P(),
        P(),
        P(),
    )
    return jax.shard_map(
        on_device, mesh=mesh, in_specs=placed, out_specs=P(("sp", "tp"), None), check_vma=False
    )
```

```python
import functools
import math

import jax
import jax.numpy as jnp
from jax import lax
from jax.experimental import pallas as pl
from jax.experimental.pallas import tpu as pltpu
from jax.sharding import PartitionSpec as P

D = 2048
KEY_CHANNELS = 64
VDIM = 128
BLOCK = 64
TOP_K = 4


eps_norm = 1e-06
decay_running = 16.0
routed_scale = 2.5


def peer(sp, tp):
    return {"sp": sp, "tp": tp}


def greet(targets):
    barrier = pltpu.get_barrier_semaphore()
    for target in targets:
        pl.semaphore_signal(
            barrier, inc=1, device_id=target, device_id_type=pl.DeviceIdType.MESH
        )
    pl.semaphore_wait(barrier, len(targets))


def remote(src, dst, send, recv, target):
    return pltpu.make_async_remote_copy(
        src_ref=src,
        dst_ref=dst,
        send_sem=send,
        recv_sem=recv,
        device_id=target,
        device_id_type=pl.DeviceIdType.MESH,
    )


def remote_call(kernel, out_shape, operands, scratch, number, flops=1_000_000):
    multi = isinstance(out_shape, (tuple, list))
    vmem = pl.BlockSpec(memory_space=pltpu.VMEM)
    return pl.pallas_call(
        kernel,
        out_shape=out_shape,
        in_specs=[vmem] * len(operands),
        out_specs=[vmem] * len(out_shape) if multi else vmem,
        scratch_shapes=scratch,
        compiler_params=pltpu.CompilerParams(
            collective_id=number, has_side_effects=True, vmem_limit_bytes=56 * 1024 * 1024
        ),
    )(*operands)


def gather_sp_kernel(count, x_ref, y_ref, xs_ref, ys_ref, send, recv):
    me, tp = lax.axis_index("sp"), lax.axis_index("tp")
    targets = [peer(lax.rem(me + d, count), tp) for d in range(1, count)]
    greet(targets)
    copies = []
    for d in range(1, count):
        for i, (src, dst) in enumerate(((x_ref, xs_ref), (y_ref, ys_ref))):
            copies.append(
                remote(src, dst.at[me], send.at[i, d], recv.at[i, d], targets[d - 1])
            )
            copies[-1].start()
    xs_ref[me] = x_ref[...]
    ys_ref[me] = y_ref[...]
    for copy in copies:
        copy.wait()


def gather_sp(state, packet):
    count = lax.axis_size("sp")
    return remote_call(
        functools.partial(gather_sp_kernel, count),
        [
            jax.ShapeDtypeStruct((count,) + state.shape, state.dtype),
            jax.ShapeDtypeStruct((count,) + packet.shape, packet.dtype),
        ],
        [state, packet],
        [pltpu.SemaphoreType.DMA((2, count)), pltpu.SemaphoreType.DMA((2, count))],
        0,
    )


def swap_tp_kernel(count, x_ref, out_ref, send, recv):
    sp, me = lax.axis_index("sp"), lax.axis_index("tp")
    width = x_ref.shape[2]
    targets = [peer(sp, lax.rem(me + d, count)) for d in range(1, count)]
    greet(targets)
    columns = pl.ds(pl.multiple_of(me * width, width), width)
    copies = []
    for d in range(1, count):
        copies.append(
            remote(
                x_ref.at[lax.rem(me + d, count)],
                out_ref.at[:, columns],
                send.at[d],
                recv.at[d],
                targets[d - 1],
            )
        )
        copies[-1].start()
    out_ref[:, columns] = x_ref[me]
    for copy in copies:
        copy.wait()


def swap_tp(stacked):
    count = lax.axis_size("tp")
    return remote_call(
        functools.partial(swap_tp_kernel, count),
        jax.ShapeDtypeStruct((stacked.shape[1], count * stacked.shape[2]), stacked.dtype),
        [stacked],
        [pltpu.SemaphoreType.DMA((count,)), pltpu.SemaphoreType.DMA((count,))],
        1,
    )


class Place:
    def __init__(self, sp_size, tp_size):
        self.deep = math.gcd(sp_size, 4)
        self.rows = sp_size // self.deep
        self.tp_size = tp_size
        self.flat = self.rows * tp_size

    def here(self):
        sp, tp = lax.axis_index("sp"), lax.axis_index("tp")
        self.sp, self.tp = sp, tp
        self.a = sp // self.rows
        self.b = lax.rem(sp, self.rows)
        self.p = self.b * self.tp_size + tp
        return self

    def column(self, a):
        return peer(a * self.rows + self.b, self.tp)

    def plane(self, p):
        return peer(self.a * self.rows + p // self.tp_size, lax.rem(p, self.tp_size))

    def across(self, q):
        return lax.rem(self.p + q, self.flat)

    def nearest(self, i):
        last = self.deep - 1
        span = jnp.minimum(self.a, last - self.a)
        zigzag = self.a + ((i + 1) // 2 if i % 2 else -(i // 2))
        return jnp.where(i <= 2 * span, zigzag, jnp.where(self.a < last - self.a, i, last - i))


def tiles_of(width, most=512):
    step = math.gcd(width, most)
    return [slice(i, i + step) for i in range(0, width, step)]


def flatten_rows(block):
    groups, rows, width = block.shape
    if rows % 16 == 0:
        return block.reshape(groups * rows, width)
    return block.astype(jnp.float32).reshape(groups * rows, width).astype(jnp.bfloat16)


def experts_kernel(
    sizes, x_ref, middle_ref, select_ref, mix_ref, far_gate, far_up, far_down,
    wide_gate, wide_up, wide_down, out_ref,
    column_ref, stage_ref, arrived_ref, made_ref, back_ref, sent_ref, came_ref, base_ref,
    hidden_ref, shared_ref, gate_ref, up_ref, down_ref, own_gate, own_up, own_down,
    weight_sem, zs, zr, ps, pr, bs, br, ss, sr,
):
    at = Place(*sizes).here()
    last = at.deep - 1
    flat, rows = stage_ref.shape[1], stage_ref.shape[2]
    width = x_ref.shape[1]
    experts = own_gate.shape[0]
    cap = rows // experts
    cuts = tiles_of(width)
    pairs = (
        (far_gate, gate_ref), (far_up, up_ref), (far_down, down_ref),
        (wide_gate, own_gate), (wide_up, own_up), (wide_down, own_down),
    )
    loads = [
        pltpu.make_async_copy(src, dst, weight_sem.at[i]) for i, (src, dst) in enumerate(pairs)
    ]
    for load in loads:
        load.start()
    has_right, has_left = at.a < last, at.a > 0
    greet(
        [at.column(lax.rem(at.a + d, at.deep)) for d in range(1, at.deep)]
        + [at.plane(at.across(q)) for q in range(1, flat)]
    )

    def relay(source, owner, side):
        return remote(
            source,
            column_ref.at[owner],
            zs.at[side, owner],
            zr.at[owner],
            at.column(at.a + (1 if side == 0 else -1)),
        )

    def sends(owner):
        right = has_right & (owner <= at.a)
        left = has_left & (owner >= at.a)
        return right, left

    def forward(source, owner):
        right, left = sends(owner)
        pl.when(right)(lambda: relay(source, owner, 0).start())
        pl.when(left)(lambda: relay(source, owner, 1).start())

    def out_copy(owner, q):
        target = at.across(q)
        return remote(
            stage_ref.at[owner, target],
            arrived_ref.at[owner, at.p],
            ps.at[owner, q],
            pr.at[owner, q],
            at.plane(target),
        )

    def back_copy(owner, q, i):
        target = at.across(q)
        return remote(
            made_ref.at[owner, target, :, cuts[i]],
            back_ref.at[owner, at.p, :, cuts[i]],
            bs.at[owner, q, i],
            br.at[owner, q, i],
            at.plane(target),
        )

    def pass_on(owner, source):
        for cut in cuts:
            picked = jnp.dot(
                select_ref[owner], source[:, cut], preferred_element_type=jnp.float32
            )
            stage_ref[owner, :, :, cut] = picked.reshape(flat, rows, -1).astype(jnp.bfloat16)
        for q in range(1, flat):
            out_copy(owner, q).start()
        arrived_ref[owner, at.p] = stage_ref[owner, at.p]

    def send_back(owner, i):
        for q in range(1, flat):
            back_copy(owner, q, i).start()

    def run_experts(owner, hold=False):
        for q in range(1, flat):
            out_copy(owner, q).wait_recv()
        for e in range(experts):
            mine = slice(e * cap, (e + 1) * cap)
            block = flatten_rows(arrived_ref[owner, :, mine, :])
            for cut in tiles_of(own_gate.shape[2], 256):
                gate = jnp.dot(block, own_gate[e, :, cut], preferred_element_type=jnp.float32)
                up = jnp.dot(block, own_up[e, :, cut], preferred_element_type=jnp.float32)
                hidden_ref[e, :, cut] = (jax.nn.silu(gate) * up).astype(jnp.bfloat16)
        for i, cut in enumerate(cuts):
            for e in range(experts):
                mine = slice(e * cap, (e + 1) * cap)
                down = jnp.dot(
                    hidden_ref[e], own_down[e, :, cut], preferred_element_type=jnp.float32
                )
                made_ref[owner, :, mine, cut] = down.reshape(flat, cap, -1).astype(jnp.bfloat16)
            if not hold:
                send_back(owner, i)
        back_ref[owner, at.p] = made_ref[owner, at.p]

    def mixed(owner, i):
        for q in range(1, flat):
            back_copy(owner, q, i).wait_recv()
        block = flatten_rows(back_ref[owner, :, :, cuts[i]])
        return jnp.dot(mix_ref[owner], block, preferred_element_type=jnp.float32)

    def toward(owner, side, i):
        return remote(
            sent_ref.at[owner, :, cuts[i]],
            came_ref.at[side, owner, :, cuts[i]],
            ss.at[owner, i],
            sr.at[side, owner, i],
            at.column(at.a - 1 + 2 * side),
        )

    def step(owner, side, more):
        for i, cut in enumerate(cuts):
            part = mixed(owner, i)
            if more:
                toward(owner, side, i).wait_recv()
                part = part + came_ref[side, owner, :, cut].astype(jnp.float32)
            sent_ref[owner, :, cut] = part.astype(jnp.bfloat16)
            toward(owner, side, i).start()

    def homeward(turn):
        for place in range(2):
            side = jnp.where(2 * at.a < at.deep, 1 - place, place)
            owner = jnp.where(side == 0, last - turn, turn)
            goes = jnp.where(side == 0, owner < at.a, owner > at.a)
            far = jnp.where(side == 0, has_right, has_left)
            pl.when(goes & far)(lambda owner=owner, side=side: step(owner, side, True))
            pl.when(goes & jnp.logical_not(far))(
                lambda owner=owner, side=side: step(owner, side, False)
            )

    def take(i):
        relay(x_ref, order[i], 0).wait_recv()
        forward(column_ref.at[order[i]], order[i])
        pass_on(order[i], column_ref.at[order[i]])

    order = [at.nearest(i) for i in range(at.deep)]
    forward(x_ref, at.a)
    pass_on(at.a, x_ref)
    for load in loads[:3]:
        load.wait()
    for cut in tiles_of(gate_ref.shape[1], 256):
        gate = jnp.dot(x_ref[...], gate_ref[:, cut], preferred_element_type=jnp.float32)
        up = jnp.dot(x_ref[...], up_ref[:, cut], preferred_element_type=jnp.float32)
        shared_ref[:, cut] = (jax.nn.silu(gate) * up).astype(jnp.bfloat16)
    for cut in cuts:
        base_ref[:, cut] = middle_ref[:, cut].astype(jnp.float32) + jnp.dot(
            shared_ref[...], down_ref[:, cut], preferred_element_type=jnp.float32
        )
    for i in range(1, at.deep + 1):
        if i < at.deep:
            take(i)
        if i == 1:
            for load in loads[3:]:
                load.wait()
        if i == at.deep:
            for turn in range(1, at.deep - 2):
                homeward(turn)
        run_experts(order[i - 1], hold=i == 1)
    for i in range(len(cuts)):
        send_back(at.a, i)
    for turn in range(max(1, at.deep - 2), at.deep):
        homeward(turn)

    for side, far in ((0, has_right), (1, has_left)):

        @pl.when(far)
        def _(side=side):
            for i, cut in enumerate(cuts):
                toward(at.a, side, i).wait_recv()
                base_ref[:, cut] += came_ref[side, at.a, :, cut].astype(jnp.float32)

    for i, cut in enumerate(cuts):
        out_ref[:, cut] = (base_ref[:, cut] + mixed(at.a, i)).astype(out_ref.dtype)
    for i in range(at.deep):
        owner = order[i]
        right, left = sends(owner)
        pl.when(right)(lambda owner=owner: relay(x_ref, owner, 0).wait_send())
        pl.when(left)(lambda owner=owner: relay(x_ref, owner, 1).wait_send())
        for q in range(1, flat):
            out_copy(owner, q).wait_send()
            for j in range(len(cuts)):
                back_copy(owner, q, j).wait_send()
        if i > 0:
            for j in range(len(cuts)):
                toward(owner, 0, j).wait_send()


def experts_layer(normed, middle, select, mix, common, routed):
    sizes = (lax.axis_size("sp"), lax.axis_size("tp"))
    at = Place(*sizes)
    tokens, width = normed.shape
    slots = select.shape[1]
    box = (at.deep, at.flat, slots // at.flat, width)
    chunk = (at.deep, tokens, width)
    dma = pltpu.SemaphoreType.DMA
    half = jnp.bfloat16
    vmem = pl.BlockSpec(memory_space=pltpu.VMEM)
    far = pl.BlockSpec(memory_space=pl.ANY)
    experts = routed[0].shape[0]
    parts = len(tiles_of(width))
    return pl.pallas_call(
        functools.partial(experts_kernel, sizes),
        out_shape=jax.ShapeDtypeStruct((tokens, width), half),
        in_specs=[vmem] * 4 + [far] * 6,
        out_specs=vmem,
        scratch_shapes=[
            pltpu.VMEM(chunk, half),
            pltpu.VMEM(box, half),
            pltpu.VMEM(box, half),
            pltpu.VMEM(box, half),
            pltpu.VMEM(box, half),
            pltpu.VMEM(chunk, half),
            pltpu.VMEM((2,) + chunk, half),
            pltpu.VMEM((tokens, width), jnp.float32),
            pltpu.VMEM((experts, slots // experts, routed[0].shape[2]), half),
            pltpu.VMEM((tokens, common[0].shape[1]), half),
            pltpu.VMEM(common[0].shape, half),
            pltpu.VMEM(common[1].shape, half),
            pltpu.VMEM(common[2].shape, half),
            pltpu.VMEM(routed[0].shape, half),
            pltpu.VMEM(routed[1].shape, half),
            pltpu.VMEM(routed[2].shape, half),
            dma((6,)),
            dma((2, at.deep)),
            dma((at.deep,)),
            dma((at.deep, at.flat)),
            dma((at.deep, at.flat)),
            dma((at.deep, at.flat, parts)),
            dma((at.deep, at.flat, parts)),
            dma((at.deep, parts)),
            dma((2, at.deep, parts)),
        ],
        compiler_params=pltpu.CompilerParams(
            collective_id=2, has_side_effects=True, vmem_limit_bytes=60 * 1024 * 1024
        ),
    )(normed, middle, select, mix, *common, *routed)


def on_device(
    queries,
    key_matrix,
    value_matrix,
    channel_decay_input,
    head_decay_offset,
    output_gate_input,
    head_norm_gain,
    residual,
    mixer_output_weight,
    expert_norm_gain,
    routes,
    chosen_router_scores,
    routed_gate_weight,
    routed_up_weight,
    routed_down_weight,
    common_gate_weight,
    common_up_weight,
    common_down_weight,
):
    device_heads = head_decay_offset.shape[1]
    seq_rows = queries.shape[0]
    blocks = seq_rows // BLOCK

    def split_local(values, columns):
        return (
            values.astype(jnp.float32)
            .reshape(blocks, BLOCK, device_heads, columns)
            .transpose(2, 0, 1, 3)
        )

    decay_spike_columns = jnp.repeat(head_decay_offset, KEY_CHANNELS, axis=1)
    decay_logarithm = (
        jax.nn.log_sigmoid(channel_decay_input.astype(jnp.float32)) / decay_running
        + decay_spike_columns
    )
    within = jnp.einsum(
        "ij,hnjd->hnid",
        jnp.tril(jnp.ones((BLOCK, BLOCK), jnp.float32)),
        split_local(decay_logarithm, KEY_CHANNELS),
        precision=lax.Precision.HIGHEST,
    )
    block_end = within[:, :, -1, :]
    q_heads = split_local(queries, KEY_CHANNELS) * KEY_CHANNELS ** (-0.5)
    k_heads = split_local(key_matrix, KEY_CHANNELS)
    v_heads = split_local(value_matrix, VDIM)
    q_decay = q_heads * jnp.exp(within)
    k_grow = k_heads * jnp.exp(-within)
    k_tail = k_heads * jnp.exp(block_end[:, :, None, :] - within)
    causal = jnp.tril(jnp.ones((BLOCK, BLOCK), dtype=bool))
    scores = jnp.where(causal, jnp.einsum("hnid,hnjd->hnij", q_decay, k_grow), 0.0)
    inside = jnp.einsum("hnij,hnje->hnie", scores, v_heads)
    block_state = jnp.einsum("hncd,hnce->hnde", k_tail, v_heads)
    inclusive = jnp.cumsum(block_end, axis=1)
    exclusive = inclusive - block_end
    before = jnp.arange(blocks)[:, None] > jnp.arange(blocks)[None, :]
    spread = jnp.exp(
        jnp.where(
            before[None, :, :, None], exclusive[:, :, None, :] - inclusive[:, None, :, :], -jnp.inf
        )
    )
    local_start = jnp.einsum("hnmd,hmde->hnde", spread, block_state)
    total_log = inclusive[:, -1, :]
    tail_weight = jnp.exp(total_log[:, None, :] - inclusive)
    device_state = jnp.einsum("hnd,hnde->hde", tail_weight, block_state)
    lanes = VDIM
    tok_count = residual.shape[0]
    sp_index = lax.axis_index("sp")
    sp_size = lax.axis_size("sp")
    state_rows = device_heads * KEY_CHANNELS
    parts = [
        total_log.reshape(-1, lanes),
        routes.T.astype(jnp.float32).reshape(-1, lanes),
        chosen_router_scores.T.reshape(-1, lanes),
    ]
    stops = [sum(part.shape[0] for part in parts[: i + 1]) for i in range(len(parts))]
    spare = -stops[-1] % 8
    packet = jnp.concatenate(parts + [jnp.zeros((spare, lanes), jnp.float32)], axis=0)
    state = device_state.reshape(state_rows, lanes).astype(jnp.bfloat16)
    states, gathered = gather_sp(state, packet)
    states = states.reshape(sp_size, device_heads, KEY_CHANNELS, VDIM).astype(jnp.float32)
    logs = gathered[:, : stops[0]].reshape(sp_size, device_heads, KEY_CHANNELS)
    ahead = (jnp.arange(sp_size) < sp_index)[:, None, None]
    logs = jnp.where(ahead, logs, 0.0)
    later = (jnp.arange(sp_size)[:, None] < jnp.arange(sp_size)[None, :])[:, :, None, None]
    after = jnp.sum(jnp.where(later, logs[None], 0.0), axis=1)
    reach = jnp.where(ahead, jnp.exp(after), 0.0)
    carried = jnp.sum(reach[..., None] * states, axis=0)
    entering = local_start + jnp.exp(exclusive)[..., None] * carried[:, None, :, :]
    output = inside + jnp.einsum("hncd,hnde->hnce", q_decay, entering)
    output = output.transpose(1, 2, 0, 3).reshape(seq_rows, device_heads, VDIM)
    inv_rms = lax.rsqrt(jnp.mean(output * output, axis=-1, keepdims=True) + eps_norm)
    normed_heads = (output * inv_rms * head_norm_gain).reshape(seq_rows, device_heads * VDIM)
    gated_output = (normed_heads * jax.nn.silu(output_gate_input.astype(jnp.float32))).astype(
        jnp.bfloat16
    )
    stacked = gated_output.reshape(lax.axis_size("tp"), tok_count, gated_output.shape[1])
    projected = jnp.dot(
        swap_tp(stacked), mixer_output_weight, preferred_element_type=jnp.float32
    )
    middle = (residual.astype(jnp.float32) + projected).astype(jnp.bfloat16)
    middle_wide = middle.astype(jnp.float32)
    norm_scale = lax.rsqrt(jnp.mean(middle_wide * middle_wide, axis=-1, keepdims=True) + eps_norm)
    normed = (middle_wide * norm_scale * expert_norm_gain).astype(jnp.bfloat16)
    devices = sp_size * lax.axis_size("tp")
    exp_dev = routed_gate_weight.shape[0]
    cap_slots = 2 * TOP_K * tok_count // (exp_dev * devices)
    at = Place(sp_size, lax.axis_size("tp")).here()
    column = lax.dynamic_index_in_dim(
        gathered.reshape(at.deep, at.rows, -1, lanes), at.b, 1, False
    )
    names = column[:, stops[0] : stops[1]].reshape(at.deep, TOP_K, 1, tok_count)
    scores_all = column[:, stops[1] : stops[2]].reshape(at.deep, TOP_K, 1, tok_count)
    weights = routed_scale * scores_all / jnp.sum(scores_all, axis=1, keepdims=True)
    plane_experts = at.flat * exp_dev
    expert = (at.a * plane_experts + jnp.arange(plane_experts)).astype(jnp.float32)
    hit = (names == expert[None, None, :, None]).astype(jnp.float32)
    chosen = jnp.sum(hit, axis=1)
    weight_of = jnp.sum(hit * weights, axis=1)
    sooner = jnp.triu(jnp.ones((tok_count, tok_count), jnp.bfloat16), 1)
    rank = jnp.einsum(
        "aeu,ut->aet",
        chosen.astype(jnp.bfloat16),
        sooner,
        preferred_element_type=jnp.float32,
    )
    slot = jnp.arange(cap_slots, dtype=jnp.float32)[None, None, :, None]
    taken = (rank[:, :, None, :] == slot) & (chosen[:, :, None, :] > 0.0)
    slots = plane_experts * cap_slots
    select = taken.astype(jnp.bfloat16).reshape(at.deep, slots, tok_count)
    mix = jnp.where(taken, weight_of[:, :, None, :], 0.0).astype(jnp.bfloat16)
    mix = mix.reshape(at.deep, slots, tok_count).transpose(0, 2, 1)
    return experts_layer(
        normed,
        middle,
        select,
        mix,
        (common_gate_weight, common_up_weight, common_down_weight),
        (routed_gate_weight, routed_up_weight, routed_down_weight),
    )


def solution(mesh):
    placed = (
        P("sp", "tp"),
        P("sp", "tp"),
        P("sp", "tp"),
        P("sp", "tp"),
        P("sp", "tp"),
        P("sp", "tp"),
        P(),
        P(("sp", "tp"), None),
        P(),
        P(),
        P(("sp", "tp"), None),
        P(("sp", "tp"), None),
        P(("sp", "tp"), None, None),
        P(("sp", "tp"), None, None),
        P(("sp", "tp"), None, None),
        P(),
        P(),
        P(),
    )
    return jax.shard_map(
        on_device, mesh=mesh, in_specs=placed, out_specs=P(("sp", "tp"), None), check_vma=False
    )
```

```python
import functools
import math

import jax
import jax.numpy as jnp
from jax import lax
from jax.experimental import pallas as pl
from jax.experimental.pallas import tpu as pltpu
from jax.sharding import PartitionSpec as P

D = 2048
KEY_CHANNELS = 64
VDIM = 128
BLOCK = 64
TOP_K = 4


eps_norm = 1e-06
decay_running = 16.0
routed_scale = 2.5


def peer(sp, tp):
    return {"sp": sp, "tp": tp}


def call_on(targets):
    barrier = pltpu.get_barrier_semaphore()
    for target in targets:
        pl.semaphore_signal(
            barrier, inc=1, device_id=target, device_id_type=pl.DeviceIdType.MESH
        )
    return lambda: pl.semaphore_wait(barrier, len(targets))


def remote(src, dst, send, recv, target):
    return pltpu.make_async_remote_copy(
        src_ref=src,
        dst_ref=dst,
        send_sem=send,
        recv_sem=recv,
        device_id=target,
        device_id_type=pl.DeviceIdType.MESH,
    )


def dot_nt(a, b):
    return lax.dot_general(a, b, (((1,), (1,)), ((), ())), preferred_element_type=jnp.float32)


def dot_tn(a, b):
    return lax.dot_general(a, b, (((0,), (0,)), ((), ())), preferred_element_type=jnp.float32)


def exact_dot(ones, values):
    total = jnp.zeros((ones.shape[0], values.shape[1]), jnp.float32)
    for _ in range(3):
        part = values.astype(jnp.bfloat16)
        values = values - part.astype(jnp.float32)
        total = total + jnp.dot(ones, part, preferred_element_type=jnp.float32)
    return total


class Place:
    def __init__(self, sp_size, tp_size):
        self.deep = math.gcd(sp_size, 4)
        self.rows = sp_size // self.deep
        self.tp_size = tp_size
        self.flat = self.rows * tp_size

    def here(self):
        sp, tp = lax.axis_index("sp"), lax.axis_index("tp")
        self.sp, self.tp = sp, tp
        self.a = sp // self.rows
        self.b = lax.rem(sp, self.rows)
        self.p = self.b * self.tp_size + tp
        return self

    def column(self, a):
        return peer(a * self.rows + self.b, self.tp)

    def plane(self, p):
        return peer(self.a * self.rows + p // self.tp_size, lax.rem(p, self.tp_size))

    def across(self, q):
        return lax.rem(self.p + q, self.flat)

    def nearest(self, i):
        last = self.deep - 1
        span = jnp.minimum(self.a, last - self.a)
        zigzag = self.a + ((i + 1) // 2 if i % 2 else -(i // 2))
        return jnp.where(i <= 2 * span, zigzag, jnp.where(self.a < last - self.a, i, last - i))


def tiles_of(width, most=512):
    step = math.gcd(width, most)
    return [slice(i, i + step) for i in range(0, width, step)]


def flatten_rows(block):
    groups, rows, width = block.shape
    if rows % 16 == 0:
        return block.reshape(groups * rows, width)
    return block.astype(jnp.float32).reshape(groups * rows, width).astype(jnp.bfloat16)


def layer_kernel(
    sizes, q_ref, k_ref, v_ref, decay_ref, offset_ref, open_ref, head_gain_ref, residual_ref,
    gain_ref, packet_ref, far_mix, far_gate, far_up, far_down,
    wide_gate, wide_up, wide_down, out_ref,
    qd_ref, qx_ref, kg_ref, kt_ref, ends_ref, starts_ref, inner_ref, state_ref, log_ref,
    states_ref, logs_ref, carried_ref, reach_ref, packets_ref, gated_ref, swapped_ref,
    mixer_ref, x_ref, middle_ref, select_ref, mix_ref,
    column_ref, stage_ref, arrived_ref, made_ref, back_ref, sent_ref, came_ref, base_ref,
    hidden_ref, shared_ref, gate_ref, up_ref, down_ref, own_gate, own_up, own_down,
    weight_sem, ks, kr, gs, gr, ls, lr, ws, wr, zs, zr, ps, pr, bs, br, ss, sr,
):
    at = Place(*sizes).here()
    last = at.deep - 1
    flat, rows = stage_ref.shape[1], stage_ref.shape[2]
    width = x_ref.shape[1]
    experts = own_gate.shape[0]
    cap = rows // experts
    cuts = tiles_of(width)
    pairs = (
        (far_mix, mixer_ref), (far_gate, gate_ref), (far_up, up_ref), (far_down, down_ref),
        (wide_gate, own_gate), (wide_up, own_up), (wide_down, own_down),
    )
    loads = [
        pltpu.make_async_copy(src, dst, weight_sem.at[i]) for i, (src, dst) in enumerate(pairs)
    ]
    for load in loads:
        load.start()
    has_right, has_left = at.a < last, at.a > 0
    count, tps = sizes
    met = call_on(
        [peer(lax.rem(at.sp + d, count), at.tp) for d in range(1, count)]
        + [at.plane(at.across(q)) for q in range(1, flat)]
    )
    half, wide = jnp.bfloat16, jnp.float32
    length, lanes = q_ref.shape
    heads = offset_ref.shape[1]
    blocks = length // BLOCK
    tokens = x_ref.shape[0]
    lane = lax.broadcasted_iota(jnp.int32, (1, lanes), 1)
    of_head = [
        (lane >= h * KEY_CHANNELS) & (lane < (h + 1) * KEY_CHANNELS) for h in range(heads)
    ]
    columns = [slice(h * VDIM, (h + 1) * VDIM) for h in range(heads)]
    tile = math.gcd(length, 4 * BLOCK)
    row = lax.broadcasted_iota(jnp.int32, (tile, tile), 0)
    col = lax.broadcasted_iota(jnp.int32, (tile, tile), 1)
    causal = (jnp.bitwise_and(row, -BLOCK) == jnp.bitwise_and(col, -BLOCK)) & (col <= row)
    ones = jnp.where(causal, 1.0, 0.0).astype(half)

    for t in range(0, length, tile):
        span = slice(t, t + tile)
        pre = decay_ref[span, :].astype(wide)
        offset = jnp.zeros((tile, lanes), wide)
        for h in range(heads):
            offset = jnp.where(of_head[h], offset_ref[span, h : h + 1], offset)
        log_decay = (
            jnp.minimum(pre, 0.0) - jnp.log1p(jnp.exp(-jnp.abs(pre)))
        ) / decay_running + offset
        within = exact_dot(ones, log_decay)
        keys = k_ref[span, :].astype(wide)
        qd_ref[span, :] = q_ref[span, :].astype(wide) * KEY_CHANNELS ** (-0.5) * jnp.exp(within)
        grown = keys * jnp.exp(-within)
        for h in range(heads):
            kg_ref[h, span, :] = jnp.where(of_head[h], grown, 0.0).astype(half)
        for n in range(0, tile, BLOCK):
            inside = slice(n, n + BLOCK)
            end = within[n + BLOCK - 1 : n + BLOCK, :]
            kt_ref[t + n : t + n + BLOCK, :] = (
                keys[inside, :] * jnp.exp(end - within[inside, :])
            ).astype(half)
            ends_ref[(t + n) // BLOCK : (t + n) // BLOCK + 1, :] = end
    state = jnp.zeros((VDIM, lanes), wide)
    passed = jnp.zeros((1, lanes), wide)
    for n in range(blocks):
        span = slice(n * BLOCK, (n + 1) * BLOCK)
        starts_ref[n] = state.astype(half)
        end = ends_ref[n : n + 1, :]
        both = dot_tn(v_ref[span, :], kt_ref[span, :])
        added = both[columns[0], :]
        for h in range(1, heads):
            added = jnp.where(of_head[h], both[columns[h], :], added)
        moved = qd_ref[span, :] * jnp.exp(passed)
        for h in range(heads):
            qx_ref[h, span, :] = jnp.where(of_head[h], moved, 0.0).astype(half)
        state = state * jnp.exp(end) + added
        passed = passed + end
    state_ref[...] = state.astype(half)
    log_ref[...] = jnp.broadcast_to(passed, log_ref.shape)
    met()

    def packet_copy(d):
        return remote(
            packet_ref,
            packets_ref.at[at.a],
            ks.at[d],
            kr.at[at.a],
            at.column(lax.rem(at.a + d, at.deep)),
        )

    def packet_from(a):
        return remote(packet_ref, packets_ref.at[a], ks.at[0], kr.at[a], at.column(at.a))

    def state_copy(d):
        target = peer(jnp.minimum(at.sp + d, count - 1), at.tp)
        return (
            remote(state_ref, states_ref.at[at.sp], gs.at[d], gr.at[at.sp], target),
            remote(log_ref, logs_ref.at[at.sp], ls.at[d], lr.at[at.sp], target),
        )

    def swap_copy(d):
        to = lax.rem(at.tp + d, tps)
        return remote(
            gated_ref.at[to], swapped_ref.at[at.tp], ws.at[d], wr.at[at.tp], peer(at.sp, to)
        )

    for d in range(1, at.deep):
        packet_copy(d).start()
    for d in range(1, count):

        @pl.when(at.sp + d < count)
        def _(d=d):
            for copy in state_copy(d):
                copy.start()

    packets_ref[at.a] = packet_ref[...]
    for t in range(0, length, tile):
        span = slice(t, t + tile)
        ahead = qd_ref[span, :].astype(half)
        for h in range(heads):
            scores = jnp.where(causal, dot_nt(ahead, kg_ref[h, span, :]), 0.0)
            inner_ref[span, columns[h]] = jnp.dot(
                scores.astype(half), v_ref[span, columns[h]], preferred_element_type=wide
            )
    for n in range(1, blocks):
        span = slice(n * BLOCK, (n + 1) * BLOCK)
        for h in range(heads):
            ahead = jnp.where(of_head[h], qd_ref[span, :], 0.0).astype(half)
            inner_ref[span, columns[h]] += dot_nt(ahead, starts_ref[n])

    slots = flat * rows
    plane_experts = flat * experts
    here = lax.broadcasted_iota(jnp.int32, (slots, plane_experts), 0)
    there = lax.broadcasted_iota(jnp.int32, (slots, plane_experts), 1) * cap
    belongs = (here >= there) & (here < there + cap)
    spread = jnp.where(belongs, 1.0, 0.0).astype(half)
    place = jnp.sum(
        jnp.where(belongs, (here - there).astype(wide), 0.0), axis=1, keepdims=True
    )
    expert = (
        at.a * plane_experts + lax.broadcasted_iota(jnp.int32, (plane_experts, 1), 0)
    ).astype(wide)
    sooner = jnp.where(
        lax.broadcasted_iota(jnp.int32, (tokens, tokens), 0)
        < lax.broadcasted_iota(jnp.int32, (tokens, tokens), 1),
        1.0,
        0.0,
    ).astype(half)
    for a in range(at.deep):
        pl.when(at.a != a)(lambda a=a: packet_from(a).wait_recv())
        scored = packets_ref[a, TOP_K:, :]
        share = routed_scale * scored / jnp.sum(scored, axis=0, keepdims=True)
        chosen = jnp.zeros((plane_experts, tokens), wide)
        weight_of = jnp.zeros((plane_experts, tokens), wide)
        for k in range(TOP_K):
            hit = packets_ref[a, k : k + 1, :] == expert
            chosen = jnp.where(hit, 1.0, chosen)
            weight_of = jnp.where(hit, share[k : k + 1, :], weight_of)
        rank = jnp.dot(chosen.astype(half), sooner, preferred_element_type=wide)
        rank = jnp.where(chosen > 0.0, rank, -1.0)
        ranks = jnp.dot(spread, rank.astype(half), preferred_element_type=wide)
        weights = jnp.dot(spread, weight_of.astype(half), preferred_element_type=wide)
        taken = ranks == place
        select_ref[a] = jnp.where(taken, 1.0, 0.0).astype(half)
        mix_ref[a] = jnp.transpose(jnp.where(taken, weights, 0.0)).astype(half)

    carried_ref[...] = jnp.zeros_like(carried_ref)
    reach_ref[...] = jnp.zeros_like(reach_ref)
    for j in reversed(range(count - 1)):

        @pl.when(j < at.sp)
        def _(j=j):
            source = peer(j, at.tp)
            remote(state_ref, states_ref.at[j], gs.at[0], gr.at[j], source).wait_recv()
            remote(log_ref, logs_ref.at[j], ls.at[0], lr.at[j], source).wait_recv()
            carried_ref[...] += jnp.exp(reach_ref[0:1, :]) * states_ref[j].astype(wide)
            reach_ref[...] += logs_ref[j]

    carried = carried_ref[...].astype(half)
    for d in [*range(1, tps), 0]:
        to = lax.rem(at.tp + d, tps)
        span = pl.ds(pl.multiple_of(to * tokens, tokens), tokens)
        for h in range(heads):
            output = inner_ref[span, columns[h]] + dot_nt(qx_ref[h, span, :], carried)
            inv_rms = lax.rsqrt(jnp.mean(output * output, axis=-1, keepdims=True) + eps_norm)
            gated_ref[to, :, columns[h]] = (
                output
                * inv_rms
                * head_gain_ref[...]
                * jax.nn.silu(open_ref[span, columns[h]].astype(wide))
            ).astype(half)
        if d > 0:
            swap_copy(d).start()
    loads[0].wait()
    span = heads * VDIM
    for d in range(tps):
        source = lax.rem(at.tp - d + tps, tps)
        if d > 0:
            remote(
                gated_ref.at[0], swapped_ref.at[source], ws.at[0], wr.at[source], peer(at.sp, source)
            ).wait_recv()
        piece = gated_ref[source] if d == 0 else swapped_ref[source]
        part_of = pl.ds(pl.multiple_of(source * span, span), span)
        for cut in cuts:
            part = jnp.dot(piece, mixer_ref[part_of, cut], preferred_element_type=wide)
            if d == 0:
                base_ref[:, cut] = residual_ref[:, cut].astype(wide) + part
            else:
                base_ref[:, cut] += part
    square = jnp.zeros((tokens, 1), wide)
    for cut in cuts:
        middle_ref[:, cut] = base_ref[:, cut].astype(half)
        middle = middle_ref[:, cut].astype(wide)
        square = square + jnp.sum(middle * middle, axis=-1, keepdims=True)
    scale = lax.rsqrt(square / width + eps_norm)
    for cut in cuts:
        x_ref[:, cut] = (middle_ref[:, cut].astype(wide) * scale * gain_ref[:, cut]).astype(half)

    def relay(source, owner, side):
        return remote(
            source,
            column_ref.at[owner],
            zs.at[side, owner],
            zr.at[owner],
            at.column(at.a + (1 if side == 0 else -1)),
        )

    def sends(owner):
        right = has_right & (owner <= at.a)
        left = has_left & (owner >= at.a)
        return right, left

    def forward(source, owner):
        right, left = sends(owner)
        pl.when(right)(lambda: relay(source, owner, 0).start())
        pl.when(left)(lambda: relay(source, owner, 1).start())

    def out_copy(owner, q):
        target = at.across(q)
        return remote(
            stage_ref.at[owner, target],
            arrived_ref.at[owner, at.p],
            ps.at[owner, q],
            pr.at[owner, q],
            at.plane(target),
        )

    def back_copy(owner, q, i):
        target = at.across(q)
        return remote(
            made_ref.at[owner, target, :, cuts[i]],
            back_ref.at[owner, at.p, :, cuts[i]],
            bs.at[owner, q, i],
            br.at[owner, q, i],
            at.plane(target),
        )

    def pass_on(owner, source):
        for cut in cuts:
            picked = jnp.dot(
                select_ref[owner], source[:, cut], preferred_element_type=jnp.float32
            )
            stage_ref[owner, :, :, cut] = picked.reshape(flat, rows, -1).astype(jnp.bfloat16)
        for q in range(1, flat):
            out_copy(owner, q).start()
        arrived_ref[owner, at.p] = stage_ref[owner, at.p]

    def send_back(owner, i):
        for q in range(1, flat):
            back_copy(owner, q, i).start()

    def run_experts(owner, hold=False):
        for q in range(1, flat):
            out_copy(owner, q).wait_recv()
        for e in range(experts):
            mine = slice(e * cap, (e + 1) * cap)
            block = flatten_rows(arrived_ref[owner, :, mine, :])
            for cut in tiles_of(own_gate.shape[2], 256):
                gate = jnp.dot(block, own_gate[e, :, cut], preferred_element_type=jnp.float32)
                up = jnp.dot(block, own_up[e, :, cut], preferred_element_type=jnp.float32)
                hidden_ref[e, :, cut] = (jax.nn.silu(gate) * up).astype(jnp.bfloat16)
        for i, cut in enumerate(cuts):
            for e in range(experts):
                mine = slice(e * cap, (e + 1) * cap)
                down = jnp.dot(
                    hidden_ref[e], own_down[e, :, cut], preferred_element_type=jnp.float32
                )
                made_ref[owner, :, mine, cut] = down.reshape(flat, cap, -1).astype(jnp.bfloat16)
            if not hold:
                send_back(owner, i)
        back_ref[owner, at.p] = made_ref[owner, at.p]

    def mixed(owner, i):
        for q in range(1, flat):
            back_copy(owner, q, i).wait_recv()
        block = flatten_rows(back_ref[owner, :, :, cuts[i]])
        return jnp.dot(mix_ref[owner], block, preferred_element_type=jnp.float32)

    def toward(owner, side, i):
        return remote(
            sent_ref.at[owner, :, cuts[i]],
            came_ref.at[side, owner, :, cuts[i]],
            ss.at[owner, i],
            sr.at[side, owner, i],
            at.column(at.a - 1 + 2 * side),
        )

    def step(owner, side, more):
        for i, cut in enumerate(cuts):
            part = mixed(owner, i)
            if more:
                toward(owner, side, i).wait_recv()
                part = part + came_ref[side, owner, :, cut].astype(jnp.float32)
            sent_ref[owner, :, cut] = part.astype(jnp.bfloat16)
            toward(owner, side, i).start()

    def homeward(turn):
        for place in range(2):
            side = jnp.where(2 * at.a < at.deep, 1 - place, place)
            owner = jnp.where(side == 0, last - turn, turn)
            goes = jnp.where(side == 0, owner < at.a, owner > at.a)
            far = jnp.where(side == 0, has_right, has_left)
            pl.when(goes & far)(lambda owner=owner, side=side: step(owner, side, True))
            pl.when(goes & jnp.logical_not(far))(
                lambda owner=owner, side=side: step(owner, side, False)
            )

    def take(i):
        relay(x_ref, order[i], 0).wait_recv()
        forward(column_ref.at[order[i]], order[i])
        pass_on(order[i], column_ref.at[order[i]])

    order = [at.nearest(i) for i in range(at.deep)]
    forward(x_ref, at.a)
    pass_on(at.a, x_ref)
    for load in loads[1:4]:
        load.wait()
    for cut in tiles_of(gate_ref.shape[1], 256):
        gate = jnp.dot(x_ref[...], gate_ref[:, cut], preferred_element_type=jnp.float32)
        up = jnp.dot(x_ref[...], up_ref[:, cut], preferred_element_type=jnp.float32)
        shared_ref[:, cut] = (jax.nn.silu(gate) * up).astype(jnp.bfloat16)
    for cut in cuts:
        base_ref[:, cut] = middle_ref[:, cut].astype(jnp.float32) + jnp.dot(
            shared_ref[...], down_ref[:, cut], preferred_element_type=jnp.float32
        )
    for i in range(1, at.deep + 1):
        if i < at.deep:
            take(i)
        if i == 1:
            for load in loads[4:]:
                load.wait()
        if i == at.deep:
            for turn in range(1, at.deep - 2):
                homeward(turn)
        run_experts(order[i - 1], hold=i == 1)
    for i in range(len(cuts)):
        send_back(at.a, i)
    for turn in range(max(1, at.deep - 2), at.deep):
        homeward(turn)

    for side, far in ((0, has_right), (1, has_left)):

        @pl.when(far)
        def _(side=side):
            for i, cut in enumerate(cuts):
                toward(at.a, side, i).wait_recv()
                base_ref[:, cut] += came_ref[side, at.a, :, cut].astype(jnp.float32)

    for i, cut in enumerate(cuts):
        out_ref[:, cut] = (base_ref[:, cut] + mixed(at.a, i)).astype(out_ref.dtype)
    for d in range(1, at.deep):
        packet_copy(d).wait_send()
    for d in range(1, count):

        @pl.when(at.sp + d < count)
        def _(d=d):
            for copy in state_copy(d):
                copy.wait_send()

    for d in range(1, tps):
        swap_copy(d).wait_send()
    for i in range(at.deep):
        owner = order[i]
        right, left = sends(owner)
        pl.when(right)(lambda owner=owner: relay(x_ref, owner, 0).wait_send())
        pl.when(left)(lambda owner=owner: relay(x_ref, owner, 1).wait_send())
        for q in range(1, flat):
            out_copy(owner, q).wait_send()
            for j in range(len(cuts)):
                back_copy(owner, q, j).wait_send()
        if i > 0:
            for j in range(len(cuts)):
                toward(owner, 0, j).wait_send()


def on_device(
    queries,
    key_matrix,
    value_matrix,
    channel_decay_input,
    head_decay_offset,
    output_gate_input,
    head_norm_gain,
    residual,
    mixer_output_weight,
    expert_norm_gain,
    routes,
    chosen_router_scores,
    routed_gate_weight,
    routed_up_weight,
    routed_down_weight,
    common_gate_weight,
    common_up_weight,
    common_down_weight,
):
    count, tps = sizes = (lax.axis_size("sp"), lax.axis_size("tp"))
    at = Place(*sizes)
    tokens, width = residual.shape
    length, lanes = queries.shape
    heads = head_decay_offset.shape[1]
    blocks = length // BLOCK
    experts = routed_gate_weight.shape[0]
    cap = 2 * TOP_K * tokens // (experts * count * tps)
    rows = experts * cap
    slots = at.flat * rows
    parts = len(tiles_of(width))
    packet = jnp.concatenate(
        [routes.T.astype(jnp.float32), chosen_router_scores.T], axis=0
    )
    common = (common_gate_weight, common_up_weight, common_down_weight)
    routed = (routed_gate_weight, routed_up_weight, routed_down_weight)
    box = (at.deep, at.flat, rows, width)
    chunk = (at.deep, tokens, width)
    dma = pltpu.SemaphoreType.DMA
    half, wide = jnp.bfloat16, jnp.float32
    vmem = pl.BlockSpec(memory_space=pltpu.VMEM)
    far = pl.BlockSpec(memory_space=pl.ANY)
    return pl.pallas_call(
        functools.partial(layer_kernel, sizes),
        out_shape=jax.ShapeDtypeStruct((tokens, width), half),
        in_specs=[vmem] * 10 + [far] * 7,
        out_specs=vmem,
        scratch_shapes=[
            pltpu.VMEM((length, lanes), wide),
            pltpu.VMEM((heads, length, lanes), half),
            pltpu.VMEM((heads, length, lanes), half),
            pltpu.VMEM((length, lanes), half),
            pltpu.VMEM((max(8, blocks), lanes), wide),
            pltpu.VMEM((blocks, VDIM, lanes), half),
            pltpu.VMEM((length, heads * VDIM), wide),
            pltpu.VMEM((VDIM, lanes), half),
            pltpu.VMEM((8, lanes), wide),
            pltpu.VMEM((count, VDIM, lanes), half),
            pltpu.VMEM((count, 8, lanes), wide),
            pltpu.VMEM((VDIM, lanes), wide),
            pltpu.VMEM((8, lanes), wide),
            pltpu.VMEM((at.deep,) + packet.shape, wide),
            pltpu.VMEM((tps, tokens, heads * VDIM), half),
            pltpu.VMEM((tps, tokens, heads * VDIM), half),
            pltpu.VMEM(mixer_output_weight.shape, half),
            pltpu.VMEM((tokens, width), half),
            pltpu.VMEM((tokens, width), half),
            pltpu.VMEM((at.deep, slots, tokens), half),
            pltpu.VMEM((at.deep, tokens, slots), half),
            pltpu.VMEM(chunk, half),
            pltpu.VMEM(box, half),
            pltpu.VMEM(box, half),
            pltpu.VMEM(box, half),
            pltpu.VMEM(box, half),
            pltpu.VMEM(chunk, half),
            pltpu.VMEM((2,) + chunk, half),
            pltpu.VMEM((tokens, width), wide),
            pltpu.VMEM((experts, at.flat * cap, routed[0].shape[2]), half),
            pltpu.VMEM((tokens, common[0].shape[1]), half),
            pltpu.VMEM(common[0].shape, half),
            pltpu.VMEM(common[1].shape, half),
            pltpu.VMEM(common[2].shape, half),
            pltpu.VMEM(routed[0].shape, half),
            pltpu.VMEM(routed[1].shape, half),
            pltpu.VMEM(routed[2].shape, half),
            dma((7,)),
            dma((at.deep,)),
            dma((at.deep,)),
            dma((count,)),
            dma((count,)),
            dma((count,)),
            dma((count,)),
            dma((tps,)),
            dma((tps,)),
            dma((2, at.deep)),
            dma((at.deep,)),
            dma((at.deep, at.flat)),
            dma((at.deep, at.flat)),
            dma((at.deep, at.flat, parts)),
            dma((at.deep, at.flat, parts)),
            dma((at.deep, parts)),
            dma((2, at.deep, parts)),
        ],
        compiler_params=pltpu.CompilerParams(
            collective_id=0, has_side_effects=True, vmem_limit_bytes=62 * 1024 * 1024
        ),
    )(
        queries,
        key_matrix,
        value_matrix,
        channel_decay_input,
        head_decay_offset,
        output_gate_input,
        head_norm_gain.reshape(1, -1),
        residual,
        expert_norm_gain.reshape(1, -1),
        packet,
        mixer_output_weight,
        *common,
        *routed,
    )


def solution(mesh):
    placed = (
        P("sp", "tp"),
        P("sp", "tp"),
        P("sp", "tp"),
        P("sp", "tp"),
        P("sp", "tp"),
        P("sp", "tp"),
        P(),
        P(("sp", "tp"), None),
        P(),
        P(),
        P(("sp", "tp"), None),
        P(("sp", "tp"), None),
        P(("sp", "tp"), None, None),
        P(("sp", "tp"), None, None),
        P(("sp", "tp"), None, None),
        P(),
        P(),
        P(),
    )
    return jax.shard_map(
        on_device, mesh=mesh, in_specs=placed, out_specs=P(("sp", "tp"), None), check_vma=False
    )
```

```python
import functools
import math

import jax
import jax.numpy as jnp
from jax import lax
from jax.experimental import pallas as pl
from jax.experimental.pallas import tpu as pltpu
from jax.sharding import PartitionSpec as P

D = 2048
KEY_CHANNELS = 64
VDIM = 128
BLOCK = 64
TOP_K = 4


eps_norm = 1e-06
decay_running = 16.0
routed_scale = 2.5


def peer(sp, tp):
    return {"sp": sp, "tp": tp}


def call_on(targets):
    barrier = pltpu.get_barrier_semaphore()
    for target in targets:
        pl.semaphore_signal(
            barrier, inc=1, device_id=target, device_id_type=pl.DeviceIdType.MESH
        )
    return lambda: pl.semaphore_wait(barrier, len(targets))


def remote(src, dst, send, recv, target):
    return pltpu.make_async_remote_copy(
        src_ref=src,
        dst_ref=dst,
        send_sem=send,
        recv_sem=recv,
        device_id=target,
        device_id_type=pl.DeviceIdType.MESH,
    )


def dot_nt(a, b):
    return lax.dot_general(a, b, (((1,), (1,)), ((), ())), preferred_element_type=jnp.float32)


def dot_tn(a, b):
    return lax.dot_general(a, b, (((0,), (0,)), ((), ())), preferred_element_type=jnp.float32)


def dot_nn(a, b):
    return jnp.dot(a, b, preferred_element_type=jnp.float32)


def exact_dot(ones, values, dot):
    total = 0.0
    for _ in range(3):
        part = values.astype(jnp.bfloat16)
        values = values - part.astype(jnp.float32)
        total = total + dot(ones, part)
    return total


class Place:
    def __init__(self, sp_size, tp_size):
        self.deep = math.gcd(sp_size, 4)
        self.rows = sp_size // self.deep
        self.tp_size = tp_size
        self.flat = self.rows * tp_size

    def here(self):
        sp, tp = lax.axis_index("sp"), lax.axis_index("tp")
        self.sp, self.tp = sp, tp
        self.a = sp // self.rows
        self.b = lax.rem(sp, self.rows)
        self.p = self.b * self.tp_size + tp
        return self

    def column(self, a):
        return peer(a * self.rows + self.b, self.tp)

    def plane(self, p):
        return peer(self.a * self.rows + p // self.tp_size, lax.rem(p, self.tp_size))

    def across(self, q):
        return lax.rem(self.p + q, self.flat)

    def nearest(self, i):
        last = self.deep - 1
        low = self.a < last - self.a
        span = jnp.where(low, self.a, last - self.a)
        away = (i + 1) // 2 if i % 2 else -(i // 2)
        zigzag = jnp.where(low, self.a - away, self.a + away)
        return jnp.where(i <= 2 * span, zigzag, jnp.where(low, i, last - i))


def tiles_of(width, most=512):
    step = math.gcd(width, most)
    return [slice(i, i + step) for i in range(0, width, step)]


def flatten_rows(block):
    groups, rows, width = block.shape
    if rows % 16 == 0:
        return block.reshape(groups * rows, width)
    return block.astype(jnp.float32).reshape(groups * rows, width).astype(jnp.bfloat16)


def layer_kernel(
    sizes, q_ref, k_ref, v_ref, decay_ref, offset_ref, open_ref, head_gain_ref, residual_ref,
    gain_ref, routes_ref, scores_ref, far_mix, far_gate, far_up, far_down,
    wide_gate, wide_up, wide_down, out_ref,
    qd_ref, qx_ref, kg_ref, kt_ref, ends_ref, starts_ref, inner_ref, state_ref, log_ref,
    states_ref, logs_ref, carried_ref, reach_ref, packet_ref, packets_ref, gated_ref, swapped_ref,
    mixer_ref, x_ref, middle_ref, select_ref, mix_ref,
    column_ref, stage_ref, arrived_ref, made_ref, back_ref, sent_ref, came_ref, base_ref,
    hidden_ref, shared_ref, gate_ref, up_ref, down_ref, own_gate, own_up, own_down,
    weight_sem, ks, kr, gs, gr, ls, lr, ws, wr, zs, zr, ps, pr, bs, br, ss, sr,
):
    at = Place(*sizes).here()
    last = at.deep - 1
    flat, rows = stage_ref.shape[1], stage_ref.shape[2]
    width = x_ref.shape[1]
    experts = own_gate.shape[0]
    cap = rows // experts
    cuts = tiles_of(width)
    sides = tiles_of(width, 1024)
    pairs = (
        (far_mix, mixer_ref), (far_gate, gate_ref), (far_up, up_ref), (far_down, down_ref),
        (wide_gate, own_gate), (wide_up, own_up), (wide_down, own_down),
    )
    loads = [
        pltpu.make_async_copy(src, dst, weight_sem.at[i]) for i, (src, dst) in enumerate(pairs)
    ]
    for load in loads:
        load.start()
    has_right, has_left = at.a < last, at.a > 0
    count, tps = sizes
    met = call_on(
        [peer(lax.rem(at.sp + d, count), at.tp) for d in range(1, count)]
        + [at.plane(at.across(q)) for q in range(1, flat)]
    )
    half, wide = jnp.bfloat16, jnp.float32
    length, lanes = q_ref.shape
    heads = offset_ref.shape[0]
    blocks = length // BLOCK
    tokens = x_ref.shape[0]
    lane = lax.broadcasted_iota(jnp.int32, (1, lanes), 1)
    of_head = [
        (lane >= h * KEY_CHANNELS) & (lane < (h + 1) * KEY_CHANNELS) for h in range(heads)
    ]
    columns = [slice(h * VDIM, (h + 1) * VDIM) for h in range(heads)]
    tile = math.gcd(length, 4 * BLOCK)
    row = lax.broadcasted_iota(jnp.int32, (tile, tile), 0)
    col = lax.broadcasted_iota(jnp.int32, (tile, tile), 1)
    causal = (jnp.bitwise_and(row, -BLOCK) == jnp.bitwise_and(col, -BLOCK)) & (col <= row)
    ones = jnp.where(causal, 1.0, 0.0).astype(half)

    for t in range(0, length, tile):
        span = slice(t, t + tile)
        pre = decay_ref[span, :].astype(wide)
        log_decay = (
            jnp.minimum(pre, 0.0) - jnp.log1p(jnp.exp(-jnp.abs(pre)))
        ) / decay_running
        dropped = exact_dot(ones, offset_ref[:, span], dot_nt)
        offset = dropped[:, 0:1]
        for h in range(1, heads):
            offset = jnp.where(of_head[h], dropped[:, h : h + 1], offset)
        within = exact_dot(ones, log_decay, dot_nn) + offset
        keys = k_ref[span, :].astype(wide)
        qd_ref[span, :] = q_ref[span, :].astype(wide) * KEY_CHANNELS ** (-0.5) * jnp.exp(within)
        grown = keys * jnp.exp(-within)
        for h in range(heads):
            kg_ref[h, span, :] = jnp.where(of_head[h], grown, 0.0).astype(half)
        for n in range(0, tile, BLOCK):
            inside = slice(n, n + BLOCK)
            end = within[n + BLOCK - 1 : n + BLOCK, :]
            kt_ref[t + n : t + n + BLOCK, :] = (
                keys[inside, :] * jnp.exp(end - within[inside, :])
            ).astype(half)
            ends_ref[(t + n) // BLOCK : (t + n) // BLOCK + 1, :] = end
    state = jnp.zeros((VDIM, lanes), wide)
    passed = jnp.zeros((1, lanes), wide)
    for n in range(blocks):
        span = slice(n * BLOCK, (n + 1) * BLOCK)
        starts_ref[n] = state.astype(half)
        end = ends_ref[n : n + 1, :]
        both = dot_tn(v_ref[span, :], kt_ref[span, :])
        added = both[columns[0], :]
        for h in range(1, heads):
            added = jnp.where(of_head[h], both[columns[h], :], added)
        moved = qd_ref[span, :] * jnp.exp(passed)
        for h in range(heads):
            qx_ref[h, span, :] = jnp.where(of_head[h], moved, 0.0).astype(half)
        state = state * jnp.exp(end) + added
        passed = passed + end
    state_ref[...] = state.astype(half)
    log_ref[...] = jnp.broadcast_to(passed, log_ref.shape)
    def packet_copy(d):
        return remote(
            packet_ref,
            packets_ref.at[at.a],
            ks.at[d],
            kr.at[at.a],
            at.column(lax.rem(at.a + d, at.deep)),
        )

    def packet_from(a):
        return remote(packet_ref, packets_ref.at[a], ks.at[0], kr.at[a], at.column(at.a))

    def state_copy(d):
        target = peer(jnp.minimum(at.sp + d, count - 1), at.tp)
        return (
            remote(state_ref, states_ref.at[at.sp], gs.at[d], gr.at[at.sp], target),
            remote(log_ref, logs_ref.at[at.sp], ls.at[d], lr.at[at.sp], target),
        )

    def swap_copy(d):
        to = lax.rem(at.tp + d, tps)
        return remote(
            gated_ref.at[to], swapped_ref.at[at.tp], ws.at[d], wr.at[at.tp], peer(at.sp, to)
        )

    packet_ref[:TOP_K, :] = routes_ref[...].astype(wide)
    packet_ref[TOP_K:, :] = scores_ref[...]
    packets_ref[at.a] = packet_ref[...]
    for t in range(0, length, tile):
        span = slice(t, t + tile)
        ahead = qd_ref[span, :].astype(half)
        for h in range(heads):
            scores = jnp.where(causal, dot_nt(ahead, kg_ref[h, span, :]), 0.0)
            inner_ref[span, columns[h]] = jnp.dot(
                scores.astype(half), v_ref[span, columns[h]], preferred_element_type=wide
            )
    for n in range(1, blocks):
        span = slice(n * BLOCK, (n + 1) * BLOCK)
        for h in range(heads):
            ahead = jnp.where(of_head[h], qd_ref[span, :], 0.0).astype(half)
            inner_ref[span, columns[h]] += dot_nt(ahead, starts_ref[n])

    met()
    for d in range(1, at.deep):
        packet_copy(d).start()
    for d in range(1, count):

        @pl.when(at.sp + d < count)
        def _(d=d):
            for copy in state_copy(d):
                copy.start()

    slots = flat * rows
    plane_experts = flat * experts
    here = lax.broadcasted_iota(jnp.int32, (slots, plane_experts), 0)
    there = lax.broadcasted_iota(jnp.int32, (slots, plane_experts), 1) * cap
    belongs = (here >= there) & (here < there + cap)
    spread = jnp.where(belongs, 1.0, 0.0).astype(half)
    place = jnp.sum(
        jnp.where(belongs, (here - there).astype(wide), 0.0), axis=1, keepdims=True
    )
    expert = (
        at.a * plane_experts + lax.broadcasted_iota(jnp.int32, (plane_experts, 1), 0)
    ).astype(wide)
    sooner = jnp.where(
        lax.broadcasted_iota(jnp.int32, (tokens, tokens), 0)
        < lax.broadcasted_iota(jnp.int32, (tokens, tokens), 1),
        1.0,
        0.0,
    ).astype(half)
    def lay_out(a):
        pl.when(at.a != a)(lambda a=a: packet_from(a).wait_recv())
        scored = packets_ref[a, TOP_K:, :]
        share = routed_scale * scored / jnp.sum(scored, axis=0, keepdims=True)
        chosen = jnp.zeros((plane_experts, tokens), wide)
        weight_of = jnp.zeros((plane_experts, tokens), wide)
        for k in range(TOP_K):
            hit = packets_ref[a, k : k + 1, :] == expert
            chosen = jnp.where(hit, 1.0, chosen)
            weight_of = jnp.where(hit, share[k : k + 1, :], weight_of)
        rank = jnp.dot(chosen.astype(half), sooner, preferred_element_type=wide)
        rank = jnp.where(chosen > 0.0, rank, -1.0)
        ranks = jnp.dot(spread, rank.astype(half), preferred_element_type=wide)
        weights = jnp.dot(spread, weight_of.astype(half), preferred_element_type=wide)
        taken = ranks == place
        select_ref[a] = jnp.where(taken, 1.0, 0.0).astype(half)
        mix_ref[a] = jnp.transpose(jnp.where(taken, weights, 0.0)).astype(half)

    early = at.deep // 2
    for a in range(early):
        lay_out(a)

    carried_ref[...] = jnp.zeros_like(carried_ref)
    reach_ref[...] = jnp.zeros_like(reach_ref)
    for j in reversed(range(count - 1)):

        @pl.when(j < at.sp)
        def _(j=j):
            source = peer(j, at.tp)
            remote(state_ref, states_ref.at[j], gs.at[0], gr.at[j], source).wait_recv()
            remote(log_ref, logs_ref.at[j], ls.at[0], lr.at[j], source).wait_recv()
            carried_ref[...] += jnp.exp(reach_ref[0:1, :]) * states_ref[j].astype(wide)
            reach_ref[...] += logs_ref[j]

    carried = carried_ref[...].astype(half)
    for d in [*range(1, tps), 0]:
        to = lax.rem(at.tp + d, tps)
        span = pl.ds(pl.multiple_of(to * tokens, tokens), tokens)
        for h in range(heads):
            output = inner_ref[span, columns[h]] + dot_nt(qx_ref[h, span, :], carried)
            inv_rms = lax.rsqrt(jnp.mean(output * output, axis=-1, keepdims=True) + eps_norm)
            gated_ref[to, :, columns[h]] = (
                output
                * inv_rms
                * head_gain_ref[...]
                * jax.nn.silu(open_ref[span, columns[h]].astype(wide))
            ).astype(half)
        if d > 0:
            swap_copy(d).start()
    for a in range(early, at.deep):
        lay_out(a)
    loads[0].wait()
    span = heads * VDIM
    for d in range(tps):
        source = lax.rem(at.tp - d + tps, tps)
        if d > 0:
            remote(
                gated_ref.at[0], swapped_ref.at[source], ws.at[0], wr.at[source], peer(at.sp, source)
            ).wait_recv()
        piece = gated_ref[source] if d == 0 else swapped_ref[source]
        part_of = pl.ds(pl.multiple_of(source * span, span), span)
        for cut in cuts:
            part = jnp.dot(piece, mixer_ref[part_of, cut], preferred_element_type=wide)
            if d == 0:
                base_ref[:, cut] = residual_ref[:, cut].astype(wide) + part
            else:
                base_ref[:, cut] += part
    square = jnp.zeros((tokens, 1), wide)
    for cut in cuts:
        middle_ref[:, cut] = base_ref[:, cut].astype(half)
        middle = middle_ref[:, cut].astype(wide)
        square = square + jnp.sum(middle * middle, axis=-1, keepdims=True)
    scale = lax.rsqrt(square / width + eps_norm)
    for cut in cuts:
        x_ref[:, cut] = (middle_ref[:, cut].astype(wide) * scale * gain_ref[:, cut]).astype(half)

    def relay(source, owner, side, j):
        return remote(
            source.at[:, sides[j]],
            column_ref.at[owner, :, sides[j]],
            zs.at[side, owner, j],
            zr.at[owner, j],
            at.column(at.a + (1 if side == 0 else -1)),
        )

    def sends(owner):
        right = has_right & (owner <= at.a)
        left = has_left & (owner >= at.a)
        return right, left

    def forward(source, owner, j):
        right, left = sends(owner)
        pl.when(right)(lambda: relay(source, owner, 0, j).start())
        pl.when(left)(lambda: relay(source, owner, 1, j).start())

    def out_copy(owner, q, j):
        target = at.across(q)
        return remote(
            stage_ref.at[owner, target, :, sides[j]],
            arrived_ref.at[owner, at.p, :, sides[j]],
            ps.at[owner, q, j],
            pr.at[owner, q, j],
            at.plane(target),
        )

    def back_copy(owner, q, i):
        target = at.across(q)
        return remote(
            made_ref.at[owner, target, :, cuts[i]],
            back_ref.at[owner, at.p, :, cuts[i]],
            bs.at[owner, q, i],
            br.at[owner, q, i],
            at.plane(target),
        )

    def pass_on(owner, source, j):
        start, stop = sides[j].start, sides[j].stop
        for cut in [cut for cut in cuts if start <= cut.start < stop]:
            picked = jnp.dot(
                select_ref[owner], source[:, cut], preferred_element_type=jnp.float32
            )
            stage_ref[owner, :, :, cut] = picked.reshape(flat, rows, -1).astype(jnp.bfloat16)
        for q in range(1, flat):
            out_copy(owner, q, j).start()
        arrived_ref[owner, at.p, :, sides[j]] = stage_ref[owner, at.p, :, sides[j]]

    def send_back(owner, i):
        for q in range(1, flat):
            back_copy(owner, q, i).start()

    def run_experts(owner):
        for q in range(1, flat):
            for j in range(len(sides)):
                out_copy(owner, q, j).wait_recv()
        for e in range(experts):
            mine = slice(e * cap, (e + 1) * cap)
            block = flatten_rows(arrived_ref[owner, :, mine, :])
            for cut in tiles_of(own_gate.shape[2], 256):
                gate = jnp.dot(block, own_gate[e, :, cut], preferred_element_type=jnp.float32)
                up = jnp.dot(block, own_up[e, :, cut], preferred_element_type=jnp.float32)
                hidden_ref[e, :, cut] = (jax.nn.silu(gate) * up).astype(jnp.bfloat16)
        for i, cut in enumerate(cuts):
            for e in range(experts):
                mine = slice(e * cap, (e + 1) * cap)
                down = jnp.dot(
                    hidden_ref[e], own_down[e, :, cut], preferred_element_type=jnp.float32
                )
                made_ref[owner, :, mine, cut] = down.reshape(flat, cap, -1).astype(jnp.bfloat16)
        back_ref[owner, at.p] = made_ref[owner, at.p]

    def send_all(owner):
        for i in range(len(cuts)):
            send_back(owner, i)

    def mixed(owner, i):
        for q in range(1, flat):
            back_copy(owner, q, i).wait_recv()
        block = flatten_rows(back_ref[owner, :, :, cuts[i]])
        return jnp.dot(mix_ref[owner], block, preferred_element_type=jnp.float32)

    def toward(owner, side, i):
        return remote(
            sent_ref.at[owner, :, cuts[i]],
            came_ref.at[side, owner, :, cuts[i]],
            ss.at[owner, i],
            sr.at[side, owner, i],
            at.column(at.a - 1 + 2 * side),
        )

    def step(owner, side, more):
        for i, cut in enumerate(cuts):
            part = mixed(owner, i)
            if more:
                toward(owner, side, i).wait_recv()
                part = part + came_ref[side, owner, :, cut].astype(jnp.float32)
            sent_ref[owner, :, cut] = part.astype(jnp.bfloat16)
            toward(owner, side, i).start()

    def homeward(turn):
        for place in range(2):
            side = jnp.where(2 * at.a < at.deep, 1 - place, place)
            owner = jnp.where(side == 0, last - turn, turn)
            goes = jnp.where(side == 0, owner < at.a, owner > at.a)
            far = jnp.where(side == 0, has_right, has_left)
            pl.when(goes & far)(lambda owner=owner, side=side: step(owner, side, True))
            pl.when(goes & jnp.logical_not(far))(
                lambda owner=owner, side=side: step(owner, side, False)
            )

    def take(i):
        for j in range(len(sides)):
            relay(x_ref, order[i], 0, j).wait_recv()
            forward(column_ref.at[order[i]], order[i], j)
            pass_on(order[i], column_ref.at[order[i]], j)

    order = [at.nearest(i) for i in range(at.deep)]
    for j in range(len(sides)):
        forward(x_ref, at.a, j)
    for j in range(len(sides)):
        pass_on(at.a, x_ref, j)
    for load in loads[1:4]:
        load.wait()
    for cut in tiles_of(gate_ref.shape[1], 256):
        gate = jnp.dot(x_ref[...], gate_ref[:, cut], preferred_element_type=jnp.float32)
        up = jnp.dot(x_ref[...], up_ref[:, cut], preferred_element_type=jnp.float32)
        shared_ref[:, cut] = (jax.nn.silu(gate) * up).astype(jnp.bfloat16)
    for cut in cuts:
        base_ref[:, cut] = middle_ref[:, cut].astype(jnp.float32) + jnp.dot(
            shared_ref[...], down_ref[:, cut], preferred_element_type=jnp.float32
        )
    for i in range(1, at.deep + 1):
        if i < at.deep:
            take(i)
        if i == 1:
            for load in loads[4:]:
                load.wait()
        if i == at.deep:
            send_all(order[1])
        run_experts(order[i - 1])
    turns = [1, *range(at.deep - 1, 1, -1)]
    for turn in turns[1:]:
        send_all(order[turn])
    send_all(at.a)
    for turn in turns:
        homeward(turn)

    for side, far in ((0, has_right), (1, has_left)):

        @pl.when(far)
        def _(side=side):
            for i, cut in enumerate(cuts):
                toward(at.a, side, i).wait_recv()
                base_ref[:, cut] += came_ref[side, at.a, :, cut].astype(jnp.float32)

    for i, cut in enumerate(cuts):
        out_ref[:, cut] = (base_ref[:, cut] + mixed(at.a, i)).astype(out_ref.dtype)
    for d in range(1, at.deep):
        packet_copy(d).wait_send()
    for d in range(1, count):

        @pl.when(at.sp + d < count)
        def _(d=d):
            for copy in state_copy(d):
                copy.wait_send()

    for d in range(1, tps):
        swap_copy(d).wait_send()
    for i in range(at.deep):
        owner = order[i]
        right, left = sends(owner)
        for j in range(len(sides)):
            pl.when(right)(lambda owner=owner, j=j: relay(x_ref, owner, 0, j).wait_send())
            pl.when(left)(lambda owner=owner, j=j: relay(x_ref, owner, 1, j).wait_send())
        for q in range(1, flat):
            for j in range(len(sides)):
                out_copy(owner, q, j).wait_send()
            for j in range(len(cuts)):
                back_copy(owner, q, j).wait_send()
        if i > 0:
            for j in range(len(cuts)):
                toward(owner, 0, j).wait_send()


def on_device(
    queries,
    key_matrix,
    value_matrix,
    channel_decay_input,
    head_decay_offset,
    output_gate_input,
    head_norm_gain,
    residual,
    mixer_output_weight,
    expert_norm_gain,
    routes,
    chosen_router_scores,
    routed_gate_weight,
    routed_up_weight,
    routed_down_weight,
    common_gate_weight,
    common_up_weight,
    common_down_weight,
):
    count, tps = sizes = (lax.axis_size("sp"), lax.axis_size("tp"))
    at = Place(*sizes)
    tokens, width = residual.shape
    length, lanes = queries.shape
    heads = head_decay_offset.shape[1]
    blocks = length // BLOCK
    experts = routed_gate_weight.shape[0]
    cap = 2 * TOP_K * tokens // (experts * count * tps)
    rows = experts * cap
    slots = at.flat * rows
    parts, halves = len(tiles_of(width)), len(tiles_of(width, 1024))
    common = (common_gate_weight, common_up_weight, common_down_weight)
    routed = (routed_gate_weight, routed_up_weight, routed_down_weight)
    box = (at.deep, at.flat, rows, width)
    chunk = (at.deep, tokens, width)
    dma = pltpu.SemaphoreType.DMA
    half, wide = jnp.bfloat16, jnp.float32
    vmem = pl.BlockSpec(memory_space=pltpu.VMEM)
    far = pl.BlockSpec(memory_space=pl.ANY)
    return pl.pallas_call(
        functools.partial(layer_kernel, sizes),
        out_shape=pltpu.VMEM((tokens, width), half),
        in_specs=[vmem] * 11 + [far] * 7,
        out_specs=vmem,
        scratch_shapes=[
            pltpu.VMEM((length, lanes), wide),
            pltpu.VMEM((heads, length, lanes), half),
            pltpu.VMEM((heads, length, lanes), half),
            pltpu.VMEM((length, lanes), half),
            pltpu.VMEM((max(8, blocks), lanes), wide),
            pltpu.VMEM((blocks, VDIM, lanes), half),
            pltpu.VMEM((length, heads * VDIM), wide),
            pltpu.VMEM((VDIM, lanes), half),
            pltpu.VMEM((8, lanes), wide),
            pltpu.VMEM((count, VDIM, lanes), half),
            pltpu.VMEM((count, 8, lanes), wide),
            pltpu.VMEM((VDIM, lanes), wide),
            pltpu.VMEM((8, lanes), wide),
            pltpu.VMEM((2 * TOP_K, tokens), wide),
            pltpu.VMEM((at.deep, 2 * TOP_K, tokens), wide),
            pltpu.VMEM((tps, tokens, heads * VDIM), half),
            pltpu.VMEM((tps, tokens, heads * VDIM), half),
            pltpu.VMEM(mixer_output_weight.shape, half),
            pltpu.VMEM((tokens, width), half),
            pltpu.VMEM((tokens, width), half),
            pltpu.VMEM((at.deep, slots, tokens), half),
            pltpu.VMEM((at.deep, tokens, slots), half),
            pltpu.VMEM(chunk, half),
            pltpu.VMEM(box, half),
            pltpu.VMEM(box, half),
            pltpu.VMEM(box, half),
            pltpu.VMEM(box, half),
            pltpu.VMEM(chunk, half),
            pltpu.VMEM((2,) + chunk, half),
            pltpu.VMEM((tokens, width), wide),
            pltpu.VMEM((experts, at.flat * cap, routed[0].shape[2]), half),
            pltpu.VMEM((tokens, common[0].shape[1]), half),
            pltpu.VMEM(common[0].shape, half),
            pltpu.VMEM(common[1].shape, half),
            pltpu.VMEM(common[2].shape, half),
            pltpu.VMEM(routed[0].shape, half),
            pltpu.VMEM(routed[1].shape, half),
            pltpu.VMEM(routed[2].shape, half),
            dma((7,)),
            dma((at.deep,)),
            dma((at.deep,)),
            dma((count,)),
            dma((count,)),
            dma((count,)),
            dma((count,)),
            dma((tps,)),
            dma((tps,)),
            dma((2, at.deep, halves)),
            dma((at.deep, halves)),
            dma((at.deep, at.flat, halves)),
            dma((at.deep, at.flat, halves)),
            dma((at.deep, at.flat, parts)),
            dma((at.deep, at.flat, parts)),
            dma((at.deep, parts)),
            dma((2, at.deep, parts)),
        ],
        compiler_params=pltpu.CompilerParams(
            collective_id=0, has_side_effects=True, vmem_limit_bytes=62 * 1024 * 1024
        ),
    )(
        queries,
        key_matrix,
        value_matrix,
        channel_decay_input,
        head_decay_offset.T,
        output_gate_input,
        head_norm_gain.reshape(1, -1),
        residual,
        expert_norm_gain.reshape(1, -1),
        routes.T,
        chosen_router_scores.T,
        mixer_output_weight,
        *common,
        *routed,
    )


def solution(mesh):
    placed = (
        P("sp", "tp"),
        P("sp", "tp"),
        P("sp", "tp"),
        P("sp", "tp"),
        P("sp", "tp"),
        P("sp", "tp"),
        P(),
        P(("sp", "tp"), None),
        P(),
        P(),
        P(("sp", "tp"), None),
        P(("sp", "tp"), None),
        P(("sp", "tp"), None, None),
        P(("sp", "tp"), None, None),
        P(("sp", "tp"), None, None),
        P(),
        P(),
        P(),
    )
    return jax.shard_map(
        on_device, mesh=mesh, in_specs=placed, out_specs=P(("sp", "tp"), None), check_vma=False
    )
```

```python
import functools
import math

import jax
import jax.numpy as jnp
from jax import lax
from jax.experimental import pallas as pl
from jax.experimental.pallas import tpu as pltpu
from jax.sharding import PartitionSpec as P

D = 2048
KEY_CHANNELS = 64
VDIM = 128
BLOCK = 64
TOP_K = 4


eps_norm = 1e-06
decay_running = 16.0
routed_scale = 2.5


def peer(sp, tp):
    return {"sp": sp, "tp": tp}


def call_on(targets):
    barrier = pltpu.get_barrier_semaphore()
    for target in targets:
        pl.semaphore_signal(
            barrier, inc=1, device_id=target, device_id_type=pl.DeviceIdType.MESH
        )
    return lambda: pl.semaphore_wait(barrier, len(targets))


def remote(src, dst, send, recv, target):
    return pltpu.make_async_remote_copy(
        src_ref=src,
        dst_ref=dst,
        send_sem=send,
        recv_sem=recv,
        device_id=target,
        device_id_type=pl.DeviceIdType.MESH,
    )


def dot_nt(a, b):
    return lax.dot_general(a, b, (((1,), (1,)), ((), ())), preferred_element_type=jnp.float32)


def dot_tn(a, b):
    return lax.dot_general(a, b, (((0,), (0,)), ((), ())), preferred_element_type=jnp.float32)


def dot_nn(a, b):
    return jnp.dot(a, b, preferred_element_type=jnp.float32)


def exact_dot(ones, values, dot):
    total = 0.0
    for _ in range(3):
        part = values.astype(jnp.bfloat16)
        values = values - part.astype(jnp.float32)
        total = total + dot(ones, part)
    return total


class Place:
    def __init__(self, sp_size, tp_size):
        self.deep = math.gcd(sp_size, 4)
        self.rows = sp_size // self.deep
        self.tp_size = tp_size
        self.flat = self.rows * tp_size

    def here(self):
        sp, tp = lax.axis_index("sp"), lax.axis_index("tp")
        self.sp, self.tp = sp, tp
        self.a = sp // self.rows
        self.b = lax.rem(sp, self.rows)
        self.p = self.b * self.tp_size + tp
        return self

    def column(self, a):
        return peer(a * self.rows + self.b, self.tp)

    def plane(self, p):
        return peer(self.a * self.rows + p // self.tp_size, lax.rem(p, self.tp_size))

    def across(self, q):
        return lax.rem(self.p + q, self.flat)

    def nearest(self, i):
        last = self.deep - 1
        low = self.a < last - self.a
        span = jnp.where(low, self.a, last - self.a)
        away = (i + 1) // 2 if i % 2 else -(i // 2)
        zigzag = jnp.where(low, self.a - away, self.a + away)
        return jnp.where(i <= 2 * span, zigzag, jnp.where(low, i, last - i))


def tiles_of(width, most=512):
    step = math.gcd(width, most)
    return [slice(i, i + step) for i in range(0, width, step)]


def flatten_rows(block):
    groups, rows, width = block.shape
    if rows % 16 == 0:
        return block.reshape(groups * rows, width)
    return block.astype(jnp.float32).reshape(groups * rows, width).astype(jnp.bfloat16)


def layer_kernel(
    sizes, q_ref, k_ref, v_ref, decay_ref, offset_ref, open_ref, head_gain_ref, residual_ref,
    gain_ref, routes_ref, scores_ref, far_mix, far_gate, far_up, far_down,
    wide_gate, wide_up, wide_down, out_ref,
    qd_ref, qx_ref, kt_ref, ends_ref, starts_ref, inner_ref, state_ref, log_ref,
    states_ref, logs_ref, carried_ref, reach_ref, packet_ref, packets_ref, gated_ref, swapped_ref,
    mixer_ref, x_ref, middle_ref, select_ref, mix_ref,
    column_ref, stage_ref, arrived_ref, made_ref, back_ref, sent_ref, came_ref, base_ref,
    hidden_ref, shared_ref, gate_ref, up_ref, down_ref, own_gate, own_up, own_down,
    weight_sem, ks, kr, gs, gr, ls, lr, ws, wr, zs, zr, ps, pr, bs, br, ss, sr,
):
    at = Place(*sizes).here()
    last = at.deep - 1
    flat, rows = stage_ref.shape[1], stage_ref.shape[2]
    width = x_ref.shape[1]
    experts = own_gate.shape[0]
    cap = rows // experts
    cuts = tiles_of(width)
    sides = tiles_of(width, 1024)
    pairs = (
        (far_mix, mixer_ref), (far_gate, gate_ref), (far_up, up_ref), (far_down, down_ref),
        (wide_gate, own_gate), (wide_up, own_up), (wide_down, own_down),
    )
    loads = [
        pltpu.make_async_copy(src, dst, weight_sem.at[i]) for i, (src, dst) in enumerate(pairs)
    ]
    for load in loads:
        load.start()
    has_right, has_left = at.a < last, at.a > 0
    count, tps = sizes
    met = call_on(
        [peer(lax.rem(at.sp + d, count), at.tp) for d in range(1, count)]
        + [at.plane(at.across(q)) for q in range(1, flat)]
    )
    half, wide = jnp.bfloat16, jnp.float32
    length, lanes = q_ref.shape
    heads = offset_ref.shape[0]
    blocks = length // BLOCK
    tokens = x_ref.shape[0]
    lane = lax.broadcasted_iota(jnp.int32, (1, lanes), 1)
    of_head = [
        (lane >= h * KEY_CHANNELS) & (lane < (h + 1) * KEY_CHANNELS) for h in range(heads)
    ]
    columns = [slice(h * VDIM, (h + 1) * VDIM) for h in range(heads)]
    tile = math.gcd(length, 4 * BLOCK)
    row = lax.broadcasted_iota(jnp.int32, (tile, tile), 0)
    col = lax.broadcasted_iota(jnp.int32, (tile, tile), 1)
    causal = (jnp.bitwise_and(row, -BLOCK) == jnp.bitwise_and(col, -BLOCK)) & (col <= row)
    ones = jnp.where(causal, 1.0, 0.0).astype(half)

    for t in range(0, length, tile):
        span = slice(t, t + tile)
        pre = decay_ref[span, :].astype(wide)
        log_decay = (
            jnp.minimum(pre, 0.0) - jnp.log1p(jnp.exp(-jnp.abs(pre)))
        ) / decay_running
        dropped = exact_dot(ones, offset_ref[:, span], dot_nt)
        offset = dropped[:, 0:1]
        for h in range(1, heads):
            offset = jnp.where(of_head[h], dropped[:, h : h + 1], offset)
        within = exact_dot(ones, log_decay, dot_nn) + offset
        keys = k_ref[span, :].astype(wide)
        qd_ref[span, :] = within
        for n in range(0, tile, BLOCK):
            inside = slice(n, n + BLOCK)
            end = within[n + BLOCK - 1 : n + BLOCK, :]
            kt_ref[t + n : t + n + BLOCK, :] = (
                keys[inside, :] * jnp.exp(end - within[inside, :])
            ).astype(half)
            ends_ref[(t + n) // BLOCK : (t + n) // BLOCK + 1, :] = end
    state = jnp.zeros((VDIM, lanes), wide)
    passed = jnp.zeros((1, lanes), wide)
    for n in range(blocks):
        span = slice(n * BLOCK, (n + 1) * BLOCK)
        starts_ref[n] = state.astype(half)
        end = ends_ref[n : n + 1, :]
        both = dot_tn(v_ref[span, :], kt_ref[span, :])
        added = both[columns[0], :]
        for h in range(1, heads):
            added = jnp.where(of_head[h], both[columns[h], :], added)
        state = state * jnp.exp(end) + added
        passed = passed + end
    state_ref[...] = state.astype(half)
    log_ref[...] = jnp.broadcast_to(passed, log_ref.shape)
    def packet_copy(d):
        return remote(
            packet_ref,
            packets_ref.at[at.a],
            ks.at[d],
            kr.at[at.a],
            at.column(lax.rem(at.a + d, at.deep)),
        )

    def packet_from(a):
        return remote(packet_ref, packets_ref.at[a], ks.at[0], kr.at[a], at.column(at.a))

    def state_copy(d):
        target = peer(jnp.minimum(at.sp + d, count - 1), at.tp)
        return (
            remote(state_ref, states_ref.at[at.sp], gs.at[d], gr.at[at.sp], target),
            remote(log_ref, logs_ref.at[at.sp], ls.at[d], lr.at[at.sp], target),
        )

    def swap_copy(d):
        to = lax.rem(at.tp + d, tps)
        return remote(
            gated_ref.at[to], swapped_ref.at[at.tp], ws.at[d], wr.at[at.tp], peer(at.sp, to)
        )

    packet_ref[:TOP_K, :] = routes_ref[...].astype(wide)
    packet_ref[TOP_K:, :] = scores_ref[...]
    packets_ref[at.a] = packet_ref[...]
    met()
    for d in range(1, at.deep):
        packet_copy(d).start()
    for d in range(1, count):

        @pl.when(at.sp + d < count)
        def _(d=d):
            for copy in state_copy(d):
                copy.start()

    for t in range(0, length, tile):
        span = slice(t, t + tile)
        within = qd_ref[span, :]
        grown = k_ref[span, :].astype(wide) * jnp.exp(-within)
        ahead = q_ref[span, :].astype(wide) * KEY_CHANNELS ** (-0.5) * jnp.exp(within)
        qd_ref[span, :] = ahead
        ahead = ahead.astype(half)
        for h in range(heads):
            kept = jnp.where(of_head[h], grown, 0.0).astype(half)
            scores = jnp.where(causal, dot_nt(ahead, kept), 0.0)
            inner_ref[span, columns[h]] = jnp.dot(
                scores.astype(half), v_ref[span, columns[h]], preferred_element_type=wide
            )
    passed = jnp.zeros((1, lanes), wide)
    for n in range(blocks):
        span = slice(n * BLOCK, (n + 1) * BLOCK)
        for h in range(heads):
            ahead = jnp.where(of_head[h], qd_ref[span, :], 0.0)
            qx_ref[h, span, :] = (ahead * jnp.exp(passed)).astype(half)
            if n > 0:
                inner_ref[span, columns[h]] += dot_nt(ahead.astype(half), starts_ref[n])
        passed = passed + ends_ref[n : n + 1, :]

    slots = flat * rows
    plane_experts = flat * experts
    here = lax.broadcasted_iota(jnp.int32, (slots, plane_experts), 0)
    there = lax.broadcasted_iota(jnp.int32, (slots, plane_experts), 1) * cap
    belongs = (here >= there) & (here < there + cap)
    spread = jnp.where(belongs, 1.0, 0.0).astype(half)
    place = jnp.sum(
        jnp.where(belongs, (here - there).astype(wide), 0.0), axis=1, keepdims=True
    )
    expert = (
        at.a * plane_experts + lax.broadcasted_iota(jnp.int32, (plane_experts, 1), 0)
    ).astype(wide)
    sooner = jnp.where(
        lax.broadcasted_iota(jnp.int32, (tokens, tokens), 0)
        < lax.broadcasted_iota(jnp.int32, (tokens, tokens), 1),
        1.0,
        0.0,
    ).astype(half)
    def lay_out(a):
        pl.when(at.a != a)(lambda a=a: packet_from(a).wait_recv())
        scored = packets_ref[a, TOP_K:, :]
        share = routed_scale * scored / jnp.sum(scored, axis=0, keepdims=True)
        chosen = jnp.zeros((plane_experts, tokens), wide)
        weight_of = jnp.zeros((plane_experts, tokens), wide)
        for k in range(TOP_K):
            hit = packets_ref[a, k : k + 1, :] == expert
            chosen = jnp.where(hit, 1.0, chosen)
            weight_of = jnp.where(hit, share[k : k + 1, :], weight_of)
        rank = jnp.dot(chosen.astype(half), sooner, preferred_element_type=wide)
        rank = jnp.where(chosen > 0.0, rank, -1.0)
        ranks = jnp.dot(spread, rank.astype(half), preferred_element_type=wide)
        weights = jnp.dot(spread, weight_of.astype(half), preferred_element_type=wide)
        taken = ranks == place
        select_ref[a] = jnp.where(taken, 1.0, 0.0).astype(half)
        mix_ref[a] = jnp.transpose(jnp.where(taken, weights, 0.0)).astype(half)

    early = at.deep // 2
    for a in range(early):
        lay_out(a)

    carried_ref[...] = jnp.zeros_like(carried_ref)
    reach_ref[...] = jnp.zeros_like(reach_ref)
    for j in reversed(range(count - 1)):

        @pl.when(j < at.sp)
        def _(j=j):
            source = peer(j, at.tp)
            remote(state_ref, states_ref.at[j], gs.at[0], gr.at[j], source).wait_recv()
            remote(log_ref, logs_ref.at[j], ls.at[0], lr.at[j], source).wait_recv()
            carried_ref[...] += jnp.exp(reach_ref[0:1, :]) * states_ref[j].astype(wide)
            reach_ref[...] += logs_ref[j]

    carried = carried_ref[...].astype(half)
    for d in [*sorted(range(1, tps), key=lambda d: abs(2 * d - tps)), 0]:
        to = lax.rem(at.tp + d, tps)
        span = pl.ds(pl.multiple_of(to * tokens, tokens), tokens)
        for h in range(heads):
            output = inner_ref[span, columns[h]] + dot_nt(qx_ref[h, span, :], carried)
            inv_rms = lax.rsqrt(jnp.mean(output * output, axis=-1, keepdims=True) + eps_norm)
            gated_ref[to, :, columns[h]] = (
                output
                * inv_rms
                * head_gain_ref[...]
                * jax.nn.silu(open_ref[span, columns[h]].astype(wide))
            ).astype(half)
        if d > 0:
            swap_copy(d).start()
    for a in range(early, at.deep):
        lay_out(a)
    loads[0].wait()
    span = heads * VDIM
    for d in range(tps):
        source = lax.rem(at.tp - d + tps, tps)
        if d > 0:
            remote(
                gated_ref.at[0], swapped_ref.at[source], ws.at[0], wr.at[source], peer(at.sp, source)
            ).wait_recv()
        piece = gated_ref[source] if d == 0 else swapped_ref[source]
        part_of = pl.ds(pl.multiple_of(source * span, span), span)
        for cut in cuts:
            part = jnp.dot(piece, mixer_ref[part_of, cut], preferred_element_type=wide)
            if d == 0:
                base_ref[:, cut] = residual_ref[:, cut].astype(wide) + part
            else:
                base_ref[:, cut] += part
    square = jnp.zeros((tokens, 1), wide)
    for cut in cuts:
        middle_ref[:, cut] = base_ref[:, cut].astype(half)
        middle = middle_ref[:, cut].astype(wide)
        square = square + jnp.sum(middle * middle, axis=-1, keepdims=True)
    scale = lax.rsqrt(square / width + eps_norm)
    for cut in cuts:
        x_ref[:, cut] = (middle_ref[:, cut].astype(wide) * scale * gain_ref[:, cut]).astype(half)

    def relay(source, owner, side, j):
        return remote(
            source.at[:, sides[j]],
            column_ref.at[owner, :, sides[j]],
            zs.at[side, owner, j],
            zr.at[owner, j],
            at.column(at.a + (1 if side == 0 else -1)),
        )

    def sends(owner):
        right = has_right & (owner <= at.a)
        left = has_left & (owner >= at.a)
        return right, left

    def forward(source, owner, j):
        right, left = sends(owner)
        pl.when(right)(lambda: relay(source, owner, 0, j).start())
        pl.when(left)(lambda: relay(source, owner, 1, j).start())

    def out_copy(owner, q, j):
        target = at.across(q)
        return remote(
            stage_ref.at[owner, target, :, sides[j]],
            arrived_ref.at[owner, at.p, :, sides[j]],
            ps.at[owner, j],
            pr.at[owner, j],
            at.plane(target),
        )

    def out_all(owner, j):
        many = slice(1, flat)
        return remote(
            stage_ref.at[owner, many, :, sides[j]],
            arrived_ref.at[owner, many, :, sides[j]],
            ps.at[owner, j],
            pr.at[owner, j],
            at.plane(at.across(1)),
        )

    def back_copy(owner, q, i):
        target = at.across(q)
        return remote(
            made_ref.at[owner, target, :, cuts[i]],
            back_ref.at[owner, at.p, :, cuts[i]],
            bs.at[owner, i],
            br.at[owner, i],
            at.plane(target),
        )

    def back_all(owner, i):
        many = slice(1, flat)
        return remote(
            made_ref.at[owner, many, :, cuts[i]],
            back_ref.at[owner, many, :, cuts[i]],
            bs.at[owner, i],
            br.at[owner, i],
            at.plane(at.across(1)),
        )

    def pass_on(owner, source, j):
        start, stop = sides[j].start, sides[j].stop
        for cut in [cut for cut in cuts if start <= cut.start < stop]:
            picked = jnp.dot(
                select_ref[owner], source[:, cut], preferred_element_type=jnp.float32
            )
            stage_ref[owner, :, :, cut] = picked.reshape(flat, rows, -1).astype(jnp.bfloat16)
        for q in range(1, flat):
            out_copy(owner, q, j).start()
        arrived_ref[owner, at.p, :, sides[j]] = stage_ref[owner, at.p, :, sides[j]]

    def send_back(owner, i):
        for q in range(1, flat):
            back_copy(owner, q, i).start()

    def run_experts(owner):
        for j in range(len(sides)):
            out_all(owner, j).wait_recv()
        for e in range(experts):
            mine = slice(e * cap, (e + 1) * cap)
            block = flatten_rows(arrived_ref[owner, :, mine, :])
            for cut in tiles_of(own_gate.shape[2], 256):
                gate = jnp.dot(block, own_gate[e, :, cut], preferred_element_type=jnp.float32)
                up = jnp.dot(block, own_up[e, :, cut], preferred_element_type=jnp.float32)
                hidden_ref[e, :, cut] = (jax.nn.silu(gate) * up).astype(jnp.bfloat16)
        for i, cut in enumerate(cuts):
            for e in range(experts):
                mine = slice(e * cap, (e + 1) * cap)
                down = jnp.dot(
                    hidden_ref[e], own_down[e, :, cut], preferred_element_type=jnp.float32
                )
                made_ref[owner, :, mine, cut] = down.reshape(flat, cap, -1).astype(jnp.bfloat16)
        back_ref[owner, at.p] = made_ref[owner, at.p]

    def send_all(owner):
        for i in range(len(cuts)):
            send_back(owner, i)

    def mixed(owner, i):
        back_all(owner, i).wait_recv()
        block = flatten_rows(back_ref[owner, :, :, cuts[i]])
        return jnp.dot(mix_ref[owner], block, preferred_element_type=jnp.float32)

    def toward(owner, side, i):
        return remote(
            sent_ref.at[owner, :, cuts[i]],
            came_ref.at[side, owner, :, cuts[i]],
            ss.at[owner, i],
            sr.at[side, owner, i],
            at.column(at.a - 1 + 2 * side),
        )

    def step(owner, side, more):
        for i, cut in enumerate(cuts):
            part = mixed(owner, i)
            if more:
                toward(owner, side, i).wait_recv()
                part = part + came_ref[side, owner, :, cut].astype(jnp.float32)
            sent_ref[owner, :, cut] = part.astype(jnp.bfloat16)
            toward(owner, side, i).start()

    def homeward(turn):
        for place in range(2):
            side = jnp.where(2 * at.a < at.deep, 1 - place, place)
            owner = jnp.where(side == 0, last - turn, turn)
            goes = jnp.where(side == 0, owner < at.a, owner > at.a)
            far = jnp.where(side == 0, has_right, has_left)
            pl.when(goes & far)(lambda owner=owner, side=side: step(owner, side, True))
            pl.when(goes & jnp.logical_not(far))(
                lambda owner=owner, side=side: step(owner, side, False)
            )

    def take(i):
        for j in range(len(sides)):
            relay(x_ref, order[i], 0, j).wait_recv()
            forward(column_ref.at[order[i]], order[i], j)
            pass_on(order[i], column_ref.at[order[i]], j)

    order = [at.nearest(i) for i in range(at.deep)]
    for j in range(len(sides)):
        forward(x_ref, at.a, j)
    for j in range(len(sides)):
        pass_on(at.a, x_ref, j)
    for load in loads[1:4]:
        load.wait()
    for cut in tiles_of(gate_ref.shape[1], 256):
        gate = jnp.dot(x_ref[...], gate_ref[:, cut], preferred_element_type=jnp.float32)
        up = jnp.dot(x_ref[...], up_ref[:, cut], preferred_element_type=jnp.float32)
        shared_ref[:, cut] = (jax.nn.silu(gate) * up).astype(jnp.bfloat16)
    for cut in cuts:
        base_ref[:, cut] = middle_ref[:, cut].astype(jnp.float32) + jnp.dot(
            shared_ref[...], down_ref[:, cut], preferred_element_type=jnp.float32
        )
    for i in range(1, at.deep + 1):
        if i < at.deep:
            take(i)
        if i == 1:
            for load in loads[4:]:
                load.wait()
        if i == at.deep:
            send_all(order[1])
        run_experts(order[i - 1])
    turns = [1, *range(at.deep - 1, 1, -1)]
    for turn in turns[1:]:
        send_all(order[turn])
    send_all(at.a)

    def drain_states(d, carry):
        @pl.when(at.sp + d < count)
        def _():
            for copy in state_copy(d):
                copy.wait_send()

        return carry

    def drain_out(owner, carry):
        for j in range(len(sides)):
            out_all(owner, j).wait_send()
        return carry

    def drain_relay(owner, carry):
        right, left = sends(owner)
        for j in range(len(sides)):
            pl.when(right)(lambda j=j: relay(x_ref, owner, 0, j).wait_send())
            pl.when(left)(lambda j=j: relay(x_ref, owner, 1, j).wait_send())
        return carry

    for d in range(1, at.deep):
        packet_copy(d).wait_send()
    for d in range(1, tps):
        swap_copy(d).wait_send()
    lax.fori_loop(1, count, drain_states, 0)
    lax.fori_loop(0, at.deep, drain_relay, 0)
    lax.fori_loop(0, at.deep, drain_out, 0)
    for turn in turns:
        homeward(turn)

    for side, far in ((0, has_right), (1, has_left)):

        @pl.when(far)
        def _(side=side):
            for i, cut in enumerate(cuts):
                toward(at.a, side, i).wait_recv()
                base_ref[:, cut] += came_ref[side, at.a, :, cut].astype(jnp.float32)

    for i, cut in enumerate(cuts):
        out_ref[:, cut] = (base_ref[:, cut] + mixed(at.a, i)).astype(out_ref.dtype)
    def drain_back(owner, carry):
        for j in range(len(cuts)):
            back_all(owner, j).wait_send()
        return carry

    def drain_home(owner, carry):
        for j in range(len(cuts)):
            pl.when(owner != at.a)(lambda j=j: toward(owner, 0, j).wait_send())
        return carry

    lax.fori_loop(0, at.deep, drain_back, 0)
    lax.fori_loop(0, at.deep, drain_home, 0)


def on_device(
    queries,
    key_matrix,
    value_matrix,
    channel_decay_input,
    head_decay_offset,
    output_gate_input,
    head_norm_gain,
    residual,
    mixer_output_weight,
    expert_norm_gain,
    routes,
    chosen_router_scores,
    routed_gate_weight,
    routed_up_weight,
    routed_down_weight,
    common_gate_weight,
    common_up_weight,
    common_down_weight,
):
    count, tps = sizes = (lax.axis_size("sp"), lax.axis_size("tp"))
    at = Place(*sizes)
    tokens, width = residual.shape
    length, lanes = queries.shape
    heads = head_decay_offset.shape[1]
    blocks = length // BLOCK
    experts = routed_gate_weight.shape[0]
    cap = 2 * TOP_K * tokens // (experts * count * tps)
    rows = experts * cap
    slots = at.flat * rows
    parts, halves = len(tiles_of(width)), len(tiles_of(width, 1024))
    common = (common_gate_weight, common_up_weight, common_down_weight)
    routed = (routed_gate_weight, routed_up_weight, routed_down_weight)
    box = (at.deep, at.flat, rows, width)
    chunk = (at.deep, tokens, width)
    dma = pltpu.SemaphoreType.DMA
    half, wide = jnp.bfloat16, jnp.float32
    vmem = pl.BlockSpec(memory_space=pltpu.VMEM)
    far = pl.BlockSpec(memory_space=pl.ANY)
    return pl.pallas_call(
        functools.partial(layer_kernel, sizes),
        out_shape=pltpu.VMEM((tokens, width), half),
        in_specs=[vmem] * 11 + [far] * 7,
        out_specs=vmem,
        scratch_shapes=[
            pltpu.VMEM((length, lanes), wide),
            pltpu.VMEM((heads, length, lanes), half),
            pltpu.VMEM((length, lanes), half),
            pltpu.VMEM((max(8, blocks), lanes), wide),
            pltpu.VMEM((blocks, VDIM, lanes), half),
            pltpu.VMEM((length, heads * VDIM), wide),
            pltpu.VMEM((VDIM, lanes), half),
            pltpu.VMEM((8, lanes), wide),
            pltpu.VMEM((count, VDIM, lanes), half),
            pltpu.VMEM((count, 8, lanes), wide),
            pltpu.VMEM((VDIM, lanes), wide),
            pltpu.VMEM((8, lanes), wide),
            pltpu.VMEM((2 * TOP_K, tokens), wide),
            pltpu.VMEM((at.deep, 2 * TOP_K, tokens), wide),
            pltpu.VMEM((tps, tokens, heads * VDIM), half),
            pltpu.VMEM((tps, tokens, heads * VDIM), half),
            pltpu.VMEM(mixer_output_weight.shape, half),
            pltpu.VMEM((tokens, width), half),
            pltpu.VMEM((tokens, width), half),
            pltpu.VMEM((at.deep, slots, tokens), half),
            pltpu.VMEM((at.deep, tokens, slots), half),
            pltpu.VMEM(chunk, half),
            pltpu.VMEM(box, half),
            pltpu.VMEM(box, half),
            pltpu.VMEM(box, half),
            pltpu.VMEM(box, half),
            pltpu.VMEM(chunk, half),
            pltpu.VMEM((2,) + chunk, half),
            pltpu.VMEM((tokens, width), wide),
            pltpu.VMEM((experts, at.flat * cap, routed[0].shape[2]), half),
            pltpu.VMEM((tokens, common[0].shape[1]), half),
            pltpu.VMEM(common[0].shape, half),
            pltpu.VMEM(common[1].shape, half),
            pltpu.VMEM(common[2].shape, half),
            pltpu.VMEM(routed[0].shape, half),
            pltpu.VMEM(routed[1].shape, half),
            pltpu.VMEM(routed[2].shape, half),
            dma((7,)),
            dma((at.deep,)),
            dma((at.deep,)),
            dma((count,)),
            dma((count,)),
            dma((count,)),
            dma((count,)),
            dma((tps,)),
            dma((tps,)),
            dma((2, at.deep, halves)),
            dma((at.deep, halves)),
            dma((at.deep, halves)),
            dma((at.deep, halves)),
            dma((at.deep, parts)),
            dma((at.deep, parts)),
            dma((at.deep, parts)),
            dma((2, at.deep, parts)),
        ],
        compiler_params=pltpu.CompilerParams(
            collective_id=0, has_side_effects=True, vmem_limit_bytes=62 * 1024 * 1024
        ),
    )(
        queries,
        key_matrix,
        value_matrix,
        channel_decay_input,
        head_decay_offset.T,
        output_gate_input,
        head_norm_gain.reshape(1, -1),
        residual,
        expert_norm_gain.reshape(1, -1),
        routes.T,
        chosen_router_scores.T,
        mixer_output_weight,
        *common,
        *routed,
    )


def solution(mesh):
    placed = (
        P("sp", "tp"),
        P("sp", "tp"),
        P("sp", "tp"),
        P("sp", "tp"),
        P("sp", "tp"),
        P("sp", "tp"),
        P(),
        P(("sp", "tp"), None),
        P(),
        P(),
        P(("sp", "tp"), None),
        P(("sp", "tp"), None),
        P(("sp", "tp"), None, None),
        P(("sp", "tp"), None, None),
        P(("sp", "tp"), None, None),
        P(),
        P(),
        P(),
    )
    return jax.shard_map(
        on_device, mesh=mesh, in_specs=placed, out_specs=P(("sp", "tp"), None), check_vma=False
    )
```

```python
import functools
import math

import jax
import jax.numpy as jnp
from jax import lax
from jax.experimental import pallas as pl
from jax.experimental.pallas import tpu as pltpu
from jax.sharding import PartitionSpec as P

D = 2048
KEY_CHANNELS = 64
VDIM = 128
BLOCK = 64
TOP_K = 4


eps_norm = 1e-06
decay_running = 16.0
routed_scale = 2.5


def peer(sp, tp):
    return {"sp": sp, "tp": tp}


def call_on(targets):
    barrier = pltpu.get_barrier_semaphore()
    for target in targets:
        pl.semaphore_signal(
            barrier, inc=1, device_id=target, device_id_type=pl.DeviceIdType.MESH
        )
    return lambda: pl.semaphore_wait(barrier, len(targets))


def remote(src, dst, send, recv, target):
    return pltpu.make_async_remote_copy(
        src_ref=src,
        dst_ref=dst,
        send_sem=send,
        recv_sem=recv,
        device_id=target,
        device_id_type=pl.DeviceIdType.MESH,
    )


def dot_nt(a, b):
    return lax.dot_general(a, b, (((1,), (1,)), ((), ())), preferred_element_type=jnp.float32)


def dot_tn(a, b):
    return lax.dot_general(a, b, (((0,), (0,)), ((), ())), preferred_element_type=jnp.float32)


def dot_nn(a, b):
    return jnp.dot(a, b, preferred_element_type=jnp.float32)


def exact_dot(ones, values, dot):
    total = 0.0
    for _ in range(3):
        part = values.astype(jnp.bfloat16)
        values = values - part.astype(jnp.float32)
        total = total + dot(ones, part)
    return total


class Place:
    def __init__(self, sp_size, tp_size):
        self.deep = math.gcd(sp_size, 4)
        self.rows = sp_size // self.deep
        self.tp_size = tp_size
        self.flat = self.rows * tp_size

    def here(self):
        sp, tp = lax.axis_index("sp"), lax.axis_index("tp")
        self.sp, self.tp = sp, tp
        self.a = sp // self.rows
        self.b = lax.rem(sp, self.rows)
        self.p = self.b * self.tp_size + tp
        return self

    def column(self, a):
        return peer(a * self.rows + self.b, self.tp)

    def plane(self, p):
        return peer(self.a * self.rows + p // self.tp_size, lax.rem(p, self.tp_size))

    def across(self, q):
        return lax.rem(self.p + q, self.flat)

    def nearest(self, i):
        last = self.deep - 1
        low = self.a < last - self.a
        span = jnp.where(low, self.a, last - self.a)
        away = (i + 1) // 2 if i % 2 else -(i // 2)
        zigzag = jnp.where(low, self.a - away, self.a + away)
        return jnp.where(i <= 2 * span, zigzag, jnp.where(low, i, last - i))


def tiles_of(width, most=512):
    step = math.gcd(width, most)
    return [slice(i, i + step) for i in range(0, width, step)]


def flatten_rows(block):
    groups, rows, width = block.shape
    if rows % 16 == 0:
        return block.reshape(groups * rows, width)
    return block.astype(jnp.float32).reshape(groups * rows, width).astype(jnp.bfloat16)


def layer_kernel(
    sizes, far_q, k_ref, v_ref, decay_ref, offset_ref, far_open, head_gain_ref, far_residual,
    gain_ref, routes_ref, scores_ref, far_mix, far_gate, far_up, far_down,
    wide_gate, wide_up, wide_down, out_ref,
    q_ref, open_ref, residual_ref, qd_ref, qx_ref, kt_ref, ends_ref, starts_ref, inner_ref, state_ref,
    states_ref, carried_ref, reach_ref, packet_ref, packets_ref, gated_ref, swapped_ref,
    mixer_ref, x_ref, middle_ref, select_ref, mix_ref,
    column_ref, stage_ref, arrived_ref, made_ref, back_ref, sent_ref, came_ref, base_ref,
    hidden_ref, shared_ref, gate_ref, up_ref, down_ref, own_gate, own_up, own_down,
    weight_sem, ks, kr, gs, gr, ws, wr, zs, zr, ps, pr, bs, br, ss, sr,
):
    at = Place(*sizes).here()
    last = at.deep - 1
    flat, rows = stage_ref.shape[1], stage_ref.shape[2]
    width = x_ref.shape[1]
    experts = own_gate.shape[0]
    cap = rows // experts
    cuts = tiles_of(width)
    sides = tiles_of(width, 1024)
    pairs = (
        (far_q, q_ref), (far_open, open_ref), (far_residual, residual_ref),
        (far_mix, mixer_ref), (far_gate, gate_ref), (far_up, up_ref), (far_down, down_ref),
        (wide_gate, own_gate), (wide_up, own_up), (wide_down, own_down),
    )
    loads = [
        pltpu.make_async_copy(src, dst, weight_sem.at[i]) for i, (src, dst) in enumerate(pairs)
    ]
    for load in loads:
        load.start()
    has_right, has_left = at.a < last, at.a > 0
    count, tps = sizes
    met = call_on(
        [peer(lax.rem(at.sp + d, count), at.tp) for d in range(1, count)]
        + [at.plane(at.across(q)) for q in range(1, flat)]
    )
    half, wide = jnp.bfloat16, jnp.float32
    length, lanes = q_ref.shape
    heads = offset_ref.shape[0]
    blocks = length // BLOCK
    tokens = x_ref.shape[0]
    lane = lax.broadcasted_iota(jnp.int32, (1, lanes), 1)
    of_head = [
        (lane >= h * KEY_CHANNELS) & (lane < (h + 1) * KEY_CHANNELS) for h in range(heads)
    ]
    columns = [slice(h * VDIM, (h + 1) * VDIM) for h in range(heads)]
    tile = math.gcd(length, 4 * BLOCK)
    row = lax.broadcasted_iota(jnp.int32, (tile, tile), 0)
    col = lax.broadcasted_iota(jnp.int32, (tile, tile), 1)
    causal = (jnp.bitwise_and(row, -BLOCK) == jnp.bitwise_and(col, -BLOCK)) & (col <= row)
    ones = jnp.where(causal, 1.0, 0.0).astype(half)

    for t in range(0, length, tile):
        span = slice(t, t + tile)
        pre = decay_ref[span, :].astype(wide)
        log_decay = (
            jnp.minimum(pre, 0.0) - jnp.log1p(jnp.exp(-jnp.abs(pre)))
        ) / decay_running
        dropped = exact_dot(ones, offset_ref[:, span], dot_nt)
        offset = dropped[:, 0:1]
        for h in range(1, heads):
            offset = jnp.where(of_head[h], dropped[:, h : h + 1], offset)
        within = exact_dot(ones, log_decay, dot_nn) + offset
        keys = k_ref[span, :].astype(wide)
        qd_ref[span, :] = within
        for n in range(0, tile, BLOCK):
            inside = slice(n, n + BLOCK)
            end = within[n + BLOCK - 1 : n + BLOCK, :]
            kt_ref[t + n : t + n + BLOCK, :] = (
                keys[inside, :] * jnp.exp(end - within[inside, :])
            ).astype(half)
            ends_ref[(t + n) // BLOCK : (t + n) // BLOCK + 1, :] = end
    state = jnp.zeros((VDIM, lanes), wide)
    passed = jnp.zeros((1, lanes), wide)
    for n in range(blocks):
        span = slice(n * BLOCK, (n + 1) * BLOCK)
        starts_ref[n] = state.astype(half)
        end = ends_ref[n : n + 1, :]
        both = dot_tn(v_ref[span, :], kt_ref[span, :])
        added = both[columns[0], :]
        for h in range(1, heads):
            added = jnp.where(of_head[h], both[columns[h], :], added)
        state = state * jnp.exp(end) + added
        passed = passed + end
    state_ref[:VDIM, :] = state.astype(half)
    index = lax.broadcasted_iota(jnp.int32, (16, lanes), 0)
    pieces = jnp.zeros((16, lanes), wide)
    for i in range(3):
        piece = passed.astype(half).astype(wide)
        pieces = jnp.where(index == i, piece, pieces)
        passed = passed - piece
    state_ref[VDIM:, :] = pieces.astype(half)
    def packet_copy(d):
        return remote(
            packet_ref,
            packets_ref.at[at.a],
            ks.at[d],
            kr.at[at.a],
            at.column(lax.rem(at.a + d, at.deep)),
        )

    def packet_from(a):
        return remote(packet_ref, packets_ref.at[a], ks.at[0], kr.at[a], at.column(at.a))

    def state_copy(d):
        target = peer(jnp.minimum(at.sp + d, count - 1), at.tp)
        return remote(state_ref, states_ref.at[at.sp], gs.at[d], gr.at[at.sp], target)

    def swap_copy(d):
        to = lax.rem(at.tp + d, tps)
        return remote(
            gated_ref.at[to], swapped_ref.at[at.tp], ws.at[d], wr.at[at.tp], peer(at.sp, to)
        )

    packet_ref[:TOP_K, :] = routes_ref[...].astype(wide)
    packet_ref[TOP_K:, :] = scores_ref[...]
    packets_ref[at.a] = packet_ref[...]
    met()
    for d in range(1, at.deep):
        packet_copy(d).start()
    for d in range(1, count):

        @pl.when(at.sp + d < count)
        def _(d=d):
            state_copy(d).start()

    loads[0].wait()
    for t in range(0, length, tile):
        span = slice(t, t + tile)
        within = qd_ref[span, :]
        grown = k_ref[span, :].astype(wide) * jnp.exp(-within)
        ahead = q_ref[span, :].astype(wide) * KEY_CHANNELS ** (-0.5) * jnp.exp(within)
        qd_ref[span, :] = ahead
        ahead = ahead.astype(half)
        for h in range(heads):
            kept = jnp.where(of_head[h], grown, 0.0).astype(half)
            scores = jnp.where(causal, dot_nt(ahead, kept), 0.0)
            inner_ref[span, columns[h]] = jnp.dot(
                scores.astype(half), v_ref[span, columns[h]], preferred_element_type=wide
            )
    passed = jnp.zeros((1, lanes), wide)
    for n in range(blocks):
        span = slice(n * BLOCK, (n + 1) * BLOCK)
        for h in range(heads):
            ahead = jnp.where(of_head[h], qd_ref[span, :], 0.0)
            qx_ref[h, span, :] = (ahead * jnp.exp(passed)).astype(half)
            if n > 0:
                inner_ref[span, columns[h]] += dot_nt(ahead.astype(half), starts_ref[n])
        passed = passed + ends_ref[n : n + 1, :]

    slots = flat * rows
    plane_experts = flat * experts
    here = lax.broadcasted_iota(jnp.int32, (slots, plane_experts), 0)
    there = lax.broadcasted_iota(jnp.int32, (slots, plane_experts), 1) * cap
    belongs = (here >= there) & (here < there + cap)
    spread = jnp.where(belongs, 1.0, 0.0).astype(half)
    place = jnp.sum(
        jnp.where(belongs, (here - there).astype(wide), 0.0), axis=1, keepdims=True
    )
    expert = (
        at.a * plane_experts + lax.broadcasted_iota(jnp.int32, (plane_experts, 1), 0)
    ).astype(wide)
    sooner = jnp.where(
        lax.broadcasted_iota(jnp.int32, (tokens, tokens), 0)
        < lax.broadcasted_iota(jnp.int32, (tokens, tokens), 1),
        1.0,
        0.0,
    ).astype(half)
    def lay_out(a):
        pl.when(at.a != a)(lambda a=a: packet_from(a).wait_recv())
        scored = packets_ref[a, TOP_K:, :]
        share = routed_scale * scored / jnp.sum(scored, axis=0, keepdims=True)
        chosen = jnp.zeros((plane_experts, tokens), wide)
        weight_of = jnp.zeros((plane_experts, tokens), wide)
        for k in range(TOP_K):
            hit = packets_ref[a, k : k + 1, :] == expert
            chosen = jnp.where(hit, 1.0, chosen)
            weight_of = jnp.where(hit, share[k : k + 1, :], weight_of)
        rank = jnp.dot(chosen.astype(half), sooner, preferred_element_type=wide)
        rank = jnp.where(chosen > 0.0, rank, -1.0)
        ranks = jnp.dot(spread, rank.astype(half), preferred_element_type=wide)
        weights = jnp.dot(spread, weight_of.astype(half), preferred_element_type=wide)
        taken = ranks == place
        select_ref[a] = jnp.where(taken, 1.0, 0.0).astype(half)
        mix_ref[a] = jnp.transpose(jnp.where(taken, weights, 0.0)).astype(half)

    early = at.deep // 2
    for a in range(early):
        lay_out(a)

    carried_ref[...] = jnp.zeros_like(carried_ref)
    reach_ref[...] = jnp.zeros_like(reach_ref)
    for j in reversed(range(count - 1)):

        @pl.when(j < at.sp)
        def _(j=j):
            source = peer(j, at.tp)
            remote(state_ref, states_ref.at[j], gs.at[0], gr.at[j], source).wait_recv()
            carried_ref[...] += jnp.exp(reach_ref[0:1, :]) * states_ref[j, :VDIM, :].astype(wide)
            log = jnp.sum(states_ref[j, VDIM:, :].astype(wide), axis=0, keepdims=True)
            reach_ref[0:1, :] += log

    carried = carried_ref[...].astype(half)
    loads[1].wait()
    for d in [*sorted(range(1, tps), key=lambda d: abs(2 * d - tps)), 0]:
        to = lax.rem(at.tp + d, tps)
        span = pl.ds(pl.multiple_of(to * tokens, tokens), tokens)
        for h in range(heads):
            output = inner_ref[span, columns[h]] + dot_nt(qx_ref[h, span, :], carried)
            inv_rms = lax.rsqrt(jnp.mean(output * output, axis=-1, keepdims=True) + eps_norm)
            gated_ref[to, :, columns[h]] = (
                output
                * inv_rms
                * head_gain_ref[...]
                * jax.nn.silu(open_ref[span, columns[h]].astype(wide))
            ).astype(half)
        if d > 0:
            swap_copy(d).start()
    for a in range(early, at.deep):
        lay_out(a)
    for load in loads[2:4]:
        load.wait()
    span = heads * VDIM
    for d in range(tps):
        source = lax.rem(at.tp - d + tps, tps)
        if d > 0:
            remote(
                gated_ref.at[0], swapped_ref.at[source], ws.at[0], wr.at[source], peer(at.sp, source)
            ).wait_recv()
        piece = gated_ref[source] if d == 0 else swapped_ref[source]
        part_of = pl.ds(pl.multiple_of(source * span, span), span)
        for cut in cuts:
            part = jnp.dot(piece, mixer_ref[part_of, cut], preferred_element_type=wide)
            if d == 0:
                base_ref[:, cut] = residual_ref[:, cut].astype(wide) + part
            else:
                base_ref[:, cut] += part
    square = jnp.zeros((tokens, 1), wide)
    for cut in cuts:
        middle_ref[:, cut] = base_ref[:, cut].astype(half)
        middle = middle_ref[:, cut].astype(wide)
        square = square + jnp.sum(middle * middle, axis=-1, keepdims=True)
    scale = lax.rsqrt(square / width + eps_norm)
    for cut in cuts:
        x_ref[:, cut] = (middle_ref[:, cut].astype(wide) * scale * gain_ref[:, cut]).astype(half)

    def relay(source, owner, side, j):
        return remote(
            source.at[:, sides[j]],
            column_ref.at[owner, :, sides[j]],
            zs.at[side, owner],
            zr.at[owner, j],
            at.column(at.a + (1 if side == 0 else -1)),
        )

    def sends(owner):
        right = has_right & (owner <= at.a)
        left = has_left & (owner >= at.a)
        return right, left

    def forward(source, owner, j):
        right, left = sends(owner)
        pl.when(right)(lambda: relay(source, owner, 0, j).start())
        pl.when(left)(lambda: relay(source, owner, 1, j).start())

    def out_copy(owner, q, j):
        target = at.across(q)
        return remote(
            stage_ref.at[owner, target, :, sides[j]],
            arrived_ref.at[owner, at.p, :, sides[j]],
            ps.at[owner],
            pr.at[owner, j],
            at.plane(target),
        )

    def out_all(owner, j):
        many = slice(1, flat)
        return remote(
            stage_ref.at[owner, many, :, sides[j]],
            arrived_ref.at[owner, many, :, sides[j]],
            ps.at[owner],
            pr.at[owner, j],
            at.plane(at.across(1)),
        )

    def back_copy(owner, q, i):
        target = at.across(q)
        return remote(
            made_ref.at[owner, target, :, cuts[i]],
            back_ref.at[owner, at.p, :, cuts[i]],
            bs.at[owner],
            br.at[owner, i],
            at.plane(target),
        )

    def back_all(owner, i):
        many = slice(1, flat)
        return remote(
            made_ref.at[owner, many, :, cuts[i]],
            back_ref.at[owner, many, :, cuts[i]],
            bs.at[owner],
            br.at[owner, i],
            at.plane(at.across(1)),
        )

    def pass_on(owner, source, j):
        start, stop = sides[j].start, sides[j].stop
        for cut in [cut for cut in cuts if start <= cut.start < stop]:
            picked = jnp.dot(
                select_ref[owner], source[:, cut], preferred_element_type=jnp.float32
            )
            stage_ref[owner, :, :, cut] = picked.reshape(flat, rows, -1).astype(jnp.bfloat16)
        for q in range(1, flat):
            out_copy(owner, q, j).start()
        arrived_ref[owner, at.p, :, sides[j]] = stage_ref[owner, at.p, :, sides[j]]

    def send_back(owner, i):
        for q in range(1, flat):
            back_copy(owner, q, i).start()

    def run_experts(owner):
        for j in range(len(sides)):
            out_all(owner, j).wait_recv()
        for e in range(experts):
            mine = slice(e * cap, (e + 1) * cap)
            block = flatten_rows(arrived_ref[owner, :, mine, :])
            for cut in tiles_of(own_gate.shape[2], 256):
                gate = jnp.dot(block, own_gate[e, :, cut], preferred_element_type=jnp.float32)
                up = jnp.dot(block, own_up[e, :, cut], preferred_element_type=jnp.float32)
                hidden_ref[e, :, cut] = (jax.nn.silu(gate) * up).astype(jnp.bfloat16)
        for i, cut in enumerate(cuts):
            for e in range(experts):
                mine = slice(e * cap, (e + 1) * cap)
                down = jnp.dot(
                    hidden_ref[e], own_down[e, :, cut], preferred_element_type=jnp.float32
                )
                made_ref[owner, :, mine, cut] = down.reshape(flat, cap, -1).astype(jnp.bfloat16)
        back_ref[owner, at.p] = made_ref[owner, at.p]

    def send_all(owner):
        for i in range(len(cuts)):
            send_back(owner, i)

    def mixed(owner, i):
        back_all(owner, i).wait_recv()
        block = flatten_rows(back_ref[owner, :, :, cuts[i]])
        return jnp.dot(mix_ref[owner], block, preferred_element_type=jnp.float32)

    def toward(owner, side, i):
        return remote(
            sent_ref.at[owner, :, cuts[i]],
            came_ref.at[side, owner, :, cuts[i]],
            ss.at[owner],
            sr.at[side, owner, i],
            at.column(at.a - 1 + 2 * side),
        )

    def step(owner, side, more, i):
        part = mixed(owner, i)
        if more:
            toward(owner, side, i).wait_recv()
            part = part + came_ref[side, owner, :, cuts[i]].astype(jnp.float32)
        sent_ref[owner, :, cuts[i]] = part.astype(jnp.bfloat16)
        toward(owner, side, i).start()

    def homeward(turn, place, i):
        side = jnp.where(2 * at.a < at.deep, 1 - place, place)
        owner = jnp.where(side == 0, last - turn, turn)
        goes = jnp.where(side == 0, owner < at.a, owner > at.a)
        far = jnp.where(side == 0, has_right, has_left)
        pl.when(goes & far)(lambda: step(owner, side, True, i))
        pl.when(goes & jnp.logical_not(far))(lambda: step(owner, side, False, i))

    def take(i):
        for j in range(len(sides)):
            relay(x_ref, order[i], 0, j).wait_recv()
            forward(column_ref.at[order[i]], order[i], j)
            pass_on(order[i], column_ref.at[order[i]], j)

    order = [at.nearest(i) for i in range(at.deep)]
    for j in range(len(sides)):
        forward(x_ref, at.a, j)
    for j in range(len(sides)):
        pass_on(at.a, x_ref, j)
    for load in loads[4:7]:
        load.wait()
    for cut in tiles_of(gate_ref.shape[1], 256):
        gate = jnp.dot(x_ref[...], gate_ref[:, cut], preferred_element_type=jnp.float32)
        up = jnp.dot(x_ref[...], up_ref[:, cut], preferred_element_type=jnp.float32)
        shared_ref[:, cut] = (jax.nn.silu(gate) * up).astype(jnp.bfloat16)
    for cut in cuts:
        base_ref[:, cut] = middle_ref[:, cut].astype(jnp.float32) + jnp.dot(
            shared_ref[...], down_ref[:, cut], preferred_element_type=jnp.float32
        )
    turns = [*range(2, at.deep), 1]
    early = [turn for turn in turns[:1] if turn < at.deep - 1]
    for i in range(1, at.deep + 1):
        if i < at.deep:
            take(i)
        if i == 1:
            for load in loads[7:]:
                load.wait()
        if i == at.deep:
            for turn in early:
                send_all(order[turn])
        run_experts(order[i - 1])
    for turn in turns[len(early) :]:
        send_all(order[turn])
    send_all(at.a)

    def sent_all(source, target, sent, came):
        remote(source, target, sent, came, at.plane(at.across(1))).wait_send()

    def drain_states(d, carry):
        @pl.when(at.sp + d < count)
        def _():
            state_copy(d).wait_send()

        return carry

    def drain_out(owner, carry):
        sent_all(stage_ref.at[owner, 1:], arrived_ref.at[owner, 1:], ps.at[owner], pr.at[owner, 0])
        return carry

    def drain_relay(owner, carry):
        for side, goes in enumerate(sends(owner)):

            @pl.when(goes)
            def _(side=side):
                sent_all(x_ref, column_ref.at[owner], zs.at[side, owner], zr.at[owner, 0])

        return carry

    for d in range(1, at.deep):
        packet_copy(d).wait_send()
    for d in range(1, tps):
        swap_copy(d).wait_send()
    lax.fori_loop(1, count, drain_states, 0)
    lax.fori_loop(0, at.deep, drain_relay, 0)
    lax.fori_loop(0, at.deep, drain_out, 0)
    for turn, later in zip(turns, [*turns[1:], None]):
        if turn == turns[0]:
            for i in range(len(cuts)):
                homeward(turn, 0, i)
        for i in range(len(cuts)):
            homeward(turn, 1, i)
            if later is not None:
                homeward(later, 0, i)

    for side, far in ((0, has_right), (1, has_left)):

        @pl.when(far)
        def _(side=side):
            for i, cut in enumerate(cuts):
                toward(at.a, side, i).wait_recv()
                base_ref[:, cut] += came_ref[side, at.a, :, cut].astype(jnp.float32)

    for i, cut in enumerate(cuts):
        out_ref[:, cut] = (base_ref[:, cut] + mixed(at.a, i)).astype(out_ref.dtype)
    def drain_back(owner, carry):
        sent_all(made_ref.at[owner, 1:], back_ref.at[owner, 1:], bs.at[owner], br.at[owner, 0])
        return carry

    def drain_home(owner, carry):
        @pl.when(owner != at.a)
        def _():
            sent_all(sent_ref.at[owner], came_ref.at[0, owner], ss.at[owner], sr.at[0, owner, 0])

        return carry

    lax.fori_loop(0, at.deep, drain_back, 0)
    lax.fori_loop(0, at.deep, drain_home, 0)


def on_device(
    queries,
    key_matrix,
    value_matrix,
    channel_decay_input,
    head_decay_offset,
    output_gate_input,
    head_norm_gain,
    residual,
    mixer_output_weight,
    expert_norm_gain,
    routes,
    chosen_router_scores,
    routed_gate_weight,
    routed_up_weight,
    routed_down_weight,
    common_gate_weight,
    common_up_weight,
    common_down_weight,
):
    count, tps = sizes = (lax.axis_size("sp"), lax.axis_size("tp"))
    at = Place(*sizes)
    tokens, width = residual.shape
    length, lanes = queries.shape
    heads = head_decay_offset.shape[1]
    blocks = length // BLOCK
    experts = routed_gate_weight.shape[0]
    cap = 2 * TOP_K * tokens // (experts * count * tps)
    rows = experts * cap
    slots = at.flat * rows
    parts, halves = len(tiles_of(width)), len(tiles_of(width, 1024))
    common = (common_gate_weight, common_up_weight, common_down_weight)
    routed = (routed_gate_weight, routed_up_weight, routed_down_weight)
    box = (at.deep, at.flat, rows, width)
    chunk = (at.deep, tokens, width)
    dma = pltpu.SemaphoreType.DMA
    half, wide = jnp.bfloat16, jnp.float32
    vmem = pl.BlockSpec(memory_space=pltpu.VMEM)
    far = pl.BlockSpec(memory_space=pl.ANY)
    return pl.pallas_call(
        functools.partial(layer_kernel, sizes),
        out_shape=pltpu.VMEM((tokens, width), half),
        in_specs=[far] + [vmem] * 4 + [far, vmem, far] + [vmem] * 3 + [far] * 7,
        out_specs=vmem,
        scratch_shapes=[
            pltpu.VMEM(queries.shape, half),
            pltpu.VMEM(output_gate_input.shape, half),
            pltpu.VMEM(residual.shape, half),
            pltpu.VMEM((length, lanes), wide),
            pltpu.VMEM((heads, length, lanes), half),
            pltpu.VMEM((length, lanes), half),
            pltpu.VMEM((max(8, blocks), lanes), wide),
            pltpu.VMEM((blocks, VDIM, lanes), half),
            pltpu.VMEM((length, heads * VDIM), wide),
            pltpu.VMEM((VDIM + 16, lanes), half),
            pltpu.VMEM((count, VDIM + 16, lanes), half),
            pltpu.VMEM((VDIM, lanes), wide),
            pltpu.VMEM((8, lanes), wide),
            pltpu.VMEM((2 * TOP_K, tokens), wide),
            pltpu.VMEM((at.deep, 2 * TOP_K, tokens), wide),
            pltpu.VMEM((tps, tokens, heads * VDIM), half),
            pltpu.VMEM((tps, tokens, heads * VDIM), half),
            pltpu.VMEM(mixer_output_weight.shape, half),
            pltpu.VMEM((tokens, width), half),
            pltpu.VMEM((tokens, width), half),
            pltpu.VMEM((at.deep, slots, tokens), half),
            pltpu.VMEM((at.deep, tokens, slots), half),
            pltpu.VMEM(chunk, half),
            pltpu.VMEM(box, half),
            pltpu.VMEM(box, half),
            pltpu.VMEM(box, half),
            pltpu.VMEM(box, half),
            pltpu.VMEM(chunk, half),
            pltpu.VMEM((2,) + chunk, half),
            pltpu.VMEM((tokens, width), wide),
            pltpu.VMEM((experts, at.flat * cap, routed[0].shape[2]), half),
            pltpu.VMEM((tokens, common[0].shape[1]), half),
            pltpu.VMEM(common[0].shape, half),
            pltpu.VMEM(common[1].shape, half),
            pltpu.VMEM(common[2].shape, half),
            pltpu.VMEM(routed[0].shape, half),
            pltpu.VMEM(routed[1].shape, half),
            pltpu.VMEM(routed[2].shape, half),
            dma((10,)),
            dma((at.deep,)),
            dma((at.deep,)),
            dma((count,)),
            dma((count,)),
            dma((tps,)),
            dma((tps,)),
            dma((2, at.deep)),
            dma((at.deep, halves)),
            dma((at.deep,)),
            dma((at.deep, halves)),
            dma((at.deep,)),
            dma((at.deep, parts)),
            dma((at.deep,)),
            dma((2, at.deep, parts)),
        ],
        compiler_params=pltpu.CompilerParams(
            collective_id=0, has_side_effects=True, vmem_limit_bytes=62 * 1024 * 1024
        ),
    )(
        queries,
        key_matrix,
        value_matrix,
        channel_decay_input,
        head_decay_offset.T,
        output_gate_input,
        head_norm_gain.reshape(1, -1),
        residual,
        expert_norm_gain.reshape(1, -1),
        routes.T,
        chosen_router_scores.T,
        mixer_output_weight,
        *common,
        *routed,
    )


def solution(mesh):
    placed = (
        P("sp", "tp"),
        P("sp", "tp"),
        P("sp", "tp"),
        P("sp", "tp"),
        P("sp", "tp"),
        P("sp", "tp"),
        P(),
        P(("sp", "tp"), None),
        P(),
        P(),
        P(("sp", "tp"), None),
        P(("sp", "tp"), None),
        P(("sp", "tp"), None, None),
        P(("sp", "tp"), None, None),
        P(("sp", "tp"), None, None),
        P(),
        P(),
        P(),
    )
    return jax.shard_map(
        on_device, mesh=mesh, in_specs=placed, out_specs=P(("sp", "tp"), None), check_vma=False
    )
```

```python
import functools
import math

import jax
import jax.numpy as jnp
from jax import lax
from jax.experimental import pallas as pl
from jax.experimental.pallas import tpu as pltpu
from jax.sharding import PartitionSpec as P

D = 2048
KEY_CHANNELS = 64
VDIM = 128
BLOCK = 64
TOP_K = 4


eps_norm = 1e-06
decay_running = 16.0
routed_scale = 2.5


def peer(sp, tp):
    return {"sp": sp, "tp": tp}


def call_on(targets):
    barrier = pltpu.get_barrier_semaphore()
    for target in targets:
        pl.semaphore_signal(
            barrier, inc=1, device_id=target, device_id_type=pl.DeviceIdType.MESH
        )
    return lambda: pl.semaphore_wait(barrier, len(targets))


def remote(src, dst, send, recv, target):
    return pltpu.make_async_remote_copy(
        src_ref=src,
        dst_ref=dst,
        send_sem=send,
        recv_sem=recv,
        device_id=target,
        device_id_type=pl.DeviceIdType.MESH,
    )


def dot_nt(a, b):
    return lax.dot_general(a, b, (((1,), (1,)), ((), ())), preferred_element_type=jnp.float32)


def dot_tn(a, b):
    return lax.dot_general(a, b, (((0,), (0,)), ((), ())), preferred_element_type=jnp.float32)


def dot_nn(a, b):
    return jnp.dot(a, b, preferred_element_type=jnp.float32)


def exact_dot(ones, values, dot):
    total = 0.0
    for _ in range(3):
        part = values.astype(jnp.bfloat16)
        values = values - part.astype(jnp.float32)
        total = total + dot(ones, part)
    return total


class Place:
    def __init__(self, sp_size, tp_size):
        self.deep = math.gcd(sp_size, 4)
        self.rows = sp_size // self.deep
        self.tp_size = tp_size
        self.flat = self.rows * tp_size

    def here(self):
        sp, tp = lax.axis_index("sp"), lax.axis_index("tp")
        self.sp, self.tp = sp, tp
        self.a = sp // self.rows
        self.b = lax.rem(sp, self.rows)
        self.p = self.b * self.tp_size + tp
        return self

    def column(self, a):
        return peer(a * self.rows + self.b, self.tp)

    def plane(self, p):
        return peer(self.a * self.rows + p // self.tp_size, lax.rem(p, self.tp_size))

    def across(self, q):
        return lax.rem(self.p + q, self.flat)

    def nearest(self, i):
        last = self.deep - 1
        low = self.a < last - self.a
        span = jnp.where(low, self.a, last - self.a)
        away = (i + 1) // 2 if i % 2 else -(i // 2)
        zigzag = jnp.where(low, self.a - away, self.a + away)
        return jnp.where(i <= 2 * span, zigzag, jnp.where(low, i, last - i))


def tiles_of(width, most=512):
    step = math.gcd(width, most)
    return [slice(i, i + step) for i in range(0, width, step)]


def flatten_rows(block):
    groups, rows, width = block.shape
    if rows % 16 == 0:
        return block.reshape(groups * rows, width)
    return block.astype(jnp.float32).reshape(groups * rows, width).astype(jnp.bfloat16)


def layer_kernel(
    sizes, far_q, k_ref, v_ref, decay_ref, offset_ref, far_open, head_gain_ref, far_residual,
    gain_ref, routes_ref, scores_ref, far_mix, far_gate, far_up, far_down,
    wide_gate, wide_up, wide_down, out_ref,
    q_ref, open_ref, residual_ref, qd_ref, qx_ref, kt_ref, ends_ref, starts_ref, inner_ref, state_ref,
    states_ref, carried_ref, reach_ref, packet_ref, packets_ref, gated_ref, swapped_ref,
    mixer_ref, x_ref, middle_ref, select_ref, mix_ref,
    column_ref, stage_ref, arrived_ref, made_ref, back_ref, sent_ref, came_ref, base_ref,
    hidden_ref, shared_ref, gate_ref, up_ref, down_ref, own_gate, own_up, own_down,
    weight_sem, ks, kr, gs, gr, ws, wr, zs, zr, ps, pr, bs, br, ss, sr,
):
    at = Place(*sizes).here()
    last = at.deep - 1
    flat, rows = stage_ref.shape[1], stage_ref.shape[2]
    width = x_ref.shape[1]
    experts = own_gate.shape[0]
    cap = rows // experts
    cuts = tiles_of(width)
    sides = tiles_of(width, 1024)
    pairs = (
        (far_q, q_ref), (far_open, open_ref), (far_residual, residual_ref),
        (far_mix, mixer_ref), (far_gate, gate_ref), (far_up, up_ref), (far_down, down_ref),
        (wide_gate, own_gate), (wide_up, own_up), (wide_down, own_down),
    )
    loads = [
        pltpu.make_async_copy(src, dst, weight_sem.at[i]) for i, (src, dst) in enumerate(pairs)
    ]
    for load in loads:
        load.start()
    has_right, has_left = at.a < last, at.a > 0
    count, tps = sizes
    met = call_on(
        [peer(lax.rem(at.sp + d, count), at.tp) for d in range(1, count)]
        + [at.plane(at.across(q)) for q in range(1, flat)]
    )
    half, wide = jnp.bfloat16, jnp.float32
    length, lanes = q_ref.shape
    heads = offset_ref.shape[0]
    blocks = length // BLOCK
    tokens = x_ref.shape[0]
    lane = lax.broadcasted_iota(jnp.int32, (1, lanes), 1)
    of_head = [
        (lane >= h * KEY_CHANNELS) & (lane < (h + 1) * KEY_CHANNELS) for h in range(heads)
    ]
    columns = [slice(h * VDIM, (h + 1) * VDIM) for h in range(heads)]
    tile = math.gcd(length, 4 * BLOCK)
    row = lax.broadcasted_iota(jnp.int32, (tile, tile), 0)
    col = lax.broadcasted_iota(jnp.int32, (tile, tile), 1)
    causal = (jnp.bitwise_and(row, -BLOCK) == jnp.bitwise_and(col, -BLOCK)) & (col <= row)
    ones = jnp.where(causal, 1.0, 0.0).astype(half)

    for t in range(0, length, tile):
        span = slice(t, t + tile)
        pre = decay_ref[span, :].astype(wide)
        log_decay = (
            jnp.minimum(pre, 0.0) - jnp.log1p(jnp.exp(-jnp.abs(pre)))
        ) / decay_running
        dropped = exact_dot(ones, offset_ref[:, span], dot_nt)
        offset = dropped[:, 0:1]
        for h in range(1, heads):
            offset = jnp.where(of_head[h], dropped[:, h : h + 1], offset)
        within = exact_dot(ones, log_decay, dot_nn) + offset
        keys = k_ref[span, :].astype(wide)
        qd_ref[span, :] = within
        for n in range(0, tile, BLOCK):
            inside = slice(n, n + BLOCK)
            end = within[n + BLOCK - 1 : n + BLOCK, :]
            kt_ref[t + n : t + n + BLOCK, :] = (
                keys[inside, :] * jnp.exp(end - within[inside, :])
            ).astype(half)
            ends_ref[(t + n) // BLOCK : (t + n) // BLOCK + 1, :] = end
    state = jnp.zeros((VDIM, lanes), wide)
    passed = jnp.zeros((1, lanes), wide)
    for n in range(blocks):
        span = slice(n * BLOCK, (n + 1) * BLOCK)
        starts_ref[n] = state.astype(half)
        end = ends_ref[n : n + 1, :]
        both = dot_tn(v_ref[span, :], kt_ref[span, :])
        added = both[columns[0], :]
        for h in range(1, heads):
            added = jnp.where(of_head[h], both[columns[h], :], added)
        state = state * jnp.exp(end) + added
        passed = passed + end
    state_ref[:VDIM, :] = state.astype(half)
    index = lax.broadcasted_iota(jnp.int32, (16, lanes), 0)
    pieces = jnp.zeros((16, lanes), wide)
    for i in range(3):
        piece = passed.astype(half).astype(wide)
        pieces = jnp.where(index == i, piece, pieces)
        passed = passed - piece
    state_ref[VDIM:, :] = pieces.astype(half)
    def packet_copy(d):
        return remote(
            packet_ref,
            packets_ref.at[at.a],
            ks.at[d],
            kr.at[at.a],
            at.column(lax.rem(at.a + d, at.deep)),
        )

    def packet_from(a):
        return remote(packet_ref, packets_ref.at[a], ks.at[0], kr.at[a], at.column(at.a))

    def state_copy(d):
        target = peer(jnp.minimum(at.sp + d, count - 1), at.tp)
        return remote(state_ref, states_ref.at[at.sp], gs.at[d], gr.at[at.sp], target)

    def swap_copy(d):
        to = lax.rem(at.tp + d, tps)
        return remote(
            gated_ref.at[to], swapped_ref.at[at.tp], ws.at[d], wr.at[at.tp], peer(at.sp, to)
        )

    packet_ref[:TOP_K, :] = routes_ref[...].astype(wide)
    packet_ref[TOP_K:, :] = scores_ref[...]
    packets_ref[at.a] = packet_ref[...]
    met()
    for d in range(1, at.deep):
        packet_copy(d).start()
    for d in range(1, count):

        @pl.when(at.sp + d < count)
        def _(d=d):
            state_copy(d).start()

    loads[0].wait()
    for t in range(0, length, tile):
        span = slice(t, t + tile)
        within = qd_ref[span, :]
        grown = k_ref[span, :].astype(wide) * jnp.exp(-within)
        ahead = q_ref[span, :].astype(wide) * KEY_CHANNELS ** (-0.5) * jnp.exp(within)
        qd_ref[span, :] = ahead
        ahead = ahead.astype(half)
        for h in range(heads):
            kept = jnp.where(of_head[h], grown, 0.0).astype(half)
            scores = jnp.where(causal, dot_nt(ahead, kept), 0.0)
            inner_ref[span, columns[h]] = jnp.dot(
                scores.astype(half), v_ref[span, columns[h]], preferred_element_type=wide
            )
    passed = jnp.zeros((1, lanes), wide)
    for n in range(blocks):
        span = slice(n * BLOCK, (n + 1) * BLOCK)
        for h in range(heads):
            ahead = jnp.where(of_head[h], qd_ref[span, :], 0.0)
            qx_ref[h, span, :] = (ahead * jnp.exp(passed)).astype(half)
            if n > 0:
                inner_ref[span, columns[h]] += dot_nt(ahead.astype(half), starts_ref[n])
        passed = passed + ends_ref[n : n + 1, :]

    slots = flat * rows
    plane_experts = flat * experts
    here = lax.broadcasted_iota(jnp.int32, (slots, plane_experts), 0)
    there = lax.broadcasted_iota(jnp.int32, (slots, plane_experts), 1) * cap
    belongs = (here >= there) & (here < there + cap)
    spread = jnp.where(belongs, 1.0, 0.0).astype(half)
    place = jnp.sum(
        jnp.where(belongs, (here - there).astype(wide), 0.0), axis=1, keepdims=True
    )
    expert = (
        at.a * plane_experts + lax.broadcasted_iota(jnp.int32, (plane_experts, 1), 0)
    ).astype(wide)
    sooner = jnp.where(
        lax.broadcasted_iota(jnp.int32, (tokens, tokens), 0)
        < lax.broadcasted_iota(jnp.int32, (tokens, tokens), 1),
        1.0,
        0.0,
    ).astype(half)
    def lay_out(a):
        pl.when(at.a != a)(lambda: packet_from(a).wait_recv())
        scored = packets_ref[a, TOP_K:, :]
        share = routed_scale * scored / jnp.sum(scored, axis=0, keepdims=True)
        chosen = jnp.zeros((plane_experts, tokens), wide)
        weight_of = jnp.zeros((plane_experts, tokens), wide)
        for k in range(TOP_K):
            hit = packets_ref[a, k : k + 1, :] == expert
            chosen = jnp.where(hit, 1.0, chosen)
            weight_of = jnp.where(hit, share[k : k + 1, :], weight_of)
        rank = jnp.dot(chosen.astype(half), sooner, preferred_element_type=wide)
        rank = jnp.where(chosen > 0.0, rank, -1.0)
        ranks = jnp.dot(spread, rank.astype(half), preferred_element_type=wide)
        weights = jnp.dot(spread, weight_of.astype(half), preferred_element_type=wide)
        taken = ranks == place
        select_ref[a] = jnp.where(taken, 1.0, 0.0).astype(half)
        mix_ref[a] = jnp.transpose(jnp.where(taken, weights, 0.0)).astype(half)

    early = at.deep // 2
    for i in range(early):
        lay_out(at.nearest(i))

    carried_ref[...] = jnp.zeros_like(carried_ref)
    reach_ref[...] = jnp.zeros_like(reach_ref)
    for j in reversed(range(count - 1)):

        @pl.when(j < at.sp)
        def _(j=j):
            source = peer(j, at.tp)
            remote(state_ref, states_ref.at[j], gs.at[0], gr.at[j], source).wait_recv()
            carried_ref[...] += jnp.exp(reach_ref[0:1, :]) * states_ref[j, :VDIM, :].astype(wide)
            log = jnp.sum(states_ref[j, VDIM:, :].astype(wide), axis=0, keepdims=True)
            reach_ref[0:1, :] += log

    carried = carried_ref[...].astype(half)
    loads[1].wait()
    for d in [*sorted(range(1, tps), key=lambda d: abs(2 * d - tps)), 0]:
        to = lax.rem(at.tp + d, tps)
        span = pl.ds(pl.multiple_of(to * tokens, tokens), tokens)
        for h in range(heads):
            output = inner_ref[span, columns[h]] + dot_nt(qx_ref[h, span, :], carried)
            inv_rms = lax.rsqrt(jnp.mean(output * output, axis=-1, keepdims=True) + eps_norm)
            gated_ref[to, :, columns[h]] = (
                output
                * inv_rms
                * head_gain_ref[...]
                * jax.nn.silu(open_ref[span, columns[h]].astype(wide))
            ).astype(half)
        if d > 0:
            swap_copy(d).start()
    for i in range(early, at.deep):
        lay_out(at.nearest(i))
    for load in loads[2:4]:
        load.wait()
    span = heads * VDIM
    for d in range(tps):
        source = lax.rem(at.tp - d + tps, tps)
        if d > 0:
            remote(
                gated_ref.at[0], swapped_ref.at[source], ws.at[0], wr.at[source], peer(at.sp, source)
            ).wait_recv()
        piece = gated_ref[source] if d == 0 else swapped_ref[source]
        part_of = pl.ds(pl.multiple_of(source * span, span), span)
        for cut in cuts:
            part = jnp.dot(piece, mixer_ref[part_of, cut], preferred_element_type=wide)
            if d == 0:
                base_ref[:, cut] = residual_ref[:, cut].astype(wide) + part
            else:
                base_ref[:, cut] += part
    square = jnp.zeros((tokens, 1), wide)
    for cut in cuts:
        middle_ref[:, cut] = base_ref[:, cut].astype(half)
        middle = middle_ref[:, cut].astype(wide)
        square = square + jnp.sum(middle * middle, axis=-1, keepdims=True)
    scale = lax.rsqrt(square / width + eps_norm)
    for cut in cuts:
        x_ref[:, cut] = (middle_ref[:, cut].astype(wide) * scale * gain_ref[:, cut]).astype(half)

    def relay(source, owner, side, j):
        return remote(
            source.at[:, sides[j]],
            column_ref.at[owner, :, sides[j]],
            zs.at[side, owner],
            zr.at[owner, j],
            at.column(at.a + (1 if side == 0 else -1)),
        )

    def sends(owner):
        right = has_right & (owner <= at.a)
        left = has_left & (owner >= at.a)
        return right, left

    def forward(source, owner, j):
        right, left = sends(owner)
        pl.when(right)(lambda: relay(source, owner, 0, j).start())
        pl.when(left)(lambda: relay(source, owner, 1, j).start())

    def out_copy(owner, q, j):
        target = at.across(q)
        return remote(
            stage_ref.at[owner, target, :, sides[j]],
            arrived_ref.at[owner, at.p, :, sides[j]],
            ps.at[owner],
            pr.at[owner, j],
            at.plane(target),
        )

    def out_all(owner, j):
        many = slice(1, flat)
        return remote(
            stage_ref.at[owner, many, :, sides[j]],
            arrived_ref.at[owner, many, :, sides[j]],
            ps.at[owner],
            pr.at[owner, j],
            at.plane(at.across(1)),
        )

    def back_copy(owner, q, i):
        target = at.across(q)
        return remote(
            made_ref.at[owner, target, :, cuts[i]],
            back_ref.at[owner, at.p, :, cuts[i]],
            bs.at[owner],
            br.at[owner, i],
            at.plane(target),
        )

    def back_all(owner, i):
        many = slice(1, flat)
        return remote(
            made_ref.at[owner, many, :, cuts[i]],
            back_ref.at[owner, many, :, cuts[i]],
            bs.at[owner],
            br.at[owner, i],
            at.plane(at.across(1)),
        )

    def pass_on(owner, source, j):
        start, stop = sides[j].start, sides[j].stop
        for cut in [cut for cut in cuts if start <= cut.start < stop]:
            picked = jnp.dot(
                select_ref[owner], source[:, cut], preferred_element_type=jnp.float32
            )
            stage_ref[owner, :, :, cut] = picked.reshape(flat, rows, -1).astype(jnp.bfloat16)
        for q in range(1, flat):
            out_copy(owner, q, j).start()
        arrived_ref[owner, at.p, :, sides[j]] = stage_ref[owner, at.p, :, sides[j]]

    def send_back(owner, i):
        for q in range(1, flat):
            back_copy(owner, q, i).start()

    def run_experts(owner):
        for j in range(len(sides)):
            out_all(owner, j).wait_recv()
        for e in range(experts):
            mine = slice(e * cap, (e + 1) * cap)
            block = flatten_rows(arrived_ref[owner, :, mine, :])
            for cut in tiles_of(own_gate.shape[2], 256):
                gate = jnp.dot(block, own_gate[e, :, cut], preferred_element_type=jnp.float32)
                up = jnp.dot(block, own_up[e, :, cut], preferred_element_type=jnp.float32)
                hidden_ref[e, :, cut] = (jax.nn.silu(gate) * up).astype(jnp.bfloat16)
        for i, cut in enumerate(cuts):
            for e in range(experts):
                mine = slice(e * cap, (e + 1) * cap)
                down = jnp.dot(
                    hidden_ref[e], own_down[e, :, cut], preferred_element_type=jnp.float32
                )
                made_ref[owner, :, mine, cut] = down.reshape(flat, cap, -1).astype(jnp.bfloat16)
        back_ref[owner, at.p] = made_ref[owner, at.p]

    def send_all(owner):
        for i in range(len(cuts)):
            send_back(owner, i)

    def mixed(owner, i):
        back_all(owner, i).wait_recv()
        block = flatten_rows(back_ref[owner, :, :, cuts[i]])
        return jnp.dot(mix_ref[owner], block, preferred_element_type=jnp.float32)

    def toward(owner, side, i):
        return remote(
            sent_ref.at[owner, :, cuts[i]],
            came_ref.at[side, owner, :, cuts[i]],
            ss.at[owner],
            sr.at[side, owner, i],
            at.column(at.a - 1 + 2 * side),
        )

    def step(owner, side, more, i):
        part = mixed(owner, i)
        if more:
            toward(owner, side, i).wait_recv()
            part = part + came_ref[side, owner, :, cuts[i]].astype(jnp.float32)
        sent_ref[owner, :, cuts[i]] = part.astype(jnp.bfloat16)
        toward(owner, side, i).start()

    def homeward(turn, place, i):
        side = jnp.where(2 * at.a < at.deep, 1 - place, place)
        owner = jnp.where(side == 0, last - turn, turn)
        goes = jnp.where(side == 0, owner < at.a, owner > at.a)
        far = jnp.where(side == 0, has_right, has_left)
        pl.when(goes & far)(lambda: step(owner, side, True, i))
        pl.when(goes & jnp.logical_not(far))(lambda: step(owner, side, False, i))

    def take(i):
        for j in range(len(sides)):
            relay(x_ref, order[i], 0, j).wait_recv()
            forward(column_ref.at[order[i]], order[i], j)
            pass_on(order[i], column_ref.at[order[i]], j)

    order = [at.nearest(i) for i in range(at.deep)]
    for j in range(len(sides)):
        forward(x_ref, at.a, j)
    for j in range(len(sides)):
        pass_on(at.a, x_ref, j)
    for load in loads[4:7]:
        load.wait()
    for cut in tiles_of(gate_ref.shape[1], 256):
        gate = jnp.dot(x_ref[...], gate_ref[:, cut], preferred_element_type=jnp.float32)
        up = jnp.dot(x_ref[...], up_ref[:, cut], preferred_element_type=jnp.float32)
        shared_ref[:, cut] = (jax.nn.silu(gate) * up).astype(jnp.bfloat16)
    for cut in cuts:
        base_ref[:, cut] = middle_ref[:, cut].astype(jnp.float32) + jnp.dot(
            shared_ref[...], down_ref[:, cut], preferred_element_type=jnp.float32
        )
    turns = [*range(2, at.deep), 1]
    early = [turn for turn in turns[:1] if turn < at.deep - 1]
    for i in range(1, at.deep + 1):
        if i < at.deep:
            take(i)
        if i == 1:
            for load in loads[7:]:
                load.wait()
        if i == at.deep:
            for turn in early:
                send_all(order[turn])
        run_experts(order[i - 1])
    for turn in turns[len(early) :]:
        send_all(order[turn])
    send_all(at.a)

    def sent_all(source, target, sent, came):
        remote(source, target, sent, came, at.plane(at.across(1))).wait_send()

    def drain_states(d, carry):
        @pl.when(at.sp + d < count)
        def _():
            state_copy(d).wait_send()

        return carry

    def drain_out(owner, carry):
        sent_all(stage_ref.at[owner, 1:], arrived_ref.at[owner, 1:], ps.at[owner], pr.at[owner, 0])
        return carry

    def drain_relay(owner, carry):
        for side, goes in enumerate(sends(owner)):

            @pl.when(goes)
            def _(side=side):
                sent_all(x_ref, column_ref.at[owner], zs.at[side, owner], zr.at[owner, 0])

        return carry

    for d in range(1, at.deep):
        packet_copy(d).wait_send()
    for d in range(1, tps):
        swap_copy(d).wait_send()
    lax.fori_loop(1, count, drain_states, 0)
    lax.fori_loop(0, at.deep, drain_relay, 0)
    lax.fori_loop(0, at.deep, drain_out, 0)
    for turn, later in zip(turns, [*turns[1:], None]):
        if turn == turns[0]:
            for i in range(len(cuts)):
                homeward(turn, 0, i)
        for i in range(len(cuts)):
            homeward(turn, 1, i)
            if later is not None:
                homeward(later, 0, i)

    for side, far in ((0, has_right), (1, has_left)):

        @pl.when(far)
        def _(side=side):
            for i, cut in enumerate(cuts):
                toward(at.a, side, i).wait_recv()
                base_ref[:, cut] += came_ref[side, at.a, :, cut].astype(jnp.float32)

    for i, cut in enumerate(cuts):
        out_ref[:, cut] = (base_ref[:, cut] + mixed(at.a, i)).astype(out_ref.dtype)
    def drain_back(owner, carry):
        sent_all(made_ref.at[owner, 1:], back_ref.at[owner, 1:], bs.at[owner], br.at[owner, 0])
        return carry

    def drain_home(owner, carry):
        @pl.when(owner != at.a)
        def _():
            sent_all(sent_ref.at[owner], came_ref.at[0, owner], ss.at[owner], sr.at[0, owner, 0])

        return carry

    lax.fori_loop(0, at.deep, drain_back, 0)
    lax.fori_loop(0, at.deep, drain_home, 0)


def on_device(
    queries,
    key_matrix,
    value_matrix,
    channel_decay_input,
    head_decay_offset,
    output_gate_input,
    head_norm_gain,
    residual,
    mixer_output_weight,
    expert_norm_gain,
    routes,
    chosen_router_scores,
    routed_gate_weight,
    routed_up_weight,
    routed_down_weight,
    common_gate_weight,
    common_up_weight,
    common_down_weight,
):
    count, tps = sizes = (lax.axis_size("sp"), lax.axis_size("tp"))
    at = Place(*sizes)
    tokens, width = residual.shape
    length, lanes = queries.shape
    heads = head_decay_offset.shape[1]
    blocks = length // BLOCK
    experts = routed_gate_weight.shape[0]
    cap = 2 * TOP_K * tokens // (experts * count * tps)
    rows = experts * cap
    slots = at.flat * rows
    parts, halves = len(tiles_of(width)), len(tiles_of(width, 1024))
    common = (common_gate_weight, common_up_weight, common_down_weight)
    routed = (routed_gate_weight, routed_up_weight, routed_down_weight)
    box = (at.deep, at.flat, rows, width)
    chunk = (at.deep, tokens, width)
    dma = pltpu.SemaphoreType.DMA
    half, wide = jnp.bfloat16, jnp.float32
    vmem = pl.BlockSpec(memory_space=pltpu.VMEM)
    far = pl.BlockSpec(memory_space=pl.ANY)
    return pl.pallas_call(
        functools.partial(layer_kernel, sizes),
        out_shape=pltpu.VMEM((tokens, width), half),
        in_specs=[far] + [vmem] * 4 + [far, vmem, far] + [vmem] * 3 + [far] * 7,
        out_specs=vmem,
        scratch_shapes=[
            pltpu.VMEM(queries.shape, half),
            pltpu.VMEM(output_gate_input.shape, half),
            pltpu.VMEM(residual.shape, half),
            pltpu.VMEM((length, lanes), wide),
            pltpu.VMEM((heads, length, lanes), half),
            pltpu.VMEM((length, lanes), half),
            pltpu.VMEM((max(8, blocks), lanes), wide),
            pltpu.VMEM((blocks, VDIM, lanes), half),
            pltpu.VMEM((length, heads * VDIM), wide),
            pltpu.VMEM((VDIM + 16, lanes), half),
            pltpu.VMEM((count, VDIM + 16, lanes), half),
            pltpu.VMEM((VDIM, lanes), wide),
            pltpu.VMEM((8, lanes), wide),
            pltpu.VMEM((2 * TOP_K, tokens), wide),
            pltpu.VMEM((at.deep, 2 * TOP_K, tokens), wide),
            pltpu.VMEM((tps, tokens, heads * VDIM), half),
            pltpu.VMEM((tps, tokens, heads * VDIM), half),
            pltpu.VMEM(mixer_output_weight.shape, half),
            pltpu.VMEM((tokens, width), half),
            pltpu.VMEM((tokens, width), half),
            pltpu.VMEM((at.deep, slots, tokens), half),
            pltpu.VMEM((at.deep, tokens, slots), half),
            pltpu.VMEM(chunk, half),
            pltpu.VMEM(box, half),
            pltpu.VMEM(box, half),
            pltpu.VMEM(box, half),
            pltpu.VMEM(box, half),
            pltpu.VMEM(chunk, half),
            pltpu.VMEM((2,) + chunk, half),
            pltpu.VMEM((tokens, width), wide),
            pltpu.VMEM((experts, at.flat * cap, routed[0].shape[2]), half),
            pltpu.VMEM((tokens, common[0].shape[1]), half),
            pltpu.VMEM(common[0].shape, half),
            pltpu.VMEM(common[1].shape, half),
            pltpu.VMEM(common[2].shape, half),
            pltpu.VMEM(routed[0].shape, half),
            pltpu.VMEM(routed[1].shape, half),
            pltpu.VMEM(routed[2].shape, half),
            dma((10,)),
            dma((at.deep,)),
            dma((at.deep,)),
            dma((count,)),
            dma((count,)),
            dma((tps,)),
            dma((tps,)),
            dma((2, at.deep)),
            dma((at.deep, halves)),
            dma((at.deep,)),
            dma((at.deep, halves)),
            dma((at.deep,)),
            dma((at.deep, parts)),
            dma((at.deep,)),
            dma((2, at.deep, parts)),
        ],
        compiler_params=pltpu.CompilerParams(
            collective_id=0, has_side_effects=True, vmem_limit_bytes=62 * 1024 * 1024
        ),
    )(
        queries,
        key_matrix,
        value_matrix,
        channel_decay_input,
        head_decay_offset.T,
        output_gate_input,
        head_norm_gain.reshape(1, -1),
        residual,
        expert_norm_gain.reshape(1, -1),
        routes.T,
        chosen_router_scores.T,
        mixer_output_weight,
        *common,
        *routed,
    )


def solution(mesh):
    placed = (
        P("sp", "tp"),
        P("sp", "tp"),
        P("sp", "tp"),
        P("sp", "tp"),
        P("sp", "tp"),
        P("sp", "tp"),
        P(),
        P(("sp", "tp"), None),
        P(),
        P(),
        P(("sp", "tp"), None),
        P(("sp", "tp"), None),
        P(("sp", "tp"), None, None),
        P(("sp", "tp"), None, None),
        P(("sp", "tp"), None, None),
        P(),
        P(),
        P(),
    )
    return jax.shard_map(
        on_device, mesh=mesh, in_specs=placed, out_specs=P(("sp", "tp"), None), check_vma=False
    )
```
